256 devices in a mesh: ep: 64 (over z, y, core), tp: 4 (over x).
Axes of the slice: x: 4, y: 4, z: 8, core: 2. Of those that a mesh axis runs over, the one named last changes fastest.
Arguments:
- tokens: bfloat16 [1536, 4096], P('ep'), may hold values from -16 to 16
- cotangent: bfloat16 [1536, 4096], P('ep'), may hold values from -1.5 to 1.5
- routes: int32 [1536, 4], P('ep'), may hold values from 0 to 63, all different within a row; in each aligned block of 24 rows (0 to 23, 24 to 47, ...) at most 3 rows name the same one
- route_weights: float32 [1536, 4], P('ep'), may hold values from 0.1 to 1.2
- expert_gate: bfloat16 [64, 4096, 192], P('ep', None, 'tp'), may hold values from -0.09375 to 0.09375
- expert_up: bfloat16 [64, 4096, 192], P('ep', None, 'tp'), may hold values from -0.09375 to 0.09375
- expert_down: bfloat16 [64, 192, 4096], P('ep', 'tp'), may hold values from -0.4375 to 0.4375
- shared_gate: bfloat16 [4096, 192], P(None, 'tp'), may hold values from -0.09375 to 0.09375
- shared_up: bfloat16 [4096, 192], P(None, 'tp'), may hold values from -0.09375 to 0.09375
- shared_down: bfloat16 [192, 4096], P('tp'), may hold values from -0.4375 to 0.4375
Outputs:
- grad_tokens: bfloat16 [1536, 4096], P('ep', 'tp')
- grad_route_weights: float32 [1536, 4], P('ep', 'tp')
- grad_expert_gate: float32 [64, 4096, 192], P('ep', None, 'tp')
- grad_expert_up: float32 [64, 4096, 192], P('ep', None, 'tp')
- grad_expert_down: float32 [64, 192, 4096], P('ep', 'tp')
- grad_shared_gate: float32 [4096, 192], P('ep', 'tp')
- grad_shared_up: float32 [4096, 192], P('ep', 'tp')
- grad_shared_down: float32 [192, 4096], P('tp', 'ep')
The draws below stay inside these ranges and needn't reach their ends.
Inputs may be any that keep to these rules, and one draw needn't show every extreme that they name: `routes`: each row names 4 different experts of 0 to 63; among the 24 rows of one index of ep (aligned blocks) no expert is named more than 3 times, and in every draw some block names some expert exactly 3 times.
All inputs are finite; a program needn't handle non-finite values.
Results may differ from the reference program's by a relative error of at most 0.015.
Values may be sent and summed in bfloat16 or wider, within the bound.
A program may use at most 64 MiB of HBM per device.

```python
import math
import jax
import jax.numpy as jnp
import numpy as np
from jax import lax

D = 4096
FF = 192
TOP = 4
TOK_DEV = 24
EXPERTS = 64
TOKENS = 1536
CAP = 3
N_EP = 64


def with_spikes(result, own_key, source, target, parts, factor):
    def block_of(position):
        return (jnp.arange(result.shape[position]) // (result.shape[position] // parts)).reshape((-1,) + (1,) * (result.ndim - 1 - position))

    one_side = jax.random.permutation(own_key, parts)[block_of(target)]
    other_side = (block_of(target) + parts // 2) % parts
    return jnp.where((block_of(source) == one_side) | (block_of(source) == other_side), factor * result, result)


def steps_of(key, shape, cuts, least, top_value):
    def one(position, parts):
        draws = jax.random.uniform(jax.random.fold_in(jax.random.fold_in(key, 6), position), (parts,), jnp.float32, least / len(cuts), top_value / len(cuts))
        return jnp.repeat(jnp.exp(draws), shape[position] // parts).reshape((-1,) + (1,) * (len(shape) - position - 1))

    loudness = one(*cuts[0])
    for cut in cuts[1:]:
        loudness = loudness * one(*cut)
    return loudness


def assign_block(own_key, own, number, rows, count, top, limit, skew):
    order = jax.random.permutation(own_key, count)
    packed, usual = load_shares(count, rows * top, limit, skew, True), load_shares(count, rows * top, limit, skew, False)
    places = jnp.arange(count)

    def named(lengths, offset_by):
        used = int((lengths > 0).sum())
        fixed = max(1, used // 4)
        passed = fixed + (places - fixed + offset_by * (used - fixed)) % max(1, count - fixed)
        return jnp.zeros((count,), jnp.int32).at[order[jnp.where(places < fixed, places, passed)]].set(jnp.asarray(lengths, jnp.int32))

    lengths = jnp.where(number % 4 == 0, named(packed, number // 4), named(usual, number - number // 4 - 1))
    mixed = jax.random.permutation(jax.random.fold_in(own, 3), count)
    donor, sink = mixed[0:count // 2 * 2:2], mixed[1:count // 2 * 2:2]
    room = jnp.minimum(lengths[donor] - 1, limit - lengths[sink]) // 2
    room = jnp.where((donor == order[0]) | (sink == order[0]) | (lengths[sink] == 0), 0, jnp.maximum(room, 0))
    passed = jax.random.randint(jax.random.fold_in(own, 4), (count // 2,), 0, 1 << 20) % (room + 1)
    lengths = lengths.at[donor].add(-passed).at[sink].add(passed)
    labels = jnp.searchsorted(jnp.cumsum(lengths), jnp.arange(rows * top), side="right").astype(jnp.int32)
    listing = labels.reshape(top, rows).T
    listing = listing[jax.random.permutation(jax.random.fold_in(own, 1), rows)]
    offset_by = jax.random.randint(jax.random.fold_in(own, 2), (rows, 1), 0, top)
    return jnp.take_along_axis(listing, (jnp.arange(top)[None, :] + offset_by) % top, axis=1)


def load_shares(number_of, total, limit, skew, full):
    loads = [(1 << 20) // math.isqrt(standing ** skew) + 1 for standing in range(1, number_of + 1)]
    largest = limit if full else min(limit, max(-(-total // number_of), total * loads[0] // sum(loads)))
    least = 1 if total - largest >= number_of - 1 else 0
    given, surplus = [largest] + [least] * (number_of - 1), total - largest - least * (number_of - 1)
    while surplus > 0:
        candidates = [i for i in range(1, number_of) if given[i] < largest] or [i for i in range(1, number_of) if given[i] < limit]
        whole, budget = sum([loads[i] for i in candidates]), surplus
        for i in candidates:
            more = min(limit - given[i], max(1, budget * loads[i] // whole), surplus)
            given[i] = given[i] + more
            surplus = surplus - more
    return np.array(given)


def scatter_about(key, shape, spread, most, pieces=(), kind=jnp.bfloat16):
    gain = steps_of(key, shape, pieces, -0.22, 0.18) if pieces else 1.0
    result = jax.random.normal(key, shape, jnp.float32) * spread * gain
    return jnp.minimum(jnp.maximum(result, -most), most).astype(kind)


def noise_with(own_key, dims, scale, most, shards, heavy, kind=jnp.bfloat16):
    array = scale * jax.random.normal(own_key, dims, jnp.float32)
    if shards:
        array = array * steps_of(own_key, dims, shards, -0.22, 0.18)
    return jnp.clip(with_spikes(array, jax.random.fold_in(own_key, 3), *heavy), -most, most).astype(kind)


def setup_inputs(seed: int = 0) -> dict:
    key_of = jax.random.split(jax.random.key(seed), 11)
    tokens = noise_with(key_of[0], (TOKENS, D), 1.0, 16.0, ((0, 64),), (0, 1, 64, 4.0))
    cotangent = scatter_about(key_of[1], (TOKENS, D), 0.25, 1.5, ((0, 64),))
    routes_keys = jax.random.split(jax.random.fold_in(key_of[2], 1), TOKENS // TOK_DEV)
    routes_turns = jax.random.permutation(jax.random.fold_in(key_of[2], 3), TOKENS // TOK_DEV)
    routes = jax.vmap(lambda own, number: assign_block(jax.random.fold_in(key_of[2], 2), own, number, TOK_DEV, EXPERTS, TOP, CAP, 2))(routes_keys, routes_turns).reshape((TOKENS, TOP))
    route_weights = jnp.clip(0.1 + 1.1 * jax.random.uniform(key_of[3], (TOKENS, TOP), jnp.float32) ** steps_of(key_of[3], (TOKENS, TOP), ((0, 64),), -0.2, 0.2), 0.1, 1.2)
    expert_gate = scatter_about(key_of[4], (EXPERTS, D, FF), D ** -0.5, 0.09375, ((0, 64), (2, 4)))
    expert_up = scatter_about(key_of[5], (EXPERTS, D, FF), D ** -0.5, 0.09375, ((0, 64), (2, 4)))
    expert_down = scatter_about(key_of[6], (EXPERTS, FF, D), FF ** -0.5, 0.4375, ((0, 64), (1, 4)))
    shared_gate = scatter_about(key_of[7], (D, FF), D ** -0.5, 0.09375, ((1, 4),))
    shared_up = scatter_about(key_of[8], (D, FF), D ** -0.5, 0.09375, ((1, 4),))
    shared_down = scatter_about(key_of[9], (FF, D), FF ** -0.5, 0.4375, ((0, 4),))
    return dict(tokens=tokens, cotangent=cotangent, routes=routes, route_weights=route_weights, expert_gate=expert_gate, expert_up=expert_up, expert_down=expert_down, shared_gate=shared_gate, shared_up=shared_up, shared_down=shared_down)


def swish_parts(gate_pre):
    sigma = jax.nn.sigmoid(gate_pre)
    return gate_pre * sigma, sigma * (1.0 + gate_pre * (1.0 - sigma))


def expert_backward(rows_x, rows_g, rows_w, w_gate, w_up, w_down):
    gate = jnp.dot(rows_x, w_gate, preferred_element_type=jnp.float32)
    up_val = jnp.dot(rows_x, w_up, preferred_element_type=jnp.float32)
    active, slope = swish_parts(gate)
    hidden = (active * up_val).astype(jnp.bfloat16)
    back = jnp.dot(rows_g, w_down.T, preferred_element_type=jnp.float32)
    gate_grad = jnp.sum(hidden.astype(jnp.float32) * back, axis=-1)
    d_hidden = rows_w[:, None] * back
    d_gate = (d_hidden * up_val * slope).astype(jnp.bfloat16)
    d_up = (d_hidden * active).astype(jnp.bfloat16)
    scaled = (rows_w[:, None] * hidden.astype(jnp.float32)).astype(jnp.bfloat16)
    grad_down = jnp.dot(scaled.T, rows_g, preferred_element_type=jnp.float32)
    grad_gate = jnp.dot(rows_x.T, d_gate, preferred_element_type=jnp.float32)
    grad_up = jnp.dot(rows_x.T, d_up, preferred_element_type=jnp.float32)
    row_dx = jnp.dot(d_gate, w_gate.T, preferred_element_type=jnp.float32)
    row_dx = row_dx + jnp.dot(d_up, w_up.T, preferred_element_type=jnp.float32)
    return row_dx, gate_grad, grad_gate, grad_up, grad_down


def reference(tokens, cotangent, routes, route_weights, expert_gate, expert_up, expert_down, shared_gate, shared_up, shared_down):
    s_gate = jnp.dot(tokens, shared_gate, preferred_element_type=jnp.float32)
    s_up = jnp.dot(tokens, shared_up, preferred_element_type=jnp.float32)
    s_active, s_slope = swish_parts(s_gate)
    s_hidden = (s_active * s_up).astype(jnp.bfloat16)
    s_back = jnp.dot(cotangent, shared_down.T, preferred_element_type=jnp.float32)
    ds_gate = (s_back * s_up * s_slope).astype(jnp.bfloat16)
    ds_up = (s_back * s_active).astype(jnp.bfloat16)
    shared_dx = jnp.dot(ds_gate, shared_gate.T, preferred_element_type=jnp.float32)
    shared_dx = shared_dx + jnp.dot(ds_up, shared_up.T, preferred_element_type=jnp.float32)
    grad_shared_gate = jnp.dot(tokens.T, ds_gate, preferred_element_type=jnp.float32)
    grad_shared_up = jnp.dot(tokens.T, ds_up, preferred_element_type=jnp.float32)
    grad_shared_down = jnp.dot(s_hidden.T, cotangent, preferred_element_type=jnp.float32)

    flat = routes.reshape(-1).astype(jnp.int32)
    assigns = flat.shape[0]
    order = jnp.argsort(flat, stable=True).astype(jnp.int32)
    expert_ids = jnp.arange(EXPERTS, dtype=jnp.int32)
    counts = jnp.sum((flat[None, :] == expert_ids[:, None]).astype(jnp.int32), axis=1)
    starts = jnp.cumsum(counts) - counts
    slot_count = N_EP * CAP
    offsets = jnp.arange(slot_count, dtype=jnp.int32)
    index = jnp.minimum(starts[:, None] + offsets[None, :], assigns - 1).astype(jnp.int32)
    assign_of = jnp.where(offsets[None, :] < counts[:, None], order[index], assigns).astype(jnp.int32)
    token_of = (assign_of // TOP).astype(jnp.int32)
    padded_x = jnp.concatenate([tokens, jnp.zeros((1, D), tokens.dtype)], axis=0)
    padded_g = jnp.concatenate([cotangent, jnp.zeros((1, D), cotangent.dtype)], axis=0)
    padded_w = jnp.concatenate([route_weights.reshape(-1), jnp.zeros((1,), route_weights.dtype)], axis=0)

    def per_expert(operands):
        w_gate, w_up, w_down, assign_row, token_row = operands
        return expert_backward(padded_x[token_row], padded_g[token_row], padded_w[assign_row], w_gate, w_up, w_down)

    row_dx, gate_grad, grad_gate, grad_up, grad_down = lax.map(
        per_expert, (expert_gate, expert_up, expert_down, assign_of, token_of))
    routed = jnp.zeros((TOKENS + 1, D), jnp.float32).at[token_of.reshape(-1)].add(row_dx.reshape(-1, D))
    grad_tokens = (routed[:TOKENS] + shared_dx).astype(jnp.bfloat16)
    grad_route = jnp.zeros((assigns + 1,), jnp.float32).at[assign_of.reshape(-1)].set(gate_grad.reshape(-1))
    grad_route = grad_route[:assigns].reshape(TOKENS, TOP)
    return (grad_tokens, grad_route, grad_gate, grad_up, grad_down, grad_shared_gate, grad_shared_up, grad_shared_down)
```

```python
import functools

import jax
import jax.numpy as jnp
from jax import lax
from jax.experimental import pallas as pl
from jax.experimental.pallas import tpu as pltpu
from jax.sharding import PartitionSpec as P

MESH = pl.DeviceIdType.MESH
F32 = jnp.float32
BF16 = jnp.bfloat16
EP_AXES = (8, 4, 2)
CAP = 3


def dot_nn(a, b):
    return lax.dot_general(a, b, (((1,), (0,)), ((), ())), preferred_element_type=F32)


def dot_nt(a, b):
    return lax.dot_general(a, b, (((1,), (1,)), ((), ())), preferred_element_type=F32)


def dot_tn(a, b):
    return lax.dot_general(a, b, (((0,), (0,)), ((), ())), preferred_element_type=F32)


def wait_bytes(ref, sem):
    pltpu.make_async_copy(ref, ref, sem).wait()


def swish_parts(v):
    sigma = jax.nn.sigmoid(v)
    return v * sigma, sigma * (1.0 + v * (1.0 - sigma))


def swap_matrix(outer, inner):
    size = outer * inner
    row = lax.broadcasted_iota(jnp.int32, (size, size), 0)
    col = lax.broadcasted_iota(jnp.int32, (size, size), 1)
    return ((row % inner) * outer + row // inner == col).astype(BF16)


def kernel(
    sizes,
    assign_of,
    slot_of,
    weight_of,
    x_ref,
    g_ref,
    wg_ref,
    wu_ref,
    wd_ref,
    sg_ref,
    su_ref,
    sd_ref,
    dx_out,
    gr_out,
    gw_out,
    gs_out,
    tiles,
    send_x,
    recv_x,
    wq,
    rows,
    part,
    rs_send,
    rs_recv,
    dall,
    back_send,
    back_recv,
    gp_send,
    gp_recv,
    dw_send,
    sdx_send,
    sdx_recv,
    sh1,
    sh1_recv,
    sh2,
    sh2_recv,
    sh3,
    sh3_recv,
    sh4,
    sh4_recv,
    comb,
    grow,
    sem,
):
    ep, tp, nz, ny, cap, tok, top, dq, ff, cb = sizes
    nb = dq // 128
    slots = ep * cap
    own_rows = slots // tp
    fo = ff // tp
    chunk = cap * 2 * nb
    me = lax.axis_index("ep")
    q = lax.axis_index("tp")
    core = lax.rem(me, 2)
    yy = lax.rem(me // 2, ny)
    zz = me // (2 * ny)
    sib = me + 1 - 2 * core

    def ep_peer(i):
        return lax.rem(me + i, ep)

    def tp_peer(i):
        return lax.rem(q + i, tp)

    def send(src, dst, kind, device):
        pltpu.make_async_remote_copy(
            src_ref=src,
            dst_ref=dst,
            send_sem=sem.at[2 * kind],
            recv_sem=sem.at[2 * kind + 1],
            device_id=device,
            device_id_type=MESH,
        ).start()

    def waits(ref, kind, side):
        wait_bytes(ref, sem.at[2 * kind + side])

    barrier = pltpu.get_barrier_semaphore()

    @pl.loop(1, ep)
    def _(i):
        pl.semaphore_signal(barrier, inc=1, device_id={"ep": ep_peer(i)}, device_id_type=MESH)

    for i in range(1, tp):
        pl.semaphore_signal(barrier, inc=1, device_id={"tp": tp_peer(i)}, device_id_type=MESH)

    col0 = q * dq
    swap_in = swap_matrix(2 * nb, 16)
    swap_out = swap_matrix(16, 2 * nb)
    for part_no in range(2):
        lo = part_no * 16
        hi = min(tok, lo + 16)
        pieces = []
        for ref in (x_ref, g_ref):
            for b in range(nb):
                cols = pl.ds(pl.multiple_of(col0 + b * 128, 128), 128)
                piece = ref[lo:hi, cols].astype(F32)
                if hi - lo < 16:
                    piece = jnp.concatenate([piece, jnp.zeros((16 - hi + lo, 128), F32)], axis=0)
                pieces.append(piece)
        stacked = jnp.concatenate(pieces, axis=0).astype(BF16)
        moved = dot_nn(swap_out, stacked)
        tiles[lo : lo + 16] = moved.reshape(16, 2 * nb, 128)

    lower = lax.broadcasted_iota(jnp.int32, (2 * nb, 128), 0) < nb

    @pl.loop(0, slots, unroll=4)
    def _(s):
        a = assign_of[s]
        tile = tiles[a // top]
        scale = jnp.where(lower, jnp.float32(1.0), weight_of[a])
        send_x[pl.ds(pl.multiple_of(s * 2 * nb, 2 * nb), 2 * nb), :] = (tile * scale).astype(BF16)

    pl.semaphore_wait(barrier, ep - 1 + tp - 1)

    def chunk_of(i, size):
        return pl.ds(pl.multiple_of(i * size, size), size)

    for t, ref in enumerate((wg_ref, wu_ref, wd_ref)):
        for i in range(1, tp):
            dst_rows = pl.ds(pl.multiple_of(t * ff + q * fo, 16), fo)
            src_cols = pl.ds(pl.multiple_of(tp_peer(i) * dq, 128), dq)
            send(ref.at[:, src_cols], wq.at[dst_rows, :], 0, {"tp": tp_peer(i)})

    @pl.loop(1, ep)
    def _(i):
        p = ep_peer(i)
        send(send_x.at[chunk_of(p, chunk), :], recv_x.at[chunk_of(me, chunk), :], 1, {"ep": p})

    recv_x[chunk_of(me, chunk), :] = send_x[chunk_of(me, chunk), :]
    own_cols = pl.ds(pl.multiple_of(q * dq, 128), dq)
    for t, ref in enumerate((wg_ref, wu_ref, wd_ref)):
        wq[pl.ds(pl.multiple_of(t * ff + q * fo, 16), fo), :] = ref[:, own_cols]

    x = x_ref[...]
    g = g_ref[...]
    s_gate = dot_nt(x, sg_ref[...])
    s_up = dot_nt(x, su_ref[...])
    s_back = dot_nt(g, sd_ref[...])
    s_active, s_slope = swish_parts(s_gate)
    s_hidden = (s_active * s_up).astype(BF16)
    ds_gate = (s_back * s_up * s_slope).astype(BF16)
    ds_up = (s_back * s_active).astype(BF16)
    for j in range(tp):
        cols = slice(j * dq, (j + 1) * dq)
        piece = dot_nn(ds_gate, sg_ref[:, cols]) + dot_nn(ds_up, su_ref[:, cols])
        sdx_send[j] = piece.astype(BF16)
    for i in range(1, tp):
        send(sdx_send.at[tp_peer(i)], sdx_recv.at[q], 2, {"tp": tp_peer(i)})
    half = 3 * fo // 2
    for z in range(nz):
        cols = slice(z * ny * cb, (z + 1) * ny * cb)
        xz = x_ref[:, cols]
        whole = jnp.concatenate(
            [dot_tn(ds_gate, xz), dot_tn(ds_up, xz), dot_tn(s_hidden, g_ref[:, cols])], axis=0
        )
        for y in range(ny):
            for h in range(2):
                sh1[h, y, z] = whole[h * half : (h + 1) * half, y * cb : (y + 1) * cb].astype(BF16)
    send(sh1.at[1 - core], sh1_recv, 3, {"ep": sib})
    waits(sh1_recv, 3, 1)
    for y in range(ny):
        for z in range(nz):
            both = sh1[core, y, z].astype(F32) + sh1_recv[y, z].astype(F32)
            sh2[y, z] = both.astype(BF16)
    for i in range(1, ny):
        y = lax.rem(yy + i, ny)
        send(sh2.at[y], sh2_recv.at[yy], 4, {"ep": (zz * ny + y) * 2 + core})
    if ny > 1:
        waits(sh2_recv.at[pl.ds(0, ny - 1)], 4, 1)
    for z in range(nz):
        total = sh2[yy, z].astype(F32)
        for i in range(1, ny):
            total = total + sh2_recv[lax.rem(yy + i, ny), z].astype(F32)
        sh3[z] = total.astype(BF16)
    for i in range(1, nz):
        z = lax.rem(zz + i, nz)
        send(sh3.at[z], sh3_recv.at[zz], 5, {"ep": (z * ny + yy) * 2 + core})

    waits(wq.at[pl.ds(0, 3 * (tp - 1) * fo), :], 0, 1)
    waits(recv_x.at[pl.ds(0, (ep - 1) * chunk), :], 1, 1)

    @pl.loop(0, slots // 16)
    def _(i):
        block = recv_x[pl.ds(pl.multiple_of(i * 32 * nb, 32 * nb), 32 * nb), :]
        moved = dot_nn(swap_in, block).astype(BF16)
        for b in range(2 * nb):
            rows[pl.ds(pl.multiple_of(i * 16, 16), 16), b * 128 : (b + 1) * 128] = moved[b * 16 : (b + 1) * 16]

    xr = rows[:, 0:dq]
    gr = rows[:, dq : 2 * dq]
    up_part = dot_nt(xr, wq[0 : 2 * ff, :])
    back_part = dot_nt(gr, wq[2 * ff : 3 * ff, :])
    part[:, 0 : 2 * ff] = up_part
    part[:, 2 * ff : 3 * ff] = back_part
    rs_send[:, 0 : 2 * ff] = up_part.astype(BF16)
    rs_send[:, 2 * ff : 3 * ff] = back_part.astype(BF16)
    for i in range(1, tp):
        send(rs_send.at[chunk_of(tp_peer(i), own_rows), :], rs_recv.at[chunk_of(q, own_rows), :], 6, {"tp": tp_peer(i)})
    waits(rs_recv.at[pl.ds(0, (tp - 1) * own_rows), :], 6, 1)
    total = part[chunk_of(q, own_rows), :]
    for i in range(1, tp):
        total = total + rs_recv[chunk_of(tp_peer(i), own_rows), :].astype(F32)
    gate = total[:, 0:ff]
    up = total[:, ff : 2 * ff]
    back = total[:, 2 * ff : 3 * ff]
    active, slope = swish_parts(gate)
    hidden = (active * up).astype(BF16)
    gp = jnp.sum(hidden.astype(F32) * back, axis=1, keepdims=True)
    d_gate = back * up * slope
    d_up = back * active
    extra = dall.shape[1] - 3 * ff
    dall[chunk_of(q, own_rows), :] = jnp.concatenate(
        [d_gate, d_up, hidden.astype(F32), jnp.broadcast_to(gp, (own_rows, extra))], axis=1
    ).astype(BF16)
    for i in range(1, tp):
        mine = dall.at[chunk_of(q, own_rows), :]
        send(mine, mine, 7, {"tp": tp_peer(i)})
    waits(dall.at[pl.ds(0, (tp - 1) * own_rows), :], 7, 1)

    dgu = dall[:, 0 : 2 * ff]
    dh = dall[:, 2 * ff : 3 * ff]
    swap_back = swap_matrix(16, nb)
    dxr = dot_nn(dgu, wq[0 : 2 * ff, :])
    for i in range(slots // 16):
        stacked = jnp.concatenate(
            [dxr[i * 16 : (i + 1) * 16, b * 128 : (b + 1) * 128] for b in range(nb)], axis=0
        ).astype(BF16)
        moved = dot_nn(swap_back, stacked)
        back_send[i * 16 : (i + 1) * 16] = moved.reshape(16, nb, 128).astype(BF16)
    src_row = lax.broadcasted_iota(jnp.int32, (ep, slots), 0)
    src_col = lax.broadcasted_iota(jnp.int32, (ep, slots), 1)
    collect = (src_col // cap == src_row).astype(F32)
    lane = lax.broadcasted_iota(jnp.int32, (slots, 128), 1)
    slot_row = lax.broadcasted_iota(jnp.int32, (slots, 128), 0)
    gp_all = dall[:, 3 * ff : 3 * ff + 1].astype(F32)
    spread = jnp.where(lane == slot_row % cap, gp_all, 0.0)
    gp_rows = dot_nn(collect, spread)
    gp_send[...] = gp_rows.reshape(ep, 1, 128)

    @pl.loop(1, ep)
    def _(i):
        p = ep_peer(i)
        send(back_send.at[pl.ds(p * cap, cap)], back_recv.at[pl.ds(me * cap, cap)], 8, {"ep": p})
        send(gp_send.at[p], gp_recv.at[me], 9, {"ep": p})

    back_recv[pl.ds(me * cap, cap)] = back_send[pl.ds(me * cap, cap)]
    gp_recv[me] = gp_send[me]

    dw_send[0 : 2 * ff, :] = dot_tn(dgu, rows[:, 0:dq]).astype(BF16)
    dw_send[2 * ff : 3 * ff, :] = dot_tn(dh, rows[:, dq : 2 * dq]).astype(BF16)
    for t in range(3):
        for i in range(1, tp):
            src_rows = pl.ds(pl.multiple_of(t * ff + tp_peer(i) * fo, 16), fo)
            send(dw_send.at[src_rows, :], gw_out.at[t, :, own_cols], 10, {"tp": tp_peer(i)})
        mine = pl.ds(pl.multiple_of(t * ff + q * fo, 16), fo)
        gw_out[t, :, own_cols] = dw_send[mine, :]

    if nz > 1:
        waits(sh3_recv.at[pl.ds(0, nz - 1)], 5, 1)
    total = sh3[zz].astype(F32)
    for i in range(1, nz):
        total = total + sh3_recv[lax.rem(zz + i, nz)].astype(F32)
    sh4[...] = total
    send(sh4, sh4_recv, 11, {"ep": sib})
    waits(sh4_recv, 11, 1)
    first = core == 0
    full = jnp.concatenate(
        [
            jnp.where(first, sh4[...], sh4_recv[...]),
            jnp.where(first, sh4_recv[...], sh4[...]),
        ],
        axis=0,
    )
    gs_out[...] = jnp.where(first, full[:, 0 : cb // 2], full[:, cb // 2 : cb])

    waits(sdx_recv.at[pl.ds(0, tp - 1)], 2, 1)
    waits(back_recv.at[pl.ds(0, (ep - 1) * cap)], 8, 1)
    waits(gp_recv.at[pl.ds(0, ep - 1)], 9, 1)
    row_lane = lax.broadcasted_iota(jnp.int32, (1, 128), 1)
    comb[...] = jnp.zeros_like(comb)
    for t in range(tok):
        total = back_recv[slot_of[t * top]].astype(F32)
        for k in range(1, top):
            total = total + back_recv[slot_of[t * top + k]].astype(F32)
        comb[t] = total
        s = slot_of[t * top + q]
        value = jnp.where(row_lane == s % cap, gp_recv[s // cap], 0.0)
        grow[t : t + 1, :] = value / jnp.full((1, 128), weight_of[t * top + q], F32)
    gr_out[...] = jnp.sum(grow[...], axis=1, keepdims=True)
    swap_tok = swap_matrix(nb, 16)
    for part_no in range(2):
        lo = part_no * 16
        hi = min(tok, lo + 16)
        v = comb[lo : lo + 16].reshape(16 * nb, 128)
        top_half = v.astype(BF16)
        rest = (v - top_half.astype(F32)).astype(BF16)
        moved = dot_nn(swap_tok, top_half) + dot_nn(swap_tok, rest)
        for b in range(nb):
            cols = slice(b * 128, (b + 1) * 128)
            value = moved[b * 16 : b * 16 + hi - lo]
            value = value + sdx_send[q, lo:hi, cols].astype(F32)
            for i in range(1, tp):
                value = value + sdx_recv[tp_peer(i), lo:hi, cols].astype(F32)
            dx_out[lo:hi, cols] = value.astype(BF16)

    waits(gw_out.at[:, :, 0 : (tp - 1) * dq], 10, 1)
    waits(wq.at[pl.ds(0, 3 * (tp - 1) * fo), :], 0, 0)
    waits(send_x.at[pl.ds(0, (ep - 1) * chunk), :], 1, 0)
    waits(sdx_send.at[pl.ds(0, tp - 1)], 2, 0)
    waits(sh1_recv, 3, 0)
    if ny > 1:
        waits(sh2.at[pl.ds(0, ny - 1)], 4, 0)
    if nz > 1:
        waits(sh3.at[pl.ds(0, nz - 1)], 5, 0)
    waits(rs_send.at[pl.ds(0, (tp - 1) * own_rows), :], 6, 0)
    waits(dall.at[pl.ds(0, (tp - 1) * own_rows), :], 7, 0)
    waits(back_send.at[pl.ds(0, (ep - 1) * cap)], 8, 0)
    waits(gp_send.at[pl.ds(0, ep - 1)], 9, 0)
    waits(dw_send.at[pl.ds(0, 3 * (tp - 1) * fo), :], 10, 0)
    waits(sh4, 11, 0)


def local(axes, cap, tokens, cotangent, routes, route_weights, expert_gate, expert_up, expert_down, shared_gate, shared_up, shared_down):
    tok, width = tokens.shape
    top = routes.shape[1]
    nz, ny, _ = axes
    ep = lax.axis_size("ep")
    tp = lax.axis_size("tp")
    fo = expert_gate.shape[2]
    ff = fo * tp
    dq = width // tp
    nb = dq // 128
    cb = width // (nz * ny)
    slots = ep * cap
    own_rows = slots // tp
    chunk = cap * 2 * nb
    wide = -(-(3 * ff + 1) // 128) * 128
    half = 3 * fo // 2

    flat = routes.reshape(-1)
    count = tok * top
    row = jnp.arange(count, dtype=jnp.int32) // top
    same = (flat[:, None] == flat[None, :]) & (row[None, :] < row[:, None])
    slot_of = flat * cap + jnp.sum(same.astype(jnp.int32), axis=1)
    hit = slot_of[None, :] == jnp.arange(slots, dtype=jnp.int32)[:, None]
    number = jnp.arange(count, dtype=jnp.int32) - count
    assign_of = count + jnp.sum(jnp.where(hit, number[None, :], 0), axis=1)
    weight_of = jnp.concatenate([route_weights.reshape(-1), jnp.zeros((8,), F32)])

    sizes = (ep, tp, nz, ny, cap, tok, top, dq, ff, cb)
    vmem = pl.BlockSpec(memory_space=pltpu.VMEM)
    smem = pl.BlockSpec(memory_space=pltpu.SMEM)
    dx, gr, gw, gs = pl.pallas_call(
        functools.partial(kernel, sizes),
        out_shape=(
            jax.ShapeDtypeStruct((tok, dq), BF16),
            jax.ShapeDtypeStruct((tok, 1), F32),
            jax.ShapeDtypeStruct((3, fo, width), BF16),
            jax.ShapeDtypeStruct((3 * fo, cb // 2), F32),
        ),
        in_specs=[smem] * 3 + [vmem] * 8,
        out_specs=(vmem,) * 4,
        scratch_shapes=[
            pltpu.VMEM((32, 2 * nb, 128), F32),
            pltpu.VMEM((slots * 2 * nb, 128), BF16),
            pltpu.VMEM((slots * 2 * nb, 128), BF16),
            pltpu.VMEM((3 * ff, dq), BF16),
            pltpu.VMEM((slots, 2 * dq), BF16),
            pltpu.VMEM((slots, wide), F32),
            pltpu.VMEM((slots, wide), BF16),
            pltpu.VMEM((slots, wide), BF16),
            pltpu.VMEM((slots, wide), BF16),
            pltpu.VMEM((slots, nb, 128), BF16),
            pltpu.VMEM((slots, nb, 128), BF16),
            pltpu.VMEM((ep, 1, 128), F32),
            pltpu.VMEM((ep, 1, 128), F32),
            pltpu.VMEM((3 * ff, dq), BF16),
            pltpu.VMEM((tp, tok, dq), BF16),
            pltpu.VMEM((tp, tok, dq), BF16),
            pltpu.VMEM((2, ny, nz, half, cb), BF16),
            pltpu.VMEM((ny, nz, half, cb), BF16),
            pltpu.VMEM((ny, nz, half, cb), BF16),
            pltpu.VMEM((ny, nz, half, cb), BF16),
            pltpu.VMEM((nz, half, cb), BF16),
            pltpu.VMEM((nz, half, cb), BF16),
            pltpu.VMEM((half, cb), F32),
            pltpu.VMEM((half, cb), F32),
            pltpu.VMEM((32, nb, 128), F32),
            pltpu.VMEM((tok, 128), F32),
            pltpu.SemaphoreType.DMA((24,)),
        ],
        compiler_params=pltpu.CompilerParams(
            collective_id=0, has_side_effects=True, vmem_limit_bytes=48 * 1024 * 1024
        ),
    )(
        assign_of,
        slot_of,
        weight_of,
        tokens,
        cotangent,
        expert_gate[0].T,
        expert_up[0].T,
        expert_down[0],
        shared_gate.T,
        shared_up.T,
        shared_down,
    )
    gw = gw.astype(F32)
    return (
        dx,
        gr,
        gw[0].T[None],
        gw[1].T[None],
        gw[2][None],
        gs[0:fo].T,
        gs[fo : 2 * fo].T,
        gs[2 * fo :],
    )


def solution(mesh):
    placed = (
        P("ep", None),
        P("ep", None),
        P("ep", None),
        P("ep", None),
        P("ep", None, "tp"),
        P("ep", None, "tp"),
        P("ep", "tp", None),
        P(None, "tp"),
        P(None, "tp"),
        P("tp", None),
    )
    return jax.shard_map(
        functools.partial(local, EP_AXES, CAP),
        mesh=mesh,
        in_specs=placed,
        out_specs=(
            P("ep", "tp"),
            P("ep", "tp"),
            P("ep", None, "tp"),
            P("ep", None, "tp"),
            P("ep", "tp", None),
            P("ep", "tp"),
            P("ep", "tp"),
            P("tp", "ep"),
        ),
        check_vma=False,
    )
```

```python
import functools

import jax
import jax.numpy as jnp
from jax import lax
from jax.experimental import pallas as pl
from jax.experimental.pallas import tpu as pltpu
from jax.sharding import PartitionSpec as P

MESH = pl.DeviceIdType.MESH
F32 = jnp.float32
BF16 = jnp.bfloat16
I32 = jnp.int32
EP_AXES = (8, 4, 2)
CAP = 3
(WEIGHTS, DISPATCH, SHARED_DX, SHARED_1, SHARED_2, SHARED_3, SHARED_4, SCATTER, GATHER, BACK, GP, GRADS) = range(
    0, 72, 6
)


def dot_nn(a, b):
    return lax.dot_general(a, b, (((1,), (0,)), ((), ())), preferred_element_type=F32)


def dot_nt(a, b):
    return lax.dot_general(a, b, (((1,), (1,)), ((), ())), preferred_element_type=F32)


def dot_tn(a, b):
    return lax.dot_general(a, b, (((0,), (0,)), ((), ())), preferred_element_type=F32)


def wait_bytes(ref, sem):
    pltpu.make_async_copy(ref, ref, sem).wait()


def swish_parts(v):
    sigma = jax.nn.sigmoid(v)
    return v * sigma, sigma * (1.0 + v * (1.0 - sigma))


def swap_matrix(outer, inner):
    size = outer * inner
    row = lax.broadcasted_iota(I32, (size, size), 0)
    col = lax.broadcasted_iota(I32, (size, size), 1)
    return ((row % inner) * outer + row // inner == col).astype(BF16)


def z_order(nz):
    steps = sorted(range(1, nz), key=lambda dz: (-min(dz, nz - dz), dz))
    near = [dz for dz in steps if min(dz, nz - dz) <= 2]
    return tuple([dz for dz in steps if dz not in near] + [0] + near)


def groups_of(ep):
    return ((0, ep // 2), (ep // 2, ep // 4), (ep // 2 + ep // 4, ep // 4))


def kernel(
    sizes,
    routes_in,
    weights_in,
    x_in,
    g_in,
    wg_in,
    wu_in,
    wd_in,
    sg_in,
    su_in,
    sd_in,
    dx_out,
    gr_out,
    gg_out,
    gu_out,
    gd_out,
    gs_out,
    routes,
    weights,
    weight_turn,
    assign_table,
    assign_of,
    scale_table,
    scale_of,
    slot_table,
    slot_of,
    turn,
    x_ref,
    g_ref,
    sg_ref,
    su_ref,
    sd_ref,
    tiles,
    send_x,
    recv_x,
    wq,
    rows,
    part,
    rs_send,
    rs_recv,
    rest,
    rest_send,
    rest_recv,
    dall,
    dfull,
    back_send,
    back_recv,
    gp_send,
    gp_recv,
    dw_send,
    sdx_send,
    sdx_recv,
    sh1,
    sh1_recv,
    sh2,
    sh2_recv,
    sh3,
    sh3_recv,
    sh4,
    sh4_recv,
    comb,
    grow,
    gs_held,
    dx_held,
    gr_held,
    sem,
    in_sem,
):
    ep, tp, nz, ny, cap, tok, top, dq, ff, cb = sizes
    nb = dq // 128
    nyc = 2 * ny
    groups = groups_of(ep)
    first_rows = groups[0][1] * cap
    own_rows = first_rows // tp
    fo = ff // tp
    chunk = cap * 2 * nb
    me = lax.axis_index("ep")
    q = lax.axis_index("tp")
    core = lax.rem(me, 2)
    yc = lax.rem(me, nyc)
    yy = yc // 2
    zz = me // nyc
    sib = me + 1 - 2 * core

    def tp_peer(i):
        return lax.rem(q + i, tp)

    def to_of(dz, w):
        return lax.rem(zz + dz, nz) * nyc + lax.rem(yc + w, nyc)

    def from_of(dz, w):
        return lax.rem(zz + nz - dz, nz) * nyc + lax.rem(yc + nyc - w, nyc)

    def send(src, dst, kind, device):
        pltpu.make_async_remote_copy(
            src_ref=src,
            dst_ref=dst,
            send_sem=sem.at[kind],
            recv_sem=sem.at[kind + 1],
            device_id=device,
            device_id_type=MESH,
        ).start()

    def waits(ref, kind, side):
        wait_bytes(ref, sem.at[kind + side])

    def positions(group):
        start, count = groups[group]
        for k, dz in enumerate(z_order(nz)):
            lo = max(k * nyc, start)
            hi = min((k + 1) * nyc, start + count)
            if lo < hi:
                yield lo - k * nyc, hi - k * nyc, dz, k * nyc

    own_place = z_order(nz).index(0) * nyc

    def block_of(i, size):
        return pl.ds(pl.multiple_of(i * size, size), size)

    barrier = pltpu.get_barrier_semaphore()
    for dz in z_order(nz):

        @pl.loop(1 if dz == 0 else 0, nyc)
        def _(w):
            pl.semaphore_signal(barrier, inc=1, device_id={"ep": to_of(dz, w)}, device_id_type=MESH)

    for i in range(1, tp):
        pl.semaphore_signal(barrier, inc=1, device_id={"tp": tp_peer(i)}, device_id_type=MESH)

    own_cols = pl.ds(pl.multiple_of(q * dq, 128), dq)
    fetches = [
        pltpu.make_async_copy(src, dst, in_sem.at[n])
        for n, (src, dst) in enumerate(
            [
                (routes_in, routes),
                (weights_in, weights),
                (x_in, x_ref),
                (g_in, g_ref),
                (sg_in, sg_ref),
                (su_in, su_ref),
                (sd_in, sd_ref),
            ]
            + [
                (ref.at[:, own_cols], wq.at[pl.ds(pl.multiple_of(t * ff + q * fo, 16), fo), :])
                for t, ref in enumerate((wg_in, wu_in, wd_in))
            ]
        )
    ]
    for fetch in fetches:
        fetch.start()

    fetches[0].wait()
    turn[...] = jnp.zeros_like(turn)
    turn[0:top, 0:tok] = routes[...]
    by_row = turn[...].T
    fetches[1].wait()
    weight_turn[...] = jnp.zeros_like(weight_turn)
    weight_turn[0:top, 0:tok] = weights[...]
    weight_by_row = weight_turn[...].T
    expert = lax.broadcasted_iota(I32, (32, 128), 1)
    token = lax.broadcasted_iota(I32, (32, 128), 0)
    named = [(by_row[0:32, k : k + 1] == expert) & (token < tok) for k in range(top)]
    count = jnp.zeros((32, 128), I32)
    for k in range(top):
        count = count + named[k].astype(I32)
    before = count
    for shift in (1, 2, 4, 8, 16):
        before = before + jnp.where(token < shift, 0, pltpu.roll(before, shift, 0))
    before = before - count
    weight = jnp.zeros((32, 128), F32)
    for k in range(top):
        weight = weight + jnp.where(named[k], weight_by_row[0:32, k : k + 1], 0.0)
    slot = jnp.zeros((32, 128), I32)
    for k in range(top):
        mine = jnp.sum(jnp.where(named[k], expert * cap + before, 0), axis=1, keepdims=True)
        slot = jnp.where(expert == k, mine, slot)
    slot_table[...] = slot
    for j in range(cap):
        here = (count > 0) & (before == j)
        which = jnp.sum(jnp.where(here, token + 1, 0), axis=0, keepdims=True)
        assign_table[j : j + 1, :] = jnp.where(which > 0, which - 1, tok)
        scale_table[j : j + 1, :] = jnp.sum(jnp.where(here, weight, 0.0), axis=0, keepdims=True)
    tables = [
        pltpu.make_async_copy(assign_table, assign_of, in_sem.at[10]),
        pltpu.make_async_copy(scale_table, scale_of, in_sem.at[11]),
        pltpu.make_async_copy(slot_table, slot_of, in_sem.at[12]),
    ]
    for table in tables:
        table.start()

    fetches[2].wait()
    fetches[3].wait()
    col0 = q * dq
    swap_out = swap_matrix(16, 2 * nb)
    for part_no in range(2):
        lo = part_no * 16
        hi = min(tok, lo + 16)
        pieces = []
        for ref in (x_ref, g_ref):
            for b in range(nb):
                cols = pl.ds(pl.multiple_of(col0 + b * 128, 128), 128)
                piece = ref[lo:hi, cols].astype(F32)
                if hi - lo < 16:
                    piece = jnp.concatenate([piece, jnp.zeros((16 - hi + lo, 128), F32)], axis=0)
                pieces.append(piece)
        stacked = jnp.concatenate(pieces, axis=0).astype(BF16)
        moved = dot_nn(swap_out, stacked)
        tiles[lo : lo + 16] = moved.reshape(16, 2 * nb, 128)

    for table in tables:
        table.wait()
    lower = lax.broadcasted_iota(I32, (2 * nb, 128), 0) < nb

    @pl.loop(0, ep, unroll=4)
    def _(e):
        for j in range(cap):
            tile = tiles[assign_of[j, e]]
            scale = jnp.where(lower, jnp.float32(1.0), scale_of[j, e])
            at = pl.ds(pl.multiple_of((e * cap + j) * 2 * nb, 2 * nb), 2 * nb)
            send_x[at, :] = (tile * scale).astype(BF16)

    pl.semaphore_wait(barrier, ep - 1 + tp - 1)

    def dispatch(group):
        for lo, hi, dz, place in positions(group):

            @pl.loop(max(lo, 1) if dz == 0 else lo, hi)
            def _(w):
                p = to_of(dz, w)
                send(
                    send_x.at[block_of(p, chunk), :],
                    recv_x.at[block_of(place + w, chunk), :],
                    DISPATCH + 2 * group,
                    {"ep": p},
                )

    for t, ref in enumerate((wg_in, wu_in, wd_in)):
        for i in range(1, tp):
            dst_rows = pl.ds(pl.multiple_of(t * ff + q * fo, 16), fo)
            src_cols = pl.ds(pl.multiple_of(tp_peer(i) * dq, 128), dq)
            send(ref.at[:, src_cols], wq.at[dst_rows, :], WEIGHTS, {"tp": tp_peer(i)})
    dispatch(0)
    dispatch(1)
    dispatch(2)
    recv_x[own_place * chunk : (own_place + 1) * chunk, :] = send_x[block_of(me, chunk), :]

    for n in (4, 5, 6):
        fetches[n].wait()
    x = x_ref[...]
    s_gate = dot_nt(x, sg_ref[...])
    s_up = dot_nt(x, su_ref[...])
    s_back = dot_nt(g_ref[...], sd_ref[...])
    s_active, s_slope = swish_parts(s_gate)
    s_hidden = (s_active * s_up).astype(BF16)
    ds_gate = (s_back * s_up * s_slope).astype(BF16)
    ds_up = (s_back * s_active).astype(BF16)
    for j in range(tp):
        cols = slice(j * dq, (j + 1) * dq)
        piece = dot_nn(ds_gate, sg_ref[:, cols]) + dot_nn(ds_up, su_ref[:, cols])
        sdx_send[j] = piece.astype(BF16)
    for i in range(1, tp):
        send(sdx_send.at[tp_peer(i)], sdx_recv.at[q], SHARED_DX, {"tp": tp_peer(i)})

    half = 3 * fo // 2
    for z in range(nz):
        cols = slice(z * ny * cb, (z + 1) * ny * cb)
        xz = x_ref[:, cols]
        whole = jnp.concatenate(
            [dot_tn(ds_gate, xz), dot_tn(ds_up, xz), dot_tn(s_hidden, g_ref[:, cols])], axis=0
        )
        for y in range(ny):
            for h in range(2):
                sh1[h, y, z] = whole[h * half : (h + 1) * half, y * cb : (y + 1) * cb].astype(BF16)
    send(sh1.at[1 - core], sh1_recv, SHARED_1, {"ep": sib})

    waits(sh1_recv, SHARED_1, 1)
    for y in range(ny):
        for z in range(nz):
            both = sh1[core, y, z].astype(F32) + sh1_recv[y, z].astype(F32)
            sh2[y, z] = both.astype(BF16)
    for i in range(1, ny):
        y = lax.rem(yy + i, ny)
        send(sh2.at[y], sh2_recv.at[yy], SHARED_2, {"ep": (zz * ny + y) * 2 + core})

    swap_in = swap_matrix(2 * nb, 16)
    swap_back = swap_matrix(16, nb)

    def arrived(group):
        start, count = groups[group]
        own = 1 if start <= own_place < start + count else 0
        waits(recv_x.at[pl.ds(0, (count - own) * chunk), :], DISPATCH + 2 * group, 1)

    def contract(group):
        base, count = groups[group][0] * cap, groups[group][1] * cap
        for n in range(count // 16):
            lo = base + n * 16
            moved = dot_nn(swap_in, recv_x[lo * 2 * nb : (lo + 16) * 2 * nb, :]).astype(BF16)
            for b in range(2 * nb):
                rows[lo : lo + 16, b * 128 : (b + 1) * 128] = moved[b * 16 : (b + 1) * 16]
        up_part = dot_nt(rows[base : base + count, 0:dq], wq[0 : 2 * ff, :])
        back_part = dot_nt(rows[base : base + count, dq : 2 * dq], wq[2 * ff : 3 * ff, :])
        return up_part, back_part

    def scatter_first():
        up_part, back_part = contract(0)
        for b in range(tp):
            here = slice(b * own_rows, (b + 1) * own_rows)
            part[b, :, 0 : 2 * ff] = up_part[here]
            part[b, :, 2 * ff : 3 * ff] = back_part[here]
            rs_send[b, :, 0 : 2 * ff] = up_part[here].astype(BF16)
            rs_send[b, :, 2 * ff : 3 * ff] = back_part[here].astype(BF16)
        for i in range(1, tp):
            send(rs_send.at[tp_peer(i)], rs_recv.at[q], SCATTER, {"tp": tp_peer(i)})

    def spread_rest(group):
        up_part, back_part = contract(group)
        n = group - 1
        rest[n, :, 0 : 2 * ff] = up_part
        rest[n, :, 2 * ff : 3 * ff] = back_part
        rest_send[n, :, 0 : 2 * ff] = up_part.astype(BF16)
        rest_send[n, :, 2 * ff : 3 * ff] = back_part.astype(BF16)
        for i in range(1, tp):
            send(rest_send.at[n], rest_recv.at[n, q], SCATTER + 2 * group, {"tp": tp_peer(i)})

    def gradients(total):
        gate = total[:, 0:ff]
        up = total[:, ff : 2 * ff]
        back = total[:, 2 * ff : 3 * ff]
        active, slope = swish_parts(gate)
        hidden = (active * up).astype(BF16).astype(F32)
        gp = jnp.sum(hidden * back, axis=1, keepdims=True)
        extra = dfull.shape[1] - 3 * ff
        return jnp.concatenate(
            [back * up * slope, back * active, hidden, jnp.broadcast_to(gp, (gp.shape[0], extra))], axis=1
        )

    def gather_first():
        waits(rs_recv.at[pl.ds(0, tp - 1)], SCATTER, 1)
        total = part[q]
        for i in range(1, tp):
            total = total + rs_recv[tp_peer(i)].astype(F32)
        dall[q] = gradients(total).astype(BF16)
        mine = dall.at[q]
        for i in range(1, tp):
            send(mine, mine, GATHER, {"tp": tp_peer(i)})

    def finish_first():
        waits(dall.at[pl.ds(0, tp - 1)], GATHER, 1)
        for b in range(tp):
            dfull[b * own_rows : (b + 1) * own_rows, :] = dall[b].astype(F32)

    def finish_rest(group):
        n = group - 1
        waits(rest_recv.at[n, pl.ds(0, tp - 1)], SCATTER + 2 * group, 1)
        total = rest[n]
        for i in range(1, tp):
            total = total + rest_recv[n, tp_peer(i)].astype(F32)
        base, count = groups[group][0] * cap, groups[group][1] * cap
        dfull[base : base + count, :] = gradients(total)

    def send_back(group):
        start, places = groups[group]
        base, count = start * cap, places * cap
        d = dfull[base : base + count, :]
        dxr = dot_nn(d[:, 0 : 2 * ff].astype(BF16), wq[0 : 2 * ff, :])
        for n in range(count // 16):
            stacked = jnp.concatenate(
                [dxr[n * 16 : (n + 1) * 16, b * 128 : (b + 1) * 128] for b in range(nb)], axis=0
            ).astype(BF16)
            moved = dot_nn(swap_back, stacked)
            back_send[base + n * 16 : base + (n + 1) * 16] = moved.reshape(16, nb, 128).astype(BF16)
        src_row = lax.broadcasted_iota(I32, (places, count), 0)
        src_col = lax.broadcasted_iota(I32, (places, count), 1)
        collect = (src_col // cap == src_row).astype(F32)
        lane = lax.broadcasted_iota(I32, (count, 128), 1)
        slot_row = lax.broadcasted_iota(I32, (count, 128), 0)
        spread = jnp.where(lane == slot_row % cap, d[:, 3 * ff : 3 * ff + 1], 0.0)
        gp_send[start : start + places] = dot_nn(collect, spread).reshape(places, 1, 128)
        for lo, hi, dz, place in positions(group):
            if dz == 0 and lo == 0:
                back_recv[pl.ds(me * cap, cap)] = back_send[place * cap : (place + 1) * cap]
                gp_recv[me] = gp_send[place]

            @pl.loop(max(lo, 1) if dz == 0 else lo, hi)
            def _(w):
                to = {"ep": from_of(dz, w)}
                send(
                    back_send.at[pl.ds((place + w) * cap, cap)],
                    back_recv.at[pl.ds(me * cap, cap)],
                    BACK,
                    to,
                )
                send(gp_send.at[place + w], gp_recv.at[me], GP, to)

    arrived(0)
    for n in (7, 8, 9):
        fetches[n].wait()
    waits(wq.at[pl.ds(0, 3 * (tp - 1) * fo), :], WEIGHTS, 1)
    scatter_first()
    arrived(1)
    spread_rest(1)
    gather_first()
    arrived(2)
    spread_rest(2)
    if ny > 1:
        waits(sh2_recv.at[pl.ds(0, ny - 1)], SHARED_2, 1)
    for z in range(nz):
        total = sh2[yy, z].astype(F32)
        for i in range(1, ny):
            total = total + sh2_recv[lax.rem(yy + i, ny), z].astype(F32)
        sh3[z] = total.astype(BF16)
    for i in range(1, nz):
        z = lax.rem(zz + i, nz)
        send(sh3.at[z], sh3_recv.at[zz], SHARED_3, {"ep": (z * ny + yy) * 2 + core})
    finish_first()
    send_back(0)
    finish_rest(1)
    send_back(1)
    finish_rest(2)
    d = dfull[...].astype(BF16)
    dw_send[0 : 2 * ff, :] = dot_tn(d[:, 0 : 2 * ff], rows[:, 0:dq]).astype(BF16)
    dw_send[2 * ff : 3 * ff, :] = dot_tn(d[:, 2 * ff : 3 * ff], rows[:, dq : 2 * dq]).astype(BF16)
    own_grads = []
    for t, out in enumerate((gg_out, gu_out, gd_out)):
        for i in range(1, tp):
            src_rows = pl.ds(pl.multiple_of(t * ff + tp_peer(i) * fo, 16), fo)
            send(dw_send.at[src_rows, :], out.at[:, own_cols], GRADS, {"tp": tp_peer(i)})
        mine = pl.ds(pl.multiple_of(t * ff + q * fo, 16), fo)
        own_grads.append(pltpu.make_async_copy(dw_send.at[mine, :], out.at[:, own_cols], in_sem.at[t]))
        own_grads[-1].start()
    send_back(2)

    if nz > 1:
        waits(sh3_recv.at[pl.ds(0, nz - 1)], SHARED_3, 1)
    total = sh3[zz].astype(F32)
    for i in range(1, nz):
        total = total + sh3_recv[lax.rem(zz + i, nz)].astype(F32)
    sh4[...] = total
    send(sh4, sh4_recv, SHARED_4, {"ep": sib})
    waits(sdx_recv.at[pl.ds(0, tp - 1)], SHARED_DX, 1)
    waits(sh4_recv, SHARED_4, 1)
    first = core == 0
    full = jnp.concatenate(
        [
            jnp.where(first, sh4[...], sh4_recv[...]),
            jnp.where(first, sh4_recv[...], sh4[...]),
        ],
        axis=0,
    )
    gs_held[...] = jnp.where(first, full[:, 0 : cb // 2], full[:, cb // 2 : cb])
    own_grads.append(pltpu.make_async_copy(gs_held, gs_out, in_sem.at[3]))
    own_grads[-1].start()

    waits(back_recv.at[pl.ds(0, (ep - 1) * cap)], BACK, 1)
    waits(gp_recv.at[pl.ds(0, ep - 1)], GP, 1)
    row_lane = lax.broadcasted_iota(I32, (1, 128), 1)
    comb[...] = jnp.zeros_like(comb)
    for t in range(tok):
        total = back_recv[slot_of[t, 0]].astype(F32)
        for k in range(1, top):
            total = total + back_recv[slot_of[t, k]].astype(F32)
        comb[t] = total
        s = slot_of[t, q]
        value = jnp.where(row_lane == s % cap, gp_recv[s // cap], 0.0)
        grow[t : t + 1, :] = value
    gr_held[...] = jnp.sum(grow[...].T, axis=0, keepdims=True)[:, 0:tok] / weights[pl.ds(q, 1), :]
    swap_tok = swap_matrix(nb, 16)
    for part_no in range(2):
        lo = part_no * 16
        hi = min(tok, lo + 16)
        v = comb[lo : lo + 16].reshape(16 * nb, 128)
        top_half = v.astype(BF16)
        rest = (v - top_half.astype(F32)).astype(BF16)
        moved = dot_nn(swap_tok, top_half) + dot_nn(swap_tok, rest)
        for b in range(nb):
            cols = slice(b * 128, (b + 1) * 128)
            value = moved[b * 16 : b * 16 + hi - lo]
            value = value + sdx_send[q, lo:hi, cols].astype(F32)
            for i in range(1, tp):
                value = value + sdx_recv[tp_peer(i), lo:hi, cols].astype(F32)
            dx_held[lo:hi, cols] = value.astype(BF16)

    for n, (src, dst) in enumerate(((dx_held, dx_out), (gr_held, gr_out))):
        own_grads.append(pltpu.make_async_copy(src, dst, in_sem.at[4 + n]))
        own_grads[-1].start()
    waits(wq.at[pl.ds(0, 3 * (tp - 1) * fo), :], WEIGHTS, 0)
    for group, (start, count) in enumerate(groups):
        own = 1 if start <= own_place < start + count else 0
        waits(send_x.at[pl.ds(0, (count - own) * chunk), :], DISPATCH + 2 * group, 0)
    waits(sdx_send.at[pl.ds(0, tp - 1)], SHARED_DX, 0)
    waits(sh1_recv, SHARED_1, 0)
    if ny > 1:
        waits(sh2.at[pl.ds(0, ny - 1)], SHARED_2, 0)
    if nz > 1:
        waits(sh3.at[pl.ds(0, nz - 1)], SHARED_3, 0)
    waits(rs_send.at[pl.ds(0, tp - 1)], SCATTER, 0)
    waits(dall.at[pl.ds(0, tp - 1)], GATHER, 0)
    for n in range(2):
        waits(rest_recv.at[n, pl.ds(0, tp - 1)], SCATTER + 2 + 2 * n, 0)
    waits(back_send.at[pl.ds(0, (ep - 1) * cap)], BACK, 0)
    waits(gp_send.at[pl.ds(0, ep - 1)], GP, 0)
    waits(sh4, SHARED_4, 0)
    waits(dw_send.at[pl.ds(0, 3 * (tp - 1) * fo), :], GRADS, 0)
    for copy in own_grads:
        copy.wait()
    waits(dw_send.at[pl.ds(0, 3 * (tp - 1) * fo), :], GRADS, 1)


def finish(fo, dx, gr, gg, gu, gd, gs, dx_o, gr_o, gg_o, gu_o, gd_o, gsg_o, gsu_o, gsd_o, narrow, wide, small, sem):
    width = gg.shape[1]
    parts = 2
    step = width // parts
    loads = []
    for t, src in enumerate((gg, gu, gd)):
        for c in range(parts):
            cols = slice(c * step, (c + 1) * step)
            loads.append(pltpu.make_async_copy(src.at[:, cols], narrow.at[t, :, cols], sem.at[t * parts + c]))
            loads[-1].start()
    last = 6 * parts
    others = [(gs, small[0]), (dx, small[1]), (gr, small[2])]
    ins = [pltpu.make_async_copy(src, dst, sem.at[last + n]) for n, (src, dst) in enumerate(others)]
    for copy in ins:
        copy.start()
    stores = []
    for t, dst in enumerate((gg_o, gu_o, gd_o)):
        for c in range(parts):
            cols = slice(c * step, (c + 1) * step)
            loads[t * parts + c].wait()
            wide[t, :, cols] = narrow[t, :, cols].astype(F32)
            stores.append(pltpu.make_async_copy(wide.at[t, :, cols], dst.at[:, cols], sem.at[(3 + t) * parts + c]))
            stores[-1].start()
    for copy in ins:
        copy.wait()
    outs = [(small[0].at[t * fo : (t + 1) * fo], dst) for t, dst in enumerate((gsg_o, gsu_o, gsd_o))]
    outs += [(small[1], dx_o), (small[2], gr_o)]
    for n, (src, dst) in enumerate(outs):
        stores.append(pltpu.make_async_copy(src, dst, sem.at[last + 3 + n]))
        stores[-1].start()
    for copy in stores:
        copy.wait()


def local(axes, cap, tokens, cotangent, routes, route_weights, expert_gate, expert_up, expert_down, shared_gate, shared_up, shared_down):
    tok, width = tokens.shape
    top = routes.shape[1]
    nz, ny, _ = axes
    ep = lax.axis_size("ep")
    tp = lax.axis_size("tp")
    fo = expert_gate.shape[2]
    ff = fo * tp
    dq = width // tp
    nb = dq // 128
    cb = width // (nz * ny)
    slots = ep * cap
    own_rows = slots // tp // 2
    wide = -(-(3 * ff + 1) // 128) * 128
    half = 3 * fo // 2

    sizes = (ep, tp, nz, ny, cap, tok, top, dq, ff, cb)
    vmem = pl.BlockSpec(memory_space=pltpu.VMEM)
    hbm = pl.BlockSpec(memory_space=pltpu.HBM)
    outs = pl.pallas_call(
        functools.partial(kernel, sizes),
        out_shape=(
            jax.ShapeDtypeStruct((tok, dq), BF16),
            jax.ShapeDtypeStruct((1, tok), F32),
            jax.ShapeDtypeStruct((fo, width), BF16),
            jax.ShapeDtypeStruct((fo, width), BF16),
            jax.ShapeDtypeStruct((fo, width), BF16),
            jax.ShapeDtypeStruct((3 * fo, cb // 2), F32),
        ),
        in_specs=[hbm] * 10,
        out_specs=(hbm,) * 6,
        scratch_shapes=[
            pltpu.VMEM((top, tok), I32),
            pltpu.VMEM((top, tok), F32),
            pltpu.VMEM((8, 128), F32),
            pltpu.VMEM((-(-cap // 8) * 8, 128), I32),
            pltpu.SMEM((-(-cap // 8) * 8, 128), I32),
            pltpu.VMEM((-(-cap // 8) * 8, 128), F32),
            pltpu.SMEM((-(-cap // 8) * 8, 128), F32),
            pltpu.VMEM((32, 128), I32),
            pltpu.SMEM((32, 128), I32),
            pltpu.VMEM((8, 128), I32),
            pltpu.VMEM((tok, width), BF16),
            pltpu.VMEM((tok, width), BF16),
            pltpu.VMEM((fo, width), BF16),
            pltpu.VMEM((fo, width), BF16),
            pltpu.VMEM((fo, width), BF16),
            pltpu.VMEM((32, 2 * nb, 128), F32),
            pltpu.VMEM((slots * 2 * nb, 128), BF16),
            pltpu.VMEM((slots * 2 * nb, 128), BF16),
            pltpu.VMEM((3 * ff, dq), BF16),
            pltpu.VMEM((slots, 2 * dq), BF16),
            pltpu.VMEM((tp, own_rows, 3 * ff), F32),
            pltpu.VMEM((tp, own_rows, 3 * ff), BF16),
            pltpu.VMEM((tp, own_rows, 3 * ff), BF16),
            pltpu.VMEM((2, slots // 4, 3 * ff), F32),
            pltpu.VMEM((2, slots // 4, 3 * ff), BF16),
            pltpu.VMEM((2, tp, slots // 4, 3 * ff), BF16),
            pltpu.VMEM((tp, own_rows, wide), BF16),
            pltpu.VMEM((slots, wide), F32),
            pltpu.VMEM((slots, nb, 128), BF16),
            pltpu.VMEM((slots, nb, 128), BF16),
            pltpu.VMEM((ep, 1, 128), F32),
            pltpu.VMEM((ep, 1, 128), F32),
            pltpu.VMEM((3 * ff, dq), BF16),
            pltpu.VMEM((tp, tok, dq), BF16),
            pltpu.VMEM((tp, tok, dq), BF16),
            pltpu.VMEM((2, ny, nz, half, cb), BF16),
            pltpu.VMEM((ny, nz, half, cb), BF16),
            pltpu.VMEM((ny, nz, half, cb), BF16),
            pltpu.VMEM((ny, nz, half, cb), BF16),
            pltpu.VMEM((nz, half, cb), BF16),
            pltpu.VMEM((nz, half, cb), BF16),
            pltpu.VMEM((half, cb), F32),
            pltpu.VMEM((half, cb), F32),
            pltpu.VMEM((32, nb, 128), F32),
            pltpu.VMEM((32, 128), F32),
            pltpu.VMEM((3 * fo, cb // 2), F32),
            pltpu.VMEM((tok, dq), BF16),
            pltpu.VMEM((1, tok), F32),
            pltpu.SemaphoreType.DMA((72,)),
            pltpu.SemaphoreType.DMA((13,)),
        ],
        compiler_params=pltpu.CompilerParams(
            collective_id=0, has_side_effects=True, vmem_limit_bytes=67043328
        ),
    )(
        routes.T,
        route_weights.T,
        tokens,
        cotangent,
        expert_gate[0].T,
        expert_up[0].T,
        expert_down[0],
        shared_gate.T,
        shared_up.T,
        shared_down,
    )
    dx, gr, gg, gu, gd, gsg, gsu, gsd = pl.pallas_call(
        functools.partial(finish, fo),
        out_shape=(
            jax.ShapeDtypeStruct((tok, dq), BF16),
            jax.ShapeDtypeStruct((1, tok), F32),
            jax.ShapeDtypeStruct((fo, width), F32),
            jax.ShapeDtypeStruct((fo, width), F32),
            jax.ShapeDtypeStruct((fo, width), F32),
            jax.ShapeDtypeStruct((fo, cb // 2), F32),
            jax.ShapeDtypeStruct((fo, cb // 2), F32),
            jax.ShapeDtypeStruct((fo, cb // 2), F32),
        ),
        in_specs=[hbm] * 6,
        out_specs=(hbm,) * 8,
        scratch_shapes=[
            pltpu.VMEM((3, fo, width), BF16),
            pltpu.VMEM((3, fo, width), F32),
            [pltpu.VMEM((3 * fo, cb // 2), F32), pltpu.VMEM((tok, dq), BF16), pltpu.VMEM((1, tok), F32)],
            pltpu.SemaphoreType.DMA((20,)),
        ],
        compiler_params=pltpu.CompilerParams(vmem_limit_bytes=67043328),
    )(*outs)
    return (dx, gr.T, gg.T[None], gu.T[None], gd[None], gsg.T, gsu.T, gsd)


def solution(mesh):
    placed = (
        P("ep", None),
        P("ep", None),
        P("ep", None),
        P("ep", None),
        P("ep", None, "tp"),
        P("ep", None, "tp"),
        P("ep", "tp", None),
        P(None, "tp"),
        P(None, "tp"),
        P("tp", None),
    )
    return jax.shard_map(
        functools.partial(local, EP_AXES, CAP),
        mesh=mesh,
        in_specs=placed,
        out_specs=(
            P("ep", "tp"),
            P("ep", "tp"),
            P("ep", None, "tp"),
            P("ep", None, "tp"),
            P("ep", "tp", None),
            P("ep", "tp"),
            P("ep", "tp"),
            P("tp", "ep"),
        ),
        check_vma=False,
    )
```

```python
import functools

import jax
import jax.numpy as jnp
from jax import lax
from jax.experimental import pallas as pl
from jax.experimental.pallas import tpu as pltpu
from jax.sharding import PartitionSpec as P

MESH = pl.DeviceIdType.MESH
F32 = jnp.float32
BF16 = jnp.bfloat16
I32 = jnp.int32
EP_AXES = (8, 4, 2)
CAP = 3
(WEIGHTS, DISPATCH, SHARED_DX, SHARED_1, SHARED_2, SHARED_3, SHARED_4, SCATTER, GATHER, BACK, GP, GRADS) = range(
    0, 72, 6
)


def dot_nn(a, b):
    return lax.dot_general(a, b, (((1,), (0,)), ((), ())), preferred_element_type=F32)


def dot_nt(a, b):
    return lax.dot_general(a, b, (((1,), (1,)), ((), ())), preferred_element_type=F32)


def dot_tn(a, b):
    return lax.dot_general(a, b, (((0,), (0,)), ((), ())), preferred_element_type=F32)


def wait_bytes(ref, sem):
    pltpu.make_async_copy(ref, ref, sem).wait()


def swish_parts(v):
    sigma = jax.nn.sigmoid(v)
    return v * sigma, sigma * (1.0 + v * (1.0 - sigma))


def swap_matrix(outer, inner):
    size = outer * inner
    row = lax.broadcasted_iota(I32, (size, size), 0)
    col = lax.broadcasted_iota(I32, (size, size), 1)
    return ((row % inner) * outer + row // inner == col).astype(BF16)


def z_order(nz):
    if nz == 8:
        return (3, 5, 1, 7, 4, 0, 2, 6)
    return tuple(range(nz))


def groups_of(ep):
    return ((0, ep // 2), (ep // 2, ep // 4), (ep // 2 + ep // 4, ep // 4))


def kernel(
    sizes,
    routes_in,
    weights_in,
    x_in,
    g_in,
    wg_in,
    wu_in,
    wd_in,
    sg_in,
    su_in,
    sd_in,
    dx_out,
    gr_out,
    gg_out,
    gu_out,
    gd_out,
    gs_out,
    routes,
    weights,
    weight_turn,
    assign_table,
    assign_of,
    scale_table,
    scale_of,
    slot_table,
    slot_of,
    turn,
    x_ref,
    g_ref,
    sg_ref,
    su_ref,
    sd_ref,
    tiles,
    send_x,
    recv_x,
    wq,
    rows,
    part,
    rs_send,
    rs_recv,
    rest,
    rest_send,
    rest_recv,
    dall,
    dfull,
    back_send,
    back_recv,
    gp_send,
    gp_mid,
    gp_recv,
    dw_send,
    sdx_send,
    sdx_recv,
    sh1,
    sh1_recv,
    sh2,
    sh2_recv,
    sh3,
    sh3_recv,
    sh4,
    sh4_recv,
    comb,
    grow,
    gs_held,
    dx_held,
    gr_held,
    sem,
    in_sem,
):
    ep, tp, nz, ny, cap, tok, top, dq, ff, cb = sizes
    nb = dq // 128
    nyc = 2 * ny
    groups = groups_of(ep)
    first_rows = groups[0][1] * cap
    own_rows = first_rows // tp
    fo = ff // tp
    chunk = cap * 2 * nb
    me = lax.axis_index("ep")
    q = lax.axis_index("tp")
    core = lax.rem(me, 2)
    yc = lax.rem(me, nyc)
    yy = yc // 2
    zz = me // nyc
    sib = me + 1 - 2 * core

    def tp_peer(i):
        return lax.rem(q + i, tp)

    def to_of(dz, w):
        return lax.rem(zz + dz, nz) * nyc + lax.rem(yc + w, nyc)

    def from_of(dz, w):
        return lax.rem(zz + nz - dz, nz) * nyc + lax.rem(yc + nyc - w, nyc)

    def send(src, dst, kind, device):
        pltpu.make_async_remote_copy(
            src_ref=src,
            dst_ref=dst,
            send_sem=sem.at[kind],
            recv_sem=sem.at[kind + 1],
            device_id=device,
            device_id_type=MESH,
        ).start()

    def waits(ref, kind, side):
        wait_bytes(ref, sem.at[kind + side])

    def positions(group):
        start, count = groups[group]
        for k, dz in enumerate(z_order(nz)):
            lo = max(k * nyc, start)
            hi = min((k + 1) * nyc, start + count)
            if lo < hi:
                yield lo - k * nyc, hi - k * nyc, dz, k * nyc

    own_place = z_order(nz).index(0) * nyc

    def block_of(i, size):
        return pl.ds(pl.multiple_of(i * size, size), size)

    barrier = pltpu.get_barrier_semaphore()
    for dz in sorted(range(nz), key=lambda dz: -min(dz, nz - dz)):
        for w in range(1 if dz == 0 else 0, nyc):
            pl.semaphore_signal(barrier, inc=1, device_id={"ep": to_of(dz, w)}, device_id_type=MESH)

    for i in range(1, tp):
        pl.semaphore_signal(barrier, inc=1, device_id={"tp": tp_peer(i)}, device_id_type=MESH)

    own_cols = pl.ds(pl.multiple_of(q * dq, 128), dq)
    fetches = [
        pltpu.make_async_copy(src, dst, in_sem.at[n])
        for n, (src, dst) in enumerate(
            [
                (routes_in, routes),
                (weights_in, weights),
                (x_in, x_ref),
                (g_in, g_ref),
                (sg_in, sg_ref),
                (su_in, su_ref),
                (sd_in, sd_ref),
            ]
            + [
                (ref.at[:, own_cols], wq.at[pl.ds(pl.multiple_of(t * ff + q * fo, 16), fo), :])
                for t, ref in enumerate((wg_in, wu_in, wd_in))
            ]
        )
    ]
    for fetch in fetches:
        fetch.start()

    fetches[0].wait()
    turn[...] = jnp.zeros_like(turn)
    turn[0:top, 0:tok] = routes[...]
    by_row = turn[...].T
    fetches[1].wait()
    weight_turn[...] = jnp.zeros_like(weight_turn)
    weight_turn[0:top, 0:tok] = weights[...]
    weight_by_row = weight_turn[...].T
    expert = lax.broadcasted_iota(I32, (32, 128), 1)
    token = lax.broadcasted_iota(I32, (32, 128), 0)
    named = [(by_row[0:32, k : k + 1] == expert) & (token < tok) for k in range(top)]
    count = jnp.zeros((32, 128), I32)
    for k in range(top):
        count = count + named[k].astype(I32)
    before = count
    for shift in (1, 2, 4, 8, 16):
        before = before + jnp.where(token < shift, 0, pltpu.roll(before, shift, 0))
    before = before - count
    weight = jnp.zeros((32, 128), F32)
    for k in range(top):
        weight = weight + jnp.where(named[k], weight_by_row[0:32, k : k + 1], 0.0)
    slot = jnp.zeros((32, 128), I32)
    for k in range(top):
        mine = jnp.sum(jnp.where(named[k], expert * cap + before, 0), axis=1, keepdims=True)
        slot = jnp.where(expert == k, mine, slot)
    slot_table[...] = slot
    for j in range(cap):
        here = (count > 0) & (before == j)
        which = jnp.sum(jnp.where(here, token + 1, 0), axis=0, keepdims=True)
        assign_table[j : j + 1, :] = jnp.where(which > 0, which - 1, tok)
        scale_table[j : j + 1, :] = jnp.sum(jnp.where(here, weight, 0.0), axis=0, keepdims=True)
    tables = [
        pltpu.make_async_copy(assign_table, assign_of, in_sem.at[10]),
        pltpu.make_async_copy(scale_table, scale_of, in_sem.at[11]),
        pltpu.make_async_copy(slot_table, slot_of, in_sem.at[12]),
    ]
    for table in tables:
        table.start()

    fetches[2].wait()
    fetches[3].wait()
    col0 = q * dq
    swap_out = swap_matrix(16, 2 * nb)
    for part_no in range(2):
        lo = part_no * 16
        hi = min(tok, lo + 16)
        pieces = []
        for ref in (x_ref, g_ref):
            for b in range(nb):
                cols = pl.ds(pl.multiple_of(col0 + b * 128, 128), 128)
                piece = ref[lo:hi, cols].astype(F32)
                if hi - lo < 16:
                    piece = jnp.concatenate([piece, jnp.zeros((16 - hi + lo, 128), F32)], axis=0)
                pieces.append(piece)
        stacked = jnp.concatenate(pieces, axis=0).astype(BF16)
        moved = dot_nn(swap_out, stacked)
        tiles[lo : lo + 16] = moved.reshape(16, 2 * nb, 128)

    for table in tables:
        table.wait()
    lower = lax.broadcasted_iota(I32, (2 * nb, 128), 0) < nb

    def pick(group):
        for lo, hi, dz, place in positions(group):

            @pl.loop(lo, hi, unroll=4)
            def _(w):
                p = to_of(dz, w)
                for j in range(cap):
                    tile = tiles[assign_of[j, p]]
                    scale = jnp.where(lower, jnp.float32(1.0), scale_of[j, p])
                    at = pl.ds(pl.multiple_of(((place + w) * cap + j) * 2 * nb, 2 * nb), 2 * nb)
                    send_x[at, :] = (tile * scale).astype(BF16)

    def dispatch(group):
        for lo, hi, dz, place in positions(group):

            @pl.loop(max(lo, 1) if dz == 0 else lo, hi, unroll=4)
            def _(w):
                here = block_of(place + w, chunk)
                send(send_x.at[here, :], recv_x.at[here, :], DISPATCH + 2 * group, {"ep": to_of(dz, w)})

    pick(0)
    pl.semaphore_wait(barrier, ep - 1 + tp - 1)

    for t, ref in enumerate((wg_in, wu_in, wd_in)):
        for i in range(1, tp):
            dst_rows = pl.ds(pl.multiple_of(t * ff + q * fo, 16), fo)
            src_cols = pl.ds(pl.multiple_of(tp_peer(i) * dq, 128), dq)
            send(ref.at[:, src_cols], wq.at[dst_rows, :], WEIGHTS, {"tp": tp_peer(i)})
    dispatch(0)
    pick(1)
    dispatch(1)
    pick(2)
    dispatch(2)
    recv_x[own_place * chunk : (own_place + 1) * chunk, :] = send_x[own_place * chunk : (own_place + 1) * chunk, :]

    for n in (4, 5, 6):
        fetches[n].wait()
    x = x_ref[...]
    s_gate = dot_nt(x, sg_ref[...])
    s_up = dot_nt(x, su_ref[...])
    s_back = dot_nt(g_ref[...], sd_ref[...])
    s_active, s_slope = swish_parts(s_gate)
    s_hidden = (s_active * s_up).astype(BF16)
    ds_gate = (s_back * s_up * s_slope).astype(BF16)
    ds_up = (s_back * s_active).astype(BF16)
    for j in range(tp):
        cols = slice(j * dq, (j + 1) * dq)
        piece = dot_nn(ds_gate, sg_ref[:, cols]) + dot_nn(ds_up, su_ref[:, cols])
        sdx_send[j] = piece.astype(BF16)
    half = 3 * fo // 2
    for z in range(nz):
        cols = slice(z * ny * cb, (z + 1) * ny * cb)
        xz = x_ref[:, cols]
        whole = jnp.concatenate(
            [dot_tn(ds_gate, xz), dot_tn(ds_up, xz), dot_tn(s_hidden, g_ref[:, cols])], axis=0
        )
        for y in range(ny):
            for h in range(2):
                sh1[h, y, z] = whole[h * half : (h + 1) * half, y * cb : (y + 1) * cb].astype(BF16)
    send(sh1.at[1 - core], sh1_recv, SHARED_1, {"ep": sib})

    waits(sh1_recv, SHARED_1, 1)
    for y in range(ny):
        for z in range(nz):
            both = sh1[core, y, z].astype(F32) + sh1_recv[y, z].astype(F32)
            sh2[y, z] = both.astype(BF16)
    for i in range(1, ny):
        y = lax.rem(yy + i, ny)
        send(sh2.at[y], sh2_recv.at[yy], SHARED_2, {"ep": (zz * ny + y) * 2 + core})

    swap_in = swap_matrix(2 * nb, 16)
    swap_back = swap_matrix(16, nb)

    def arrived(group):
        start, count = groups[group]
        own = 1 if start <= own_place < start + count else 0
        waits(recv_x.at[pl.ds(0, (count - own) * chunk), :], DISPATCH + 2 * group, 1)

    def contract(group):
        base, count = groups[group][0] * cap, groups[group][1] * cap
        for n in range(count // 16):
            lo = base + n * 16
            moved = dot_nn(swap_in, recv_x[lo * 2 * nb : (lo + 16) * 2 * nb, :]).astype(BF16)
            for b in range(2 * nb):
                rows[lo : lo + 16, b * 128 : (b + 1) * 128] = moved[b * 16 : (b + 1) * 16]
        up_part = dot_nt(rows[base : base + count, 0:dq], wq[0 : 2 * ff, :])
        back_part = dot_nt(rows[base : base + count, dq : 2 * dq], wq[2 * ff : 3 * ff, :])
        return up_part, back_part

    def scatter_first():
        up_part, back_part = contract(0)
        for b in range(tp):
            here = slice(b * own_rows, (b + 1) * own_rows)
            part[b, :, 0 : 2 * ff] = up_part[here]
            part[b, :, 2 * ff : 3 * ff] = back_part[here]
            rs_send[b, :, 0 : 2 * ff] = up_part[here].astype(BF16)
            rs_send[b, :, 2 * ff : 3 * ff] = back_part[here].astype(BF16)
        for i in range(1, tp):
            send(rs_send.at[tp_peer(i)], rs_recv.at[q], SCATTER, {"tp": tp_peer(i)})

    def spread_rest(group):
        up_part, back_part = contract(group)
        n = group - 1
        rest[n, :, 0 : 2 * ff] = up_part
        rest[n, :, 2 * ff : 3 * ff] = back_part
        rest_send[n, :, 0 : 2 * ff] = up_part.astype(BF16)
        rest_send[n, :, 2 * ff : 3 * ff] = back_part.astype(BF16)
        for i in range(1, tp):
            send(rest_send.at[n], rest_recv.at[n, q], SCATTER + 2 * group, {"tp": tp_peer(i)})

    def gradients(total):
        gate = total[:, 0:ff]
        up = total[:, ff : 2 * ff]
        back = total[:, 2 * ff : 3 * ff]
        active, slope = swish_parts(gate)
        hidden = (active * up).astype(BF16).astype(F32)
        gp = jnp.sum(hidden * back, axis=1, keepdims=True)
        extra = dfull.shape[1] - 3 * ff
        return jnp.concatenate(
            [back * up * slope, back * active, hidden, jnp.broadcast_to(gp, (gp.shape[0], extra))], axis=1
        )

    def gather_first():
        waits(rs_recv.at[pl.ds(0, tp - 1)], SCATTER, 1)
        total = part[q]
        for i in range(1, tp):
            total = total + rs_recv[tp_peer(i)].astype(F32)
        dall[q] = gradients(total).astype(BF16)
        mine = dall.at[q]
        for i in range(1, tp):
            send(mine, mine, GATHER, {"tp": tp_peer(i)})

    def finish_first():
        waits(dall.at[pl.ds(0, tp - 1)], GATHER, 1)
        for b in range(tp):
            dfull[b * own_rows : (b + 1) * own_rows, :] = dall[b].astype(F32)

    def finish_rest(group):
        n = group - 1
        waits(rest_recv.at[n, pl.ds(0, tp - 1)], SCATTER + 2 * group, 1)
        total = rest[n]
        for i in range(1, tp):
            total = total + rest_recv[n, tp_peer(i)].astype(F32)
        base, count = groups[group][0] * cap, groups[group][1] * cap
        dfull[base : base + count, :] = gradients(total)

    def send_back(group):
        start, places = groups[group]
        base, count = start * cap, places * cap
        d = dfull[base : base + count, :]
        dxr = dot_nn(d[:, 0 : 2 * ff].astype(BF16), wq[0 : 2 * ff, :])
        for n in range(count // 16):
            stacked = jnp.concatenate(
                [dxr[n * 16 : (n + 1) * 16, b * 128 : (b + 1) * 128] for b in range(nb)], axis=0
            ).astype(BF16)
            moved = dot_nn(swap_back, stacked)
            back_send[base + n * 16 : base + (n + 1) * 16] = moved.reshape(16, nb, 128).astype(BF16)
        for lo, hi, dz, place in positions(group):
            if dz == 0 and lo == 0:
                back_recv[pl.ds(me * cap, cap)] = back_send[place * cap : (place + 1) * cap]

            @pl.loop(max(lo, 1) if dz == 0 else lo, hi, unroll=4)
            def _(w):
                to = {"ep": from_of(dz, w)}
                send(
                    back_send.at[pl.ds((place + w) * cap, cap)],
                    back_recv.at[pl.ds(me * cap, cap)],
                    BACK,
                    to,
                )

    def send_route_sums(group):
        start, places = groups[group]
        base, count = start * cap, places * cap
        d = dfull[base : base + count, :]
        src_row = lax.broadcasted_iota(I32, (places, count), 0)
        src_col = lax.broadcasted_iota(I32, (places, count), 1)
        collect = (src_col // cap == src_row).astype(F32)
        lane = lax.broadcasted_iota(I32, (count, 128), 1)
        slot_row = lax.broadcasted_iota(I32, (count, 128), 0)
        spread = jnp.where(lane == slot_row % cap, d[:, 3 * ff : 3 * ff + 1], 0.0)
        gp_send[start : start + places] = dot_nn(collect, spread).reshape(places, 1, 128)
        for lo, hi, dz, place in positions(group):
            if dz == 0:
                gp_mid[zz, lo:hi] = gp_send[place + lo : place + hi]
            else:
                send(
                    gp_send.at[pl.ds(place + lo, hi - lo)],
                    gp_mid.at[zz, pl.ds(lo, hi - lo)],
                    GP,
                    {"ep": from_of(dz, 0)},
                )

    def spread_route_sums():
        if nz > 1:
            waits(gp_mid.at[pl.ds(0, nz - 1)], GP, 1)
        for w in range(1, nyc):
            send(gp_mid.at[:, w], gp_recv.at[:, yc], GP + 2, {"ep": from_of(0, w)})
        gp_recv[:, yc] = gp_mid[:, 0]

    arrived(0)
    for n in (7, 8, 9):
        fetches[n].wait()
    waits(wq.at[pl.ds(0, 3 * (tp - 1) * fo), :], WEIGHTS, 1)
    scatter_first()
    gather_first()
    arrived(1)
    spread_rest(1)
    arrived(2)
    spread_rest(2)
    for i in range(1, tp):
        send(sdx_send.at[tp_peer(i)], sdx_recv.at[q], SHARED_DX, {"tp": tp_peer(i)})
    if ny > 1:
        waits(sh2_recv.at[pl.ds(0, ny - 1)], SHARED_2, 1)
    for z in range(nz):
        total = sh2[yy, z].astype(F32)
        for i in range(1, ny):
            total = total + sh2_recv[lax.rem(yy + i, ny), z].astype(F32)
        sh3[z] = total.astype(BF16)
    for i in range(1, nz):
        z = lax.rem(zz + i, nz)
        send(sh3.at[z], sh3_recv.at[zz], SHARED_3, {"ep": (z * ny + yy) * 2 + core})
    finish_first()
    send_back(0)
    send_route_sums(0)
    finish_rest(1)
    finish_rest(2)
    d = dfull[...].astype(BF16)
    dw_send[0 : 2 * ff, :] = dot_tn(d[:, 0 : 2 * ff], rows[:, 0:dq]).astype(BF16)
    dw_send[2 * ff : 3 * ff, :] = dot_tn(d[:, 2 * ff : 3 * ff], rows[:, dq : 2 * dq]).astype(BF16)
    own_grads = []
    for t, out in enumerate((gg_out, gu_out, gd_out)):
        for i in range(1, tp):
            src_rows = pl.ds(pl.multiple_of(t * ff + tp_peer(i) * fo, 16), fo)
            send(dw_send.at[src_rows, :], out.at[:, own_cols], GRADS, {"tp": tp_peer(i)})
        mine = pl.ds(pl.multiple_of(t * ff + q * fo, 16), fo)
        own_grads.append(pltpu.make_async_copy(dw_send.at[mine, :], out.at[:, own_cols], in_sem.at[t]))
        own_grads[-1].start()
    send_route_sums(1)
    send_route_sums(2)
    send_back(1)
    send_back(2)
    spread_route_sums()

    if nz > 1:
        waits(sh3_recv.at[pl.ds(0, nz - 1)], SHARED_3, 1)
    total = sh3[zz].astype(F32)
    for i in range(1, nz):
        total = total + sh3_recv[lax.rem(zz + i, nz)].astype(F32)
    sh4[...] = total
    send(sh4, sh4_recv, SHARED_4, {"ep": sib})
    waits(sdx_recv.at[pl.ds(0, tp - 1)], SHARED_DX, 1)
    waits(sh4_recv, SHARED_4, 1)
    first = core == 0
    full = jnp.concatenate(
        [
            jnp.where(first, sh4[...], sh4_recv[...]),
            jnp.where(first, sh4_recv[...], sh4[...]),
        ],
        axis=0,
    )
    gs_held[...] = jnp.where(first, full[:, 0 : cb // 2], full[:, cb // 2 : cb])
    own_grads.append(pltpu.make_async_copy(gs_held, gs_out, in_sem.at[3]))
    own_grads[-1].start()

    waits(back_recv.at[pl.ds(0, (ep - 1) * cap)], BACK, 1)
    waits(gp_recv.at[:, pl.ds(0, nyc - 1)], GP + 2, 1)
    row_lane = lax.broadcasted_iota(I32, (1, 128), 1)
    comb[...] = jnp.zeros_like(comb)
    for t in range(tok):
        total = back_recv[slot_of[t, 0]].astype(F32)
        for k in range(1, top):
            total = total + back_recv[slot_of[t, k]].astype(F32)
        comb[t] = total
        s = slot_of[t, q]
        value = jnp.where(row_lane == s % cap, gp_recv[s // (cap * nyc), (s // cap) % nyc], 0.0)
        grow[t : t + 1, :] = value
    gr_held[...] = jnp.sum(grow[...].T, axis=0, keepdims=True)[:, 0:tok] / weights[pl.ds(q, 1), :]
    swap_tok = swap_matrix(nb, 16)
    for part_no in range(2):
        lo = part_no * 16
        hi = min(tok, lo + 16)
        v = comb[lo : lo + 16].reshape(16 * nb, 128)
        top_half = v.astype(BF16)
        rest = (v - top_half.astype(F32)).astype(BF16)
        moved = dot_nn(swap_tok, top_half) + dot_nn(swap_tok, rest)
        for b in range(nb):
            cols = slice(b * 128, (b + 1) * 128)
            value = moved[b * 16 : b * 16 + hi - lo]
            value = value + sdx_send[q, lo:hi, cols].astype(F32)
            for i in range(1, tp):
                value = value + sdx_recv[tp_peer(i), lo:hi, cols].astype(F32)
            dx_held[lo:hi, cols] = value.astype(BF16)

    for n, (src, dst) in enumerate(((dx_held, dx_out), (gr_held, gr_out))):
        own_grads.append(pltpu.make_async_copy(src, dst, in_sem.at[4 + n]))
        own_grads[-1].start()
    waits(wq.at[pl.ds(0, 3 * (tp - 1) * fo), :], WEIGHTS, 0)
    for group, (start, count) in enumerate(groups):
        own = 1 if start <= own_place < start + count else 0
        waits(send_x.at[pl.ds(0, (count - own) * chunk), :], DISPATCH + 2 * group, 0)
    waits(sdx_send.at[pl.ds(0, tp - 1)], SHARED_DX, 0)
    waits(sh1_recv, SHARED_1, 0)
    if ny > 1:
        waits(sh2.at[pl.ds(0, ny - 1)], SHARED_2, 0)
    if nz > 1:
        waits(sh3.at[pl.ds(0, nz - 1)], SHARED_3, 0)
    waits(rs_send.at[pl.ds(0, tp - 1)], SCATTER, 0)
    waits(dall.at[pl.ds(0, tp - 1)], GATHER, 0)
    for n in range(2):
        waits(rest_recv.at[n, pl.ds(0, tp - 1)], SCATTER + 2 + 2 * n, 0)
    waits(back_send.at[pl.ds(0, (ep - 1) * cap)], BACK, 0)
    if nz > 1:
        waits(gp_mid.at[pl.ds(0, nz - 1)], GP, 0)
    waits(gp_recv.at[:, pl.ds(0, nyc - 1)], GP + 2, 0)
    waits(sh4, SHARED_4, 0)
    waits(dw_send.at[pl.ds(0, 3 * (tp - 1) * fo), :], GRADS, 0)
    for copy in own_grads:
        copy.wait()
    waits(dw_send.at[pl.ds(0, 3 * (tp - 1) * fo), :], GRADS, 1)


def finish(fo, dx, gr, gg, gu, gd, gs, dx_o, gr_o, gg_o, gu_o, gd_o, gsg_o, gsu_o, gsd_o, narrow, wide, small, sem):
    width = gg.shape[1]
    parts = 2
    step = width // parts
    loads = []
    for t, src in enumerate((gg, gu, gd)):
        for c in range(parts):
            cols = slice(c * step, (c + 1) * step)
            loads.append(pltpu.make_async_copy(src.at[:, cols], narrow.at[t, :, cols], sem.at[t * parts + c]))
            loads[-1].start()
    last = 6 * parts
    others = [(gs, small[0]), (dx, small[1]), (gr, small[2])]
    ins = [pltpu.make_async_copy(src, dst, sem.at[last + n]) for n, (src, dst) in enumerate(others)]
    for copy in ins:
        copy.start()
    stores = []
    for t, dst in enumerate((gg_o, gu_o, gd_o)):
        for c in range(parts):
            cols = slice(c * step, (c + 1) * step)
            loads[t * parts + c].wait()
            wide[t, :, cols] = narrow[t, :, cols].astype(F32)
            stores.append(pltpu.make_async_copy(wide.at[t, :, cols], dst.at[:, cols], sem.at[(3 + t) * parts + c]))
            stores[-1].start()
    for copy in ins:
        copy.wait()
    outs = [(small[0].at[t * fo : (t + 1) * fo], dst) for t, dst in enumerate((gsg_o, gsu_o, gsd_o))]
    outs += [(small[1], dx_o), (small[2], gr_o)]
    for n, (src, dst) in enumerate(outs):
        stores.append(pltpu.make_async_copy(src, dst, sem.at[last + 3 + n]))
        stores[-1].start()
    for copy in stores:
        copy.wait()


def local(axes, cap, tokens, cotangent, routes, route_weights, expert_gate, expert_up, expert_down, shared_gate, shared_up, shared_down):
    tok, width = tokens.shape
    top = routes.shape[1]
    nz, ny, _ = axes
    ep = lax.axis_size("ep")
    tp = lax.axis_size("tp")
    fo = expert_gate.shape[2]
    ff = fo * tp
    dq = width // tp
    nb = dq // 128
    cb = width // (nz * ny)
    slots = ep * cap
    own_rows = slots // tp // 2
    wide = -(-(3 * ff + 1) // 128) * 128
    half = 3 * fo // 2

    sizes = (ep, tp, nz, ny, cap, tok, top, dq, ff, cb)
    vmem = pl.BlockSpec(memory_space=pltpu.VMEM)
    hbm = pl.BlockSpec(memory_space=pltpu.HBM)
    outs = pl.pallas_call(
        functools.partial(kernel, sizes),
        out_shape=(
            jax.ShapeDtypeStruct((tok, dq), BF16),
            jax.ShapeDtypeStruct((1, tok), F32),
            jax.ShapeDtypeStruct((fo, width), BF16),
            jax.ShapeDtypeStruct((fo, width), BF16),
            jax.ShapeDtypeStruct((fo, width), BF16),
            jax.ShapeDtypeStruct((3 * fo, cb // 2), F32),
        ),
        in_specs=[hbm] * 10,
        out_specs=(hbm,) * 6,
        scratch_shapes=[
            pltpu.VMEM((top, tok), I32),
            pltpu.VMEM((top, tok), F32),
            pltpu.VMEM((8, 128), F32),
            pltpu.VMEM((-(-cap // 8) * 8, 128), I32),
            pltpu.SMEM((-(-cap // 8) * 8, 128), I32),
            pltpu.VMEM((-(-cap // 8) * 8, 128), F32),
            pltpu.SMEM((-(-cap // 8) * 8, 128), F32),
            pltpu.VMEM((32, 128), I32),
            pltpu.SMEM((32, 128), I32),
            pltpu.VMEM((8, 128), I32),
            pltpu.VMEM((tok, width), BF16),
            pltpu.VMEM((tok, width), BF16),
            pltpu.VMEM((fo, width), BF16),
            pltpu.VMEM((fo, width), BF16),
            pltpu.VMEM((fo, width), BF16),
            pltpu.VMEM((32, 2 * nb, 128), F32),
            pltpu.VMEM((slots * 2 * nb, 128), BF16),
            pltpu.VMEM((slots * 2 * nb, 128), BF16),
            pltpu.VMEM((3 * ff, dq), BF16),
            pltpu.VMEM((slots, 2 * dq), BF16),
            pltpu.VMEM((tp, own_rows, 3 * ff), F32),
            pltpu.VMEM((tp, own_rows, 3 * ff), BF16),
            pltpu.VMEM((tp, own_rows, 3 * ff), BF16),
            pltpu.VMEM((2, slots // 4, 3 * ff), F32),
            pltpu.VMEM((2, slots // 4, 3 * ff), BF16),
            pltpu.VMEM((2, tp, slots // 4, 3 * ff), BF16),
            pltpu.VMEM((tp, own_rows, wide), BF16),
            pltpu.VMEM((slots, wide), F32),
            pltpu.VMEM((slots, nb, 128), BF16),
            pltpu.VMEM((slots, nb, 128), BF16),
            pltpu.VMEM((ep, 1, 128), F32),
            pltpu.VMEM((nz, 2 * ny, 1, 128), F32),
            pltpu.VMEM((nz, 2 * ny, 1, 128), F32),
            pltpu.VMEM((3 * ff, dq), BF16),
            pltpu.VMEM((tp, tok, dq), BF16),
            pltpu.VMEM((tp, tok, dq), BF16),
            pltpu.VMEM((2, ny, nz, half, cb), BF16),
            pltpu.VMEM((ny, nz, half, cb), BF16),
            pltpu.VMEM((ny, nz, half, cb), BF16),
            pltpu.VMEM((ny, nz, half, cb), BF16),
            pltpu.VMEM((nz, half, cb), BF16),
            pltpu.VMEM((nz, half, cb), BF16),
            pltpu.VMEM((half, cb), F32),
            pltpu.VMEM((half, cb), F32),
            pltpu.VMEM((32, nb, 128), F32),
            pltpu.VMEM((32, 128), F32),
            pltpu.VMEM((3 * fo, cb // 2), F32),
            pltpu.VMEM((tok, dq), BF16),
            pltpu.VMEM((1, tok), F32),
            pltpu.SemaphoreType.DMA((72,)),
            pltpu.SemaphoreType.DMA((13,)),
        ],
        compiler_params=pltpu.CompilerParams(
            collective_id=0, has_side_effects=True, vmem_limit_bytes=67043328
        ),
    )(
        routes.T,
        route_weights.T,
        tokens,
        cotangent,
        expert_gate[0].T,
        expert_up[0].T,
        expert_down[0],
        shared_gate.T,
        shared_up.T,
        shared_down,
    )
    dx, gr, gg, gu, gd, gsg, gsu, gsd = pl.pallas_call(
        functools.partial(finish, fo),
        out_shape=(
            jax.ShapeDtypeStruct((tok, dq), BF16),
            jax.ShapeDtypeStruct((1, tok), F32),
            jax.ShapeDtypeStruct((fo, width), F32),
            jax.ShapeDtypeStruct((fo, width), F32),
            jax.ShapeDtypeStruct((fo, width), F32),
            jax.ShapeDtypeStruct((fo, cb // 2), F32),
            jax.ShapeDtypeStruct((fo, cb // 2), F32),
            jax.ShapeDtypeStruct((fo, cb // 2), F32),
        ),
        in_specs=[hbm] * 6,
        out_specs=(hbm,) * 8,
        scratch_shapes=[
            pltpu.VMEM((3, fo, width), BF16),
            pltpu.VMEM((3, fo, width), F32),
            [pltpu.VMEM((3 * fo, cb // 2), F32), pltpu.VMEM((tok, dq), BF16), pltpu.VMEM((1, tok), F32)],
            pltpu.SemaphoreType.DMA((20,)),
        ],
        compiler_params=pltpu.CompilerParams(vmem_limit_bytes=67043328),
    )(*outs)
    return (dx, gr.T, gg.T[None], gu.T[None], gd[None], gsg.T, gsu.T, gsd)


def solution(mesh):
    placed = (
        P("ep", None),
        P("ep", None),
        P("ep", None),
        P("ep", None),
        P("ep", None, "tp"),
        P("ep", None, "tp"),
        P("ep", "tp", None),
        P(None, "tp"),
        P(None, "tp"),
        P("tp", None),
    )
    return jax.shard_map(
        functools.partial(local, EP_AXES, CAP),
        mesh=mesh,
        in_specs=placed,
        out_specs=(
            P("ep", "tp"),
            P("ep", "tp"),
            P("ep", None, "tp"),
            P("ep", None, "tp"),
            P("ep", "tp", None),
            P("ep", "tp"),
            P("ep", "tp"),
            P("tp", "ep"),
        ),
        check_vma=False,
    )
```

```python
import functools

import jax
import jax.numpy as jnp
from jax import lax
from jax.experimental import pallas as pl
from jax.experimental.pallas import tpu as pltpu
from jax.sharding import PartitionSpec as P

MESH = pl.DeviceIdType.MESH
F32 = jnp.float32
BF16 = jnp.bfloat16
I32 = jnp.int32
EP_AXES = (8, 4, 2)
CAP = 3
(WEIGHTS, SHARED_DX, SHARED_1, SHARED_2, SHARED_3, SHARED_4, GATHER, BACK, GRADS, GP, DISPATCH, SCATTER) = (
    *range(0, 20, 2),
    22,
    28,
)
PAIRS = 17


def dot_nn(a, b):
    return lax.dot_general(a, b, (((1,), (0,)), ((), ())), preferred_element_type=F32)


def dot_nt(a, b):
    return lax.dot_general(a, b, (((1,), (1,)), ((), ())), preferred_element_type=F32)


def dot_tn(a, b):
    return lax.dot_general(a, b, (((0,), (0,)), ((), ())), preferred_element_type=F32)


def wait_bytes(ref, sem):
    pltpu.make_async_copy(ref, ref, sem).wait()


def swish_parts(v):
    sigma = jax.nn.sigmoid(v)
    return v * sigma, sigma * (1.0 + v * (1.0 - sigma))


def swap_matrix(outer, inner):
    size = outer * inner
    row = lax.broadcasted_iota(I32, (size, size), 0)
    col = lax.broadcasted_iota(I32, (size, size), 1)
    return ((row % inner) * outer + row // inner == col).astype(BF16)


def z_order(nz):
    if nz == 8:
        return (1, 7, 0, 2, 6, 3, 5, 4)
    return tuple(range(nz))


def groups_of(ep):
    part = ep // 8
    return ((0, 5 * part), (5 * part, 2 * part), (7 * part, part))


def own_rows_of(first_rows, tp):
    return -(-first_rows // (8 * tp)) * 8


def kernel(
    sizes,
    routes_in,
    weights_in,
    x_in,
    g_in,
    wg_in,
    wu_in,
    wd_in,
    sg_in,
    su_in,
    sd_in,
    dx_out,
    gr_out,
    gg_out,
    gu_out,
    gd_out,
    gs_out,
    routes,
    weights,
    weight_turn,
    assign_table,
    assign_of,
    scale_table,
    scale_of,
    slot_table,
    slot_of,
    turn,
    x_ref,
    g_ref,
    sg_ref,
    su_ref,
    sd_ref,
    staged,
    tiles,
    send_x,
    recv_x,
    wq,
    rows,
    part,
    rs_send,
    rs_recv,
    rest,
    rest_send,
    rest_recv,
    dall,
    dfull,
    back_send,
    back_recv,
    gp_send,
    gp_mid,
    gp_recv,
    dw_send,
    sdx_send,
    sdx_recv,
    sh1,
    sh1_recv,
    sh2,
    sh2_recv,
    sh3,
    sh3_recv,
    sh4,
    sh4_recv,
    comb,
    grow,
    gs_held,
    dx_held,
    gr_held,
    sem,
    in_sem,
):
    ep, tp, nz, ny, cap, tok, top, dq, ff, cb = sizes
    slots = ep * cap
    nb = dq // 128
    nyc = 2 * ny
    groups = groups_of(ep)
    first_rows = groups[0][1] * cap
    own_rows = own_rows_of(first_rows, tp)
    fo = ff // tp
    chunk = cap * 2 * nb
    me = lax.axis_index("ep")
    q = lax.axis_index("tp")
    core = lax.rem(me, 2)
    yc = lax.rem(me, nyc)
    yy = yc // 2
    zz = me // nyc
    sib = me + 1 - 2 * core

    tp_order = sorted(range(1, tp), key=lambda i: -min(i, tp - i))

    def tp_peer(i):
        return lax.rem(q + i, tp)

    def to_of(dz, w):
        return lax.rem(zz + dz, nz) * nyc + lax.rem(yc + w, nyc)

    def from_of(dz, w):
        return lax.rem(zz + nz - dz, nz) * nyc + lax.rem(yc + nyc - w, nyc)

    def send(src, dst, kind, device):
        pltpu.make_async_remote_copy(
            src_ref=src,
            dst_ref=dst,
            send_sem=sem.at[kind],
            recv_sem=sem.at[kind + 1],
            device_id=device,
            device_id_type=MESH,
        ).start()

    def waits(ref, kind, side):
        wait_bytes(ref, sem.at[kind + side])

    def positions(group):
        start, count = groups[group]
        for k, dz in enumerate(z_order(nz)):
            lo = max(k * nyc, start)
            hi = min((k + 1) * nyc, start + count)
            if lo < hi:
                yield lo - k * nyc, hi - k * nyc, dz, k * nyc

    own_place = z_order(nz).index(0) * nyc

    def block_of(i, size):
        return pl.ds(pl.multiple_of(i * size, size), size)

    barrier = pltpu.get_barrier_semaphore()
    for dz in sorted(range(nz), key=lambda dz: -min(dz, nz - dz)):
        for w in range(1 if dz == 0 else 0, nyc):
            pl.semaphore_signal(barrier, inc=1, device_id={"ep": to_of(dz, w)}, device_id_type=MESH)

    for i in range(1, tp):
        pl.semaphore_signal(barrier, inc=1, device_id={"tp": tp_peer(i)}, device_id_type=MESH)

    own_cols = pl.ds(pl.multiple_of(q * dq, 128), dq)
    fetches = [
        pltpu.make_async_copy(src, dst, in_sem.at[n])
        for n, (src, dst) in enumerate(
            [
                (routes_in, routes),
                (weights_in, weights),
                (x_in, x_ref),
                (g_in, g_ref),
                (sg_in, sg_ref),
                (su_in, su_ref),
                (sd_in, sd_ref),
            ]
            + [(ref, staged.at[t]) for t, ref in enumerate((wg_in, wu_in, wd_in))]
        )
    ]
    for fetch in fetches:
        fetch.start()

    fetches[0].wait()
    turn[...] = jnp.zeros_like(turn)
    turn[0:top, 0:tok] = routes[...]
    by_row = turn[...].T
    fetches[1].wait()
    weight_turn[...] = jnp.zeros_like(weight_turn)
    weight_turn[0:top, 0:tok] = weights[...]
    weight_by_row = weight_turn[...].T
    expert = lax.broadcasted_iota(I32, (32, 128), 1)
    token = lax.broadcasted_iota(I32, (32, 128), 0)
    named = [(by_row[0:32, k : k + 1] == expert) & (token < tok) for k in range(top)]
    count = jnp.zeros((32, 128), I32)
    for k in range(top):
        count = count + named[k].astype(I32)
    before = count
    for shift in (1, 2, 4, 8, 16):
        before = before + jnp.where(token < shift, 0, pltpu.roll(before, shift, 0))
    before = before - count
    weight = jnp.zeros((32, 128), F32)
    for k in range(top):
        weight = weight + jnp.where(named[k], weight_by_row[0:32, k : k + 1], 0.0)
    slot = jnp.zeros((32, 128), I32)
    for k in range(top):
        mine = jnp.sum(jnp.where(named[k], expert * cap + before, 0), axis=1, keepdims=True)
        slot = jnp.where(expert == k, mine, slot)
    slot_table[...] = slot
    for j in range(cap):
        here = (count > 0) & (before == j)
        which = jnp.sum(jnp.where(here, token + 1, 0), axis=0, keepdims=True)
        assign_table[j : j + 1, :] = jnp.where(which > 0, which - 1, tok)
        scale_table[j : j + 1, :] = jnp.sum(jnp.where(here, weight, 0.0), axis=0, keepdims=True)
    tables = [
        pltpu.make_async_copy(assign_table, assign_of, in_sem.at[10]),
        pltpu.make_async_copy(scale_table, scale_of, in_sem.at[11]),
        pltpu.make_async_copy(slot_table, slot_of, in_sem.at[12]),
    ]
    for table in tables:
        table.start()

    fetches[2].wait()
    fetches[3].wait()
    col0 = q * dq
    swap_out = swap_matrix(16, 2 * nb)
    for part_no in range(2):
        lo = part_no * 16
        hi = min(tok, lo + 16)
        pieces = []
        for ref in (x_ref, g_ref):
            for b in range(nb):
                cols = pl.ds(pl.multiple_of(col0 + b * 128, 128), 128)
                piece = ref[lo:hi, cols].astype(F32)
                if hi - lo < 16:
                    piece = jnp.concatenate([piece, jnp.zeros((16 - hi + lo, 128), F32)], axis=0)
                pieces.append(piece)
        stacked = jnp.concatenate(pieces, axis=0).astype(BF16)
        moved = dot_nn(swap_out, stacked)
        tiles[lo : lo + 16] = moved.reshape(16, 2 * nb, 128)

    for table in tables:
        table.wait()
    lower = lax.broadcasted_iota(I32, (2 * nb, 128), 0) < nb

    def pick(group):
        for lo, hi, dz, place in positions(group):

            @pl.loop(lo, hi, unroll=4)
            def _(w):
                p = to_of(dz, w)
                for j in range(cap):
                    tile = tiles[assign_of[j, p]]
                    scale = jnp.where(lower, jnp.float32(1.0), scale_of[j, p])
                    at = pl.ds(pl.multiple_of(((place + w) * cap + j) * 2 * nb, 2 * nb), 2 * nb)
                    send_x[at, :] = (tile * scale).astype(BF16)

    def dispatch(group):
        for lo, hi, dz, place in positions(group):

            @pl.loop(max(lo, 1) if dz == 0 else lo, hi, unroll=4)
            def _(w):
                here = block_of(place + w, chunk)
                send(send_x.at[here, :], recv_x.at[here, :], DISPATCH + 2 * group, {"ep": to_of(dz, w)})

    pick(0)
    pl.semaphore_wait(barrier, ep - 1 + tp - 1)

    for n in (7, 8, 9):
        fetches[n].wait()
    for i in tp_order:
        for t in range(3):
            dst_rows = pl.ds(pl.multiple_of(t * ff + q * fo, 16), fo)
            src_cols = pl.ds(pl.multiple_of(tp_peer(i) * dq, 128), dq)
            send(staged.at[t, :, src_cols], wq.at[dst_rows, :], WEIGHTS, {"tp": tp_peer(i)})
    dispatch(0)
    pick(1)
    dispatch(1)
    pick(2)
    dispatch(2)
    recv_x[own_place * chunk : (own_place + 1) * chunk, :] = send_x[own_place * chunk : (own_place + 1) * chunk, :]

    for n in (4, 5, 6):
        fetches[n].wait()
    x = x_ref[...]
    s_gate = dot_nt(x, sg_ref[...])
    s_up = dot_nt(x, su_ref[...])
    s_back = dot_nt(g_ref[...], sd_ref[...])
    s_active, s_slope = swish_parts(s_gate)
    s_hidden = (s_active * s_up).astype(BF16)
    ds_gate = (s_back * s_up * s_slope).astype(BF16)
    ds_up = (s_back * s_active).astype(BF16)
    for j in range(tp):
        cols = slice(j * dq, (j + 1) * dq)
        piece = dot_nn(ds_gate, sg_ref[:, cols]) + dot_nn(ds_up, su_ref[:, cols])
        sdx_send[j] = piece.astype(BF16)
    half = 3 * fo // 2
    for z in range(nz):
        cols = slice(z * ny * cb, (z + 1) * ny * cb)
        xz = x_ref[:, cols]
        whole = jnp.concatenate(
            [dot_tn(ds_gate, xz), dot_tn(ds_up, xz), dot_tn(s_hidden, g_ref[:, cols])], axis=0
        )
        for y in range(ny):
            for h in range(2):
                sh1[h, y, z] = whole[h * half : (h + 1) * half, y * cb : (y + 1) * cb].astype(BF16)
    send(sh1.at[1 - core], sh1_recv, SHARED_1, {"ep": sib})

    waits(sh1_recv, SHARED_1, 1)
    for y in range(ny):
        for z in range(nz):
            both = sh1[core, y, z].astype(F32) + sh1_recv[y, z].astype(F32)
            sh2[y, z] = both.astype(BF16)
    for i in range(1, ny):
        y = lax.rem(yy + i, ny)
        send(sh2.at[y], sh2_recv.at[yy], SHARED_2, {"ep": (zz * ny + y) * 2 + core})

    swap_in = {n: swap_matrix(2 * nb, n) for n in (8, 16)}
    swap_back = {n: swap_matrix(n, nb) for n in (8, 16)}

    def steps_of(base, count):
        lo = base
        while lo < base + count:
            n = 16 if lo % 16 == 0 and lo + 16 <= base + count else 8
            yield lo, n
            lo += n

    def arrived(group):
        start, count = groups[group]
        own = 1 if start <= own_place < start + count else 0
        waits(recv_x.at[pl.ds(0, (count - own) * chunk), :], DISPATCH + 2 * group, 1)

    def contract(group):
        base, count = groups[group][0] * cap, groups[group][1] * cap
        for lo, n in steps_of(base, count):
            moved = dot_nn(swap_in[n], recv_x[lo * 2 * nb : (lo + n) * 2 * nb, :])
            for b in range(2 * nb):
                rows[lo : lo + n, b * 128 : (b + 1) * 128] = moved[b * n : (b + 1) * n].astype(BF16)
        up_part = dot_nt(rows[base : base + count, 0:dq], wq[0 : 2 * ff, :])
        back_part = dot_nt(rows[base : base + count, dq : 2 * dq], wq[2 * ff : 3 * ff, :])
        return up_part, back_part

    def packed_rows(n):
        return n + -(-n // 16) * 8

    def pack(ref, up, back):
        n = up.shape[0]
        half_n = packed_rows(n) - n
        ref[0:n, :] = up.astype(ref.dtype)
        ref[n : n + half_n, 0:ff] = back[0:half_n].astype(ref.dtype)
        ref[n : n + n - half_n, ff : 2 * ff] = back[half_n:n].astype(ref.dtype)

    def unpacked(total, n):
        half_n = packed_rows(n) - n
        back = jnp.concatenate([total[n : n + half_n, 0:ff], total[n : n + n - half_n, ff : 2 * ff]], axis=0)
        return total[0:n, 0:ff], total[0:n, ff : 2 * ff], back

    def scatter_first():
        up_part, back_part = contract(0)
        for b in range(tp):
            lo, hi = b * own_rows, min((b + 1) * own_rows, first_rows)
            up, back = up_part[lo:hi], back_part[lo:hi]
            if hi - lo < own_rows:
                up = jnp.concatenate([up, jnp.zeros((own_rows - hi + lo, 2 * ff), F32)], axis=0)
                back = jnp.concatenate([back, jnp.zeros((own_rows - hi + lo, ff), F32)], axis=0)
            pack(part.at[b], up, back)
            pack(rs_send.at[b], up, back)
        for i in tp_order:
            send(rs_send.at[tp_peer(i)], rs_recv.at[q], SCATTER, {"tp": tp_peer(i)})

    def spread_rest(group):
        up_part, back_part = contract(group)
        n = group - 1
        pack(rest[n], up_part, back_part)
        pack(rest_send[n], up_part, back_part)
        for i in tp_order:
            send(rest_send[n], rest_recv[n].at[q], SCATTER + 2 * group, {"tp": tp_peer(i)})

    def gradients(total, n):
        gate, up, back = unpacked(total, n)
        active, slope = swish_parts(gate)
        hidden = (active * up).astype(BF16).astype(F32)
        gp = jnp.sum(hidden * back, axis=1, keepdims=True)
        extra = dfull.shape[1] - 3 * ff
        return jnp.concatenate(
            [back * up * slope, back * active, hidden, jnp.broadcast_to(gp, (gp.shape[0], extra))], axis=1
        )

    def gather_first():
        waits(rs_recv.at[pl.ds(0, tp - 1)], SCATTER, 1)
        total = part[q]
        for i in range(1, tp):
            total = total + rs_recv[tp_peer(i)].astype(F32)
        dall[q] = gradients(total, own_rows).astype(BF16)
        mine = dall.at[q]
        for i in tp_order:
            send(mine, mine, GATHER, {"tp": tp_peer(i)})

    def finish_first():
        waits(dall.at[pl.ds(0, tp - 1)], GATHER, 1)
        for b in range(tp):
            lo, hi = b * own_rows, min((b + 1) * own_rows, first_rows)
            dfull[lo:hi, :] = dall[b].astype(F32)[0 : hi - lo]

    def finish_rest(group):
        n = group - 1
        waits(rest_recv[n].at[pl.ds(0, tp - 1)], SCATTER + 2 * group, 1)
        total = rest[n][...]
        for i in range(1, tp):
            total = total + rest_recv[n][tp_peer(i)].astype(F32)
        base, count = groups[group][0] * cap, groups[group][1] * cap
        dfull[base : base + count, :] = gradients(total, count)

    def send_back(group):
        start, places = groups[group]
        base, count = start * cap, places * cap
        d = dfull[base : base + count, :]
        dxr = dot_nn(d[:, 0 : 2 * ff].astype(BF16), wq[0 : 2 * ff, :])
        for lo, n in steps_of(0, count):
            stacked = jnp.concatenate(
                [dxr[lo : lo + n, b * 128 : (b + 1) * 128] for b in range(nb)], axis=0
            ).astype(BF16)
            moved = dot_nn(swap_back[n], stacked)
            back_send[base + lo : base + lo + n] = moved.reshape(n, nb, 128).astype(BF16)
        for lo, hi, dz, place in positions(group):
            if dz == 0 and lo == 0:
                back_recv[pl.ds(me * cap, cap)] = back_send[place * cap : (place + 1) * cap]

            @pl.loop(max(lo, 1) if dz == 0 else lo, hi, unroll=4)
            def _(w):
                to = {"ep": from_of(dz, w)}
                send(
                    back_send.at[pl.ds((place + w) * cap, cap)],
                    back_recv.at[pl.ds(me * cap, cap)],
                    BACK,
                    to,
                )

    def send_route_sums(group):
        start, places = groups[group]
        base, count = start * cap, places * cap
        d = dfull[base : base + count, :]
        src_row = lax.broadcasted_iota(I32, (places, count), 0)
        src_col = lax.broadcasted_iota(I32, (places, count), 1)
        collect = (src_col // cap == src_row).astype(F32)
        lane = lax.broadcasted_iota(I32, (count, 128), 1)
        slot_row = lax.broadcasted_iota(I32, (count, 128), 0)
        spread = jnp.where(lane == slot_row % cap, d[:, 3 * ff : 3 * ff + 1], 0.0)
        gp_send[start : start + places] = dot_nn(collect, spread).reshape(places, 1, 128)
        for lo, hi, dz, place in positions(group):
            if dz == 0:
                gp_mid[zz, lo:hi] = gp_send[place + lo : place + hi]
            else:
                send(
                    gp_send.at[pl.ds(place + lo, hi - lo)],
                    gp_mid.at[zz, pl.ds(lo, hi - lo)],
                    GP,
                    {"ep": from_of(dz, 0)},
                )

    def spread_route_sums():
        if nz > 1:
            waits(gp_mid.at[pl.ds(0, nz - 1)], GP, 1)
        for w in range(1, nyc):
            send(gp_mid.at[:, w], gp_recv.at[:, yc], GP + 2, {"ep": from_of(0, w)})
        gp_recv[:, yc] = gp_mid[:, 0]

    arrived(0)
    for t in range(3):
        wq[pl.ds(pl.multiple_of(t * ff + q * fo, 16), fo), :] = staged[t, :, own_cols]
    waits(wq.at[pl.ds(0, 3 * (tp - 1) * fo), :], WEIGHTS, 1)
    scatter_first()
    arrived(1)
    spread_rest(1)
    gather_first()
    arrived(2)
    spread_rest(2)
    for i in tp_order:
        send(sdx_send.at[tp_peer(i)], sdx_recv.at[q], SHARED_DX, {"tp": tp_peer(i)})
    if ny > 1:
        waits(sh2_recv.at[pl.ds(0, ny - 1)], SHARED_2, 1)
    for z in range(nz):
        total = sh2[yy, z].astype(F32)
        for i in range(1, ny):
            total = total + sh2_recv[lax.rem(yy + i, ny), z].astype(F32)
        sh3[z] = total.astype(BF16)
    for i in range(1, nz):
        z = lax.rem(zz + i, nz)
        send(sh3.at[z], sh3_recv.at[zz], SHARED_3, {"ep": (z * ny + yy) * 2 + core})
    finish_rest(1)
    send_route_sums(1)
    send_back(1)
    finish_first()
    finish_rest(2)
    d = dfull[:, 0 : 3 * ff].astype(BF16)
    own_grads = []

    def send_grads(t, out):
        for i in tp_order:
            src_rows = pl.ds(pl.multiple_of(t * ff + tp_peer(i) * fo, 16), fo)
            send(dw_send.at[src_rows, :], out.at[:, own_cols], GRADS, {"tp": tp_peer(i)})
        mine = pl.ds(pl.multiple_of(t * ff + q * fo, 16), fo)
        own_grads.append(pltpu.make_async_copy(dw_send.at[mine, :], out.at[:, own_cols], in_sem.at[t]))
        own_grads[-1].start()

    dw_send[2 * ff : 3 * ff, :] = dot_tn(d[:, 2 * ff : 3 * ff], rows[:, dq : 2 * dq]).astype(BF16)
    send_grads(2, gd_out)
    dw_send[0 : 2 * ff, :] = dot_tn(d[:, 0 : 2 * ff], rows[:, 0:dq]).astype(BF16)
    send_grads(0, gg_out)
    send_grads(1, gu_out)
    send_route_sums(2)
    send_route_sums(0)
    send_back(2)
    send_back(0)
    spread_route_sums()

    if nz > 1:
        waits(sh3_recv.at[pl.ds(0, nz - 1)], SHARED_3, 1)
    total = sh3[zz].astype(F32)
    for i in range(1, nz):
        total = total + sh3_recv[lax.rem(zz + i, nz)].astype(F32)
    sh4[...] = total
    send(sh4, sh4_recv, SHARED_4, {"ep": sib})
    waits(sdx_recv.at[pl.ds(0, tp - 1)], SHARED_DX, 1)
    waits(sh4_recv, SHARED_4, 1)
    first = core == 0
    full = jnp.concatenate(
        [
            jnp.where(first, sh4[...], sh4_recv[...]),
            jnp.where(first, sh4_recv[...], sh4[...]),
        ],
        axis=0,
    )
    gs_held[...] = jnp.where(first, full[:, 0 : cb // 2], full[:, cb // 2 : cb])
    own_grads.append(pltpu.make_async_copy(gs_held, gs_out, in_sem.at[3]))
    own_grads[-1].start()

    waits(back_recv.at[pl.ds(0, (ep - 1) * cap)], BACK, 1)
    waits(gp_recv.at[:, pl.ds(0, nyc - 1)], GP + 2, 1)
    row_lane = lax.broadcasted_iota(I32, (1, 128), 1)
    comb[...] = jnp.zeros_like(comb)
    for t in range(tok):
        total = back_recv[slot_of[t, 0]].astype(F32)
        for k in range(1, top):
            total = total + back_recv[slot_of[t, k]].astype(F32)
        comb[t] = total
        s = slot_of[t, q]
        value = jnp.where(row_lane == s % cap, gp_recv[s // (cap * nyc), (s // cap) % nyc], 0.0)
        grow[t : t + 1, :] = value
    gr_held[...] = jnp.sum(grow[...].T, axis=0, keepdims=True)[:, 0:tok] / weights[pl.ds(q, 1), :]
    swap_tok = swap_matrix(nb, 16)
    for part_no in range(2):
        lo = part_no * 16
        hi = min(tok, lo + 16)
        v = comb[lo : lo + 16].reshape(16 * nb, 128)
        top_half = v.astype(BF16)
        rest = (v - top_half.astype(F32)).astype(BF16)
        moved = dot_nn(swap_tok, top_half) + dot_nn(swap_tok, rest)
        for b in range(nb):
            cols = slice(b * 128, (b + 1) * 128)
            value = moved[b * 16 : b * 16 + hi - lo]
            value = value + sdx_send[q, lo:hi, cols].astype(F32)
            for i in range(1, tp):
                value = value + sdx_recv[tp_peer(i), lo:hi, cols].astype(F32)
            dx_held[lo:hi, cols] = value.astype(BF16)

    for n, (src, dst) in enumerate(((dx_held, dx_out), (gr_held, gr_out))):
        own_grads.append(pltpu.make_async_copy(src, dst, in_sem.at[4 + n]))
        own_grads[-1].start()
    waits(wq.at[pl.ds(0, 3 * (tp - 1) * fo), :], WEIGHTS, 0)
    for group, (start, count) in enumerate(groups):
        own = 1 if start <= own_place < start + count else 0
        waits(send_x.at[pl.ds(0, (count - own) * chunk), :], DISPATCH + 2 * group, 0)
    waits(sdx_send.at[pl.ds(0, tp - 1)], SHARED_DX, 0)
    waits(sh1_recv, SHARED_1, 0)
    if ny > 1:
        waits(sh2.at[pl.ds(0, ny - 1)], SHARED_2, 0)
    if nz > 1:
        waits(sh3.at[pl.ds(0, nz - 1)], SHARED_3, 0)
    waits(rs_send.at[pl.ds(0, tp - 1)], SCATTER, 0)
    waits(dall.at[pl.ds(0, tp - 1)], GATHER, 0)
    for n in range(2):
        waits(rest_recv[n].at[pl.ds(0, tp - 1)], SCATTER + 2 + 2 * n, 0)
    waits(back_send.at[pl.ds(0, (ep - 1) * cap)], BACK, 0)
    if nz > 1:
        waits(gp_mid.at[pl.ds(0, nz - 1)], GP, 0)
    waits(gp_recv.at[:, pl.ds(0, nyc - 1)], GP + 2, 0)
    waits(sh4, SHARED_4, 0)
    waits(dw_send.at[pl.ds(0, 3 * (tp - 1) * fo), :], GRADS, 0)
    for copy in own_grads:
        copy.wait()
    waits(dw_send.at[pl.ds(0, 3 * (tp - 1) * fo), :], GRADS, 1)


def finish(fo, dx, gr, gg, gu, gd, gs, dx_o, gr_o, gg_o, gu_o, gd_o, gsg_o, gsu_o, gsd_o, wide, small, sem):
    width = gg.shape[1]
    parts = 2
    step = width // parts
    last = 6 * parts
    others = [(gs, small[0]), (dx, small[1]), (gr, small[2])]
    ins = [pltpu.make_async_copy(src, dst, sem.at[last + n]) for n, (src, dst) in enumerate(others)]
    for copy in ins:
        copy.start()
    stores = []
    for t, (src, dst) in enumerate(((gg, gg_o), (gu, gu_o), (gd, gd_o))):
        for c in range(parts):
            cols = slice(c * step, (c + 1) * step)
            wide[t, :, cols] = src[:, cols].astype(F32)
            stores.append(pltpu.make_async_copy(wide.at[t, :, cols], dst.at[:, cols], sem.at[(3 + t) * parts + c]))
            stores[-1].start()
    for copy in ins:
        copy.wait()
    outs = [(small[0].at[t * fo : (t + 1) * fo], dst) for t, dst in enumerate((gsg_o, gsu_o, gsd_o))]
    outs += [(small[1], dx_o), (small[2], gr_o)]
    for n, (src, dst) in enumerate(outs):
        stores.append(pltpu.make_async_copy(src, dst, sem.at[last + 3 + n]))
        stores[-1].start()
    for copy in stores:
        copy.wait()


def local(axes, cap, tokens, cotangent, routes, route_weights, expert_gate, expert_up, expert_down, shared_gate, shared_up, shared_down):
    tok, width = tokens.shape
    top = routes.shape[1]
    nz, ny, _ = axes
    ep = lax.axis_size("ep")
    tp = lax.axis_size("tp")
    fo = expert_gate.shape[2]
    ff = fo * tp
    dq = width // tp
    nb = dq // 128
    cb = width // (nz * ny)
    slots = ep * cap
    groups = groups_of(ep)
    own_rows = own_rows_of(groups[0][1] * cap, tp)
    taller = lambda n: n + -(-n // 16) * 8
    rest_rows = [count * cap for _, count in groups[1:]]
    wide = -(-(3 * ff + 1) // 128) * 128
    half = 3 * fo // 2

    sizes = (ep, tp, nz, ny, cap, tok, top, dq, ff, cb)
    vmem = pl.BlockSpec(memory_space=pltpu.VMEM)
    hbm = pl.BlockSpec(memory_space=pltpu.HBM)
    outs = pl.pallas_call(
        functools.partial(kernel, sizes),
        out_shape=(
            jax.ShapeDtypeStruct((tok, dq), BF16),
            jax.ShapeDtypeStruct((1, tok), F32),
            jax.ShapeDtypeStruct((fo, width), BF16),
            jax.ShapeDtypeStruct((fo, width), BF16),
            jax.ShapeDtypeStruct((fo, width), BF16),
            jax.ShapeDtypeStruct((3 * fo, cb // 2), F32),
        ),
        in_specs=[hbm] * 10,
        out_specs=(hbm, hbm, vmem, vmem, vmem, hbm),
        scratch_shapes=[
            pltpu.VMEM((top, tok), I32),
            pltpu.VMEM((top, tok), F32),
            pltpu.VMEM((8, 128), F32),
            pltpu.VMEM((-(-cap // 8) * 8, 128), I32),
            pltpu.SMEM((-(-cap // 8) * 8, 128), I32),
            pltpu.VMEM((-(-cap // 8) * 8, 128), F32),
            pltpu.SMEM((-(-cap // 8) * 8, 128), F32),
            pltpu.VMEM((32, 128), I32),
            pltpu.SMEM((32, 128), I32),
            pltpu.VMEM((8, 128), I32),
            pltpu.VMEM((tok, width), BF16),
            pltpu.VMEM((tok, width), BF16),
            pltpu.VMEM((fo, width), BF16),
            pltpu.VMEM((fo, width), BF16),
            pltpu.VMEM((fo, width), BF16),
            pltpu.VMEM((3, fo, width), BF16),
            pltpu.VMEM((32, 2 * nb, 128), F32),
            pltpu.VMEM((slots * 2 * nb, 128), BF16),
            pltpu.VMEM((slots * 2 * nb, 128), BF16),
            pltpu.VMEM((3 * ff, dq), BF16),
            pltpu.VMEM((slots, 2 * dq), BF16),
            pltpu.VMEM((tp, taller(own_rows), 2 * ff), F32),
            pltpu.VMEM((tp, taller(own_rows), 2 * ff), BF16),
            pltpu.VMEM((tp, taller(own_rows), 2 * ff), BF16),
            [pltpu.VMEM((taller(n), 2 * ff), F32) for n in rest_rows],
            [pltpu.VMEM((taller(n), 2 * ff), BF16) for n in rest_rows],
            [pltpu.VMEM((tp, taller(n), 2 * ff), BF16) for n in rest_rows],
            pltpu.VMEM((tp, own_rows, wide), BF16),
            pltpu.VMEM((slots, wide), F32),
            pltpu.VMEM((slots, nb, 128), BF16),
            pltpu.VMEM((slots, nb, 128), BF16),
            pltpu.VMEM((ep, 1, 128), F32),
            pltpu.VMEM((nz, 2 * ny, 1, 128), F32),
            pltpu.VMEM((nz, 2 * ny, 1, 128), F32),
            pltpu.VMEM((3 * ff, dq), BF16),
            pltpu.VMEM((tp, tok, dq), BF16),
            pltpu.VMEM((tp, tok, dq), BF16),
            pltpu.VMEM((2, ny, nz, half, cb), BF16),
            pltpu.VMEM((ny, nz, half, cb), BF16),
            pltpu.VMEM((ny, nz, half, cb), BF16),
            pltpu.VMEM((ny, nz, half, cb), BF16),
            pltpu.VMEM((nz, half, cb), BF16),
            pltpu.VMEM((nz, half, cb), BF16),
            pltpu.VMEM((half, cb), F32),
            pltpu.VMEM((half, cb), F32),
            pltpu.VMEM((32, nb, 128), F32),
            pltpu.VMEM((32, 128), F32),
            pltpu.VMEM((3 * fo, cb // 2), F32),
            pltpu.VMEM((tok, dq), BF16),
            pltpu.VMEM((1, tok), F32),
            pltpu.SemaphoreType.DMA((2 * PAIRS,)),
            pltpu.SemaphoreType.DMA((13,)),
        ],
        compiler_params=pltpu.CompilerParams(
            collective_id=0, has_side_effects=True, vmem_limit_bytes=50*1024*1024
        ),
    )(
        *[pltpu.with_memory_space_constraint(a, pltpu.HBM) for a in (
        routes.T,
        route_weights.T,
        tokens,
        cotangent,
        expert_gate[0].T,
        expert_up[0].T,
        expert_down[0],
        shared_gate.T,
        shared_up.T,
        shared_down,
        )]
    )
    dx, gr, gg, gu, gd, gsg, gsu, gsd = pl.pallas_call(
        functools.partial(finish, fo),
        out_shape=(
            jax.ShapeDtypeStruct((tok, dq), BF16),
            jax.ShapeDtypeStruct((1, tok), F32),
            jax.ShapeDtypeStruct((fo, width), F32),
            jax.ShapeDtypeStruct((fo, width), F32),
            jax.ShapeDtypeStruct((fo, width), F32),
            jax.ShapeDtypeStruct((fo, cb // 2), F32),
            jax.ShapeDtypeStruct((fo, cb // 2), F32),
            jax.ShapeDtypeStruct((fo, cb // 2), F32),
        ),
        in_specs=[hbm, hbm, vmem, vmem, vmem, hbm],
        out_specs=(hbm,) * 8,
        scratch_shapes=[
            pltpu.VMEM((3, fo, width), F32),
            [pltpu.VMEM((3 * fo, cb // 2), F32), pltpu.VMEM((tok, dq), BF16), pltpu.VMEM((1, tok), F32)],
            pltpu.SemaphoreType.DMA((20,)),
        ],
        compiler_params=pltpu.CompilerParams(vmem_limit_bytes=16*1024*1024),
    )(*outs)
    return (dx, gr.T, gg.T[None], gu.T[None], gd[None], gsg.T, gsu.T, gsd)


def solution(mesh):
    placed = (
        P("ep", None),
        P("ep", None),
        P("ep", None),
        P("ep", None),
        P("ep", None, "tp"),
        P("ep", None, "tp"),
        P("ep", "tp", None),
        P(None, "tp"),
        P(None, "tp"),
        P("tp", None),
    )
    return jax.shard_map(
        functools.partial(local, EP_AXES, CAP),
        mesh=mesh,
        in_specs=placed,
        out_specs=(
            P("ep", "tp"),
            P("ep", "tp"),
            P("ep", None, "tp"),
            P("ep", None, "tp"),
            P("ep", "tp", None),
            P("ep", "tp"),
            P("ep", "tp"),
            P("tp", "ep"),
        ),
        check_vma=False,
    )
```

```python
import functools

import jax
import jax.numpy as jnp
from jax import lax
from jax.experimental import pallas as pl
from jax.experimental.pallas import tpu as pltpu
from jax.sharding import PartitionSpec as P

MESH = pl.DeviceIdType.MESH
F32 = jnp.float32
BF16 = jnp.bfloat16
I32 = jnp.int32
EP_AXES = (8, 4, 2)
CAP = 3
(WEIGHTS, SHARED_DX, SHARED_1, SHARED_2, SHARED_3, SHARED_4, GATHER, BACK, GRADS, GP, DISPATCH, SCATTER) = (
    *range(0, 20, 2),
    22,
    28,
)
DOWN, SCATTER_BACK = 34, 36
PAIRS = 19


def dot_nn(a, b):
    return lax.dot_general(a, b, (((1,), (0,)), ((), ())), preferred_element_type=F32)


def dot_nt(a, b):
    return lax.dot_general(a, b, (((1,), (1,)), ((), ())), preferred_element_type=F32)


def dot_tn(a, b):
    return lax.dot_general(a, b, (((0,), (0,)), ((), ())), preferred_element_type=F32)


def wait_bytes(ref, sem):
    pltpu.make_async_copy(ref, ref, sem).wait()


def swish_parts(v):
    sigma = jax.nn.sigmoid(v)
    return v * sigma, sigma * (1.0 + v * (1.0 - sigma))


def swap_matrix(outer, inner):
    size = outer * inner
    row = lax.broadcasted_iota(I32, (size, size), 0)
    col = lax.broadcasted_iota(I32, (size, size), 1)
    return ((row % inner) * outer + row // inner == col).astype(BF16)


def z_order(nz):
    if nz == 8:
        return (1, 7, 0, 2, 6, 3, 5, 4)
    return tuple(range(nz))


def groups_of(ep):
    part = ep // 8
    return ((0, 5 * part), (5 * part, 2 * part), (7 * part, part))


def own_rows_of(first_rows, tp):
    return -(-first_rows // (8 * tp)) * 8


def kernel(
    sizes,
    routes_in,
    weights_in,
    x_in,
    g_in,
    wg_in,
    wu_in,
    wd_in,
    sg_in,
    su_in,
    sd_in,
    dx_out,
    gr_out,
    gg_out,
    gu_out,
    gd_out,
    gs_out,
    routes,
    weights,
    weight_turn,
    assign_table,
    assign_of,
    scale_table,
    scale_of,
    slot_table,
    slot_of,
    turn,
    x_ref,
    g_ref,
    sg_ref,
    su_ref,
    sd_ref,
    staged,
    tiles,
    send_x,
    recv_x,
    wq,
    rows,
    part,
    rs_send,
    rs_recv,
    rest,
    rest_send,
    rest_recv,
    dall,
    dfull,
    back_send,
    back_recv,
    gp_send,
    gp_mid,
    gp_recv,
    dw_send,
    sdx_send,
    sdx_recv,
    sh1,
    sh1_recv,
    sh2,
    sh2_recv,
    sh3,
    sh3_recv,
    sh4,
    sh4_recv,
    comb,
    grow,
    gs_held,
    dx_held,
    gr_held,
    sem,
    in_sem,
):
    ep, tp, nz, ny, cap, tok, top, dq, ff, cb = sizes
    slots = ep * cap
    nb = dq // 128
    nyc = 2 * ny
    groups = groups_of(ep)
    first_rows = groups[0][1] * cap
    own_rows = own_rows_of(first_rows, tp)
    fo = ff // tp
    chunk = cap * 2 * nb
    me = lax.axis_index("ep")
    q = lax.axis_index("tp")
    core = lax.rem(me, 2)
    yc = lax.rem(me, nyc)
    yy = yc // 2
    zz = me // nyc
    sib = me + 1 - 2 * core

    tp_order = sorted(range(1, tp), key=lambda i: -min(i, tp - i))

    def tp_peer(i):
        return lax.rem(q + i, tp)

    def to_of(dz, w):
        return lax.rem(zz + dz, nz) * nyc + lax.rem(yc + w, nyc)

    def from_of(dz, w):
        return lax.rem(zz + nz - dz, nz) * nyc + lax.rem(yc + nyc - w, nyc)

    def send(src, dst, kind, device):
        pltpu.make_async_remote_copy(
            src_ref=src,
            dst_ref=dst,
            send_sem=sem.at[kind],
            recv_sem=sem.at[kind + 1],
            device_id=device,
            device_id_type=MESH,
        ).start()

    def waits(ref, kind, side):
        wait_bytes(ref, sem.at[kind + side])

    def positions(group):
        start, count = groups[group]
        for k, dz in enumerate(z_order(nz)):
            lo = max(k * nyc, start)
            hi = min((k + 1) * nyc, start + count)
            if lo < hi:
                yield lo - k * nyc, hi - k * nyc, dz, k * nyc

    own_place = z_order(nz).index(0) * nyc

    def block_of(i, size):
        return pl.ds(pl.multiple_of(i * size, size), size)

    barrier = pltpu.get_barrier_semaphore()
    for dz in sorted(range(nz), key=lambda dz: -min(dz, nz - dz)):
        for w in range(1 if dz == 0 else 0, nyc):
            pl.semaphore_signal(barrier, inc=1, device_id={"ep": to_of(dz, w)}, device_id_type=MESH)

    for i in range(1, tp):
        pl.semaphore_signal(barrier, inc=1, device_id={"tp": tp_peer(i)}, device_id_type=MESH)

    own_cols = pl.ds(pl.multiple_of(q * dq, 128), dq)
    fetches = [
        pltpu.make_async_copy(src, dst, in_sem.at[n])
        for n, (src, dst) in enumerate(
            [
                (routes_in, routes),
                (weights_in, weights),
                (x_in, x_ref),
                (g_in, g_ref),
                (sg_in, sg_ref),
                (su_in, su_ref),
                (sd_in, sd_ref),
            ]
            + [(ref, staged.at[t]) for t, ref in enumerate((wg_in, wu_in, wd_in))]
        )
    ]
    for fetch in fetches:
        fetch.start()

    fetches[0].wait()
    turn[...] = jnp.zeros_like(turn)
    turn[0:top, 0:tok] = routes[...]
    by_row = turn[...].T
    fetches[1].wait()
    weight_turn[...] = jnp.zeros_like(weight_turn)
    weight_turn[0:top, 0:tok] = weights[...]
    weight_by_row = weight_turn[...].T
    expert = lax.broadcasted_iota(I32, (32, 128), 1)
    token = lax.broadcasted_iota(I32, (32, 128), 0)
    named = [(by_row[0:32, k : k + 1] == expert) & (token < tok) for k in range(top)]
    count = jnp.zeros((32, 128), I32)
    for k in range(top):
        count = count + named[k].astype(I32)
    before = count
    for shift in (1, 2, 4, 8, 16):
        before = before + jnp.where(token < shift, 0, pltpu.roll(before, shift, 0))
    before = before - count
    weight = jnp.zeros((32, 128), F32)
    for k in range(top):
        weight = weight + jnp.where(named[k], weight_by_row[0:32, k : k + 1], 0.0)
    slot = jnp.zeros((32, 128), I32)
    for k in range(top):
        mine = jnp.sum(jnp.where(named[k], expert * cap + before, 0), axis=1, keepdims=True)
        slot = jnp.where(expert == k, mine, slot)
    slot_table[...] = slot
    for j in range(cap):
        here = (count > 0) & (before == j)
        which = jnp.sum(jnp.where(here, token + 1, 0), axis=0, keepdims=True)
        assign_table[j : j + 1, :] = jnp.where(which > 0, which - 1, tok)
        scale_table[j : j + 1, :] = jnp.sum(jnp.where(here, weight, 0.0), axis=0, keepdims=True)
    tables = [
        pltpu.make_async_copy(assign_table, assign_of, in_sem.at[10]),
        pltpu.make_async_copy(scale_table, scale_of, in_sem.at[11]),
        pltpu.make_async_copy(slot_table, slot_of, in_sem.at[12]),
    ]
    for table in tables:
        table.start()

    fetches[2].wait()
    fetches[3].wait()
    col0 = q * dq
    swap_out = swap_matrix(16, 2 * nb)
    for part_no in range(2):
        lo = part_no * 16
        hi = min(tok, lo + 16)
        pieces = []
        for ref in (x_ref, g_ref):
            for b in range(nb):
                cols = pl.ds(pl.multiple_of(col0 + b * 128, 128), 128)
                piece = ref[lo:hi, cols].astype(F32)
                if hi - lo < 16:
                    piece = jnp.concatenate([piece, jnp.zeros((16 - hi + lo, 128), F32)], axis=0)
                pieces.append(piece)
        stacked = jnp.concatenate(pieces, axis=0).astype(BF16)
        moved = dot_nn(swap_out, stacked)
        tiles[lo : lo + 16] = moved.reshape(16, 2 * nb, 128)

    for table in tables:
        table.wait()
    lower = lax.broadcasted_iota(I32, (2 * nb, 128), 0) < nb

    def pick(group):
        for lo, hi, dz, place in positions(group):

            @pl.loop(lo, hi, unroll=4)
            def _(w):
                p = to_of(dz, w)
                for j in range(cap):
                    tile = tiles[assign_of[j, p]]
                    scale = jnp.where(lower, jnp.float32(1.0), scale_of[j, p])
                    at = pl.ds(pl.multiple_of(((place + w) * cap + j) * 2 * nb, 2 * nb), 2 * nb)
                    send_x[at, :] = (tile * scale).astype(BF16)

    def dispatch(group):
        for lo, hi, dz, place in positions(group):

            @pl.loop(max(lo, 1) if dz == 0 else lo, hi, unroll=4)
            def _(w):
                here = block_of(place + w, chunk)
                send(send_x.at[here, :], recv_x.at[here, :], DISPATCH + 2 * group, {"ep": to_of(dz, w)})

    pick(0)
    pl.semaphore_wait(barrier, ep - 1 + tp - 1)

    for n in (7, 8, 9):
        fetches[n].wait()
    for types, kind in (((0, 1), WEIGHTS), ((2,), DOWN)):
        for i in tp_order:
            for t in types:
                dst_rows = pl.ds(pl.multiple_of(t * ff + q * fo, 16), fo)
                src_cols = pl.ds(pl.multiple_of(tp_peer(i) * dq, 128), dq)
                send(staged.at[t, :, src_cols], wq.at[dst_rows, :], kind, {"tp": tp_peer(i)})
    dispatch(0)
    pick(1)
    dispatch(1)
    pick(2)
    dispatch(2)
    recv_x[own_place * chunk : (own_place + 1) * chunk, :] = send_x[own_place * chunk : (own_place + 1) * chunk, :]

    for n in (4, 5, 6):
        fetches[n].wait()
    x = x_ref[...]
    s_gate = dot_nt(x, sg_ref[...])
    s_up = dot_nt(x, su_ref[...])
    s_back = dot_nt(g_ref[...], sd_ref[...])
    s_active, s_slope = swish_parts(s_gate)
    s_hidden = (s_active * s_up).astype(BF16)
    ds_gate = (s_back * s_up * s_slope).astype(BF16)
    ds_up = (s_back * s_active).astype(BF16)
    for j in range(tp):
        cols = slice(j * dq, (j + 1) * dq)
        piece = dot_nn(ds_gate, sg_ref[:, cols]) + dot_nn(ds_up, su_ref[:, cols])
        sdx_send[j] = piece.astype(BF16)
    half = 3 * fo // 2
    for z in range(nz):
        cols = slice(z * ny * cb, (z + 1) * ny * cb)
        xz = x_ref[:, cols]
        whole = jnp.concatenate(
            [dot_tn(ds_gate, xz), dot_tn(ds_up, xz), dot_tn(s_hidden, g_ref[:, cols])], axis=0
        )
        for y in range(ny):
            for h in range(2):
                sh1[h, y, z] = whole[h * half : (h + 1) * half, y * cb : (y + 1) * cb].astype(BF16)
    send(sh1.at[1 - core], sh1_recv, SHARED_1, {"ep": sib})

    waits(sh1_recv, SHARED_1, 1)
    for y in range(ny):
        for z in range(nz):
            both = sh1[core, y, z].astype(F32) + sh1_recv[y, z].astype(F32)
            sh2[y, z] = both.astype(BF16)
    for i in range(1, ny):
        y = lax.rem(yy + i, ny)
        send(sh2.at[y], sh2_recv.at[yy], SHARED_2, {"ep": (zz * ny + y) * 2 + core})

    swap_in = {n: swap_matrix(2 * nb, n) for n in (8, 16)}
    swap_back = {n: swap_matrix(n, nb) for n in (8, 16)}

    def steps_of(base, count):
        lo = base
        while lo < base + count:
            n = 16 if lo % 16 == 0 and lo + 16 <= base + count else 8
            yield lo, n
            lo += n

    def arrived(group):
        start, count = groups[group]
        own = 1 if start <= own_place < start + count else 0
        waits(recv_x.at[pl.ds(0, (count - own) * chunk), :], DISPATCH + 2 * group, 1)

    def relayout(group):
        base, count = groups[group][0] * cap, groups[group][1] * cap
        for lo, n in steps_of(base, count):
            moved = dot_nn(swap_in[n], recv_x[lo * 2 * nb : (lo + n) * 2 * nb, :])
            for b in range(2 * nb):
                rows[lo : lo + n, b * 128 : (b + 1) * 128] = moved[b * n : (b + 1) * n].astype(BF16)

    def contract(group):
        base, count = groups[group][0] * cap, groups[group][1] * cap
        relayout(group)
        up_part = dot_nt(rows[base : base + count, 0:dq], wq[0 : 2 * ff, :])
        back_part = dot_nt(rows[base : base + count, dq : 2 * dq], wq[2 * ff : 3 * ff, :])
        return up_part, back_part

    def packed_rows(n):
        return n + -(-n // 16) * 8

    def pack(ref, up, back):
        n = up.shape[0]
        half_n = packed_rows(n) - n
        ref[0:n, :] = up.astype(ref.dtype)
        ref[n : n + half_n, 0:ff] = back[0:half_n].astype(ref.dtype)
        ref[n : n + n - half_n, ff : 2 * ff] = back[half_n:n].astype(ref.dtype)

    def unpacked(total, n):
        half_n = packed_rows(n) - n
        back = jnp.concatenate([total[n : n + half_n, 0:ff], total[n : n + n - half_n, ff : 2 * ff]], axis=0)
        return total[0:n, 0:ff], total[0:n, ff : 2 * ff], back

    own_tall = packed_rows(own_rows)

    def blocks_of(whole):
        for b in range(tp):
            lo, hi = b * own_rows, min((b + 1) * own_rows, first_rows)
            block = whole[lo:hi]
            if hi - lo < own_rows:
                block = jnp.concatenate([block, jnp.zeros((own_rows - hi + lo, whole.shape[1]), F32)], axis=0)
            yield b, block

    def scatter_up():
        relayout(0)
        for b, block in blocks_of(dot_nt(rows[0:first_rows, 0:dq], wq[0 : 2 * ff, :])):
            part[b, 0:own_rows, :] = block
            rs_send[b, 0:own_rows, :] = block.astype(BF16)
        here = pl.ds(0, own_rows)
        for i in tp_order:
            send(rs_send.at[tp_peer(i), here], rs_recv.at[q, here], SCATTER, {"tp": tp_peer(i)})

    def scatter_back():
        half_n = own_tall - own_rows
        for b, block in blocks_of(dot_nt(rows[0:first_rows, dq : 2 * dq], wq[2 * ff : 3 * ff, :])):
            for ref in (part, rs_send):
                ref[b, own_rows:own_tall, 0:ff] = block[0:half_n].astype(ref.dtype)
                ref[b, own_rows : 2 * own_rows - half_n, ff : 2 * ff] = block[half_n:own_rows].astype(ref.dtype)
        here = pl.ds(own_rows, half_n)
        for i in tp_order:
            send(rs_send.at[tp_peer(i), here], rs_recv.at[q, here], SCATTER_BACK, {"tp": tp_peer(i)})

    def spread_rest(group):
        up_part, back_part = contract(group)
        n = group - 1
        pack(rest[n], up_part, back_part)
        pack(rest_send[n], up_part, back_part)
        for i in tp_order:
            send(rest_send[n], rest_recv[n].at[q], SCATTER + 2 * group, {"tp": tp_peer(i)})

    def gradients(total, n):
        gate, up, back = unpacked(total, n)
        active, slope = swish_parts(gate)
        hidden = (active * up).astype(BF16).astype(F32)
        gp = jnp.sum(hidden * back, axis=1, keepdims=True)
        extra = dfull.shape[1] - 3 * ff
        return jnp.concatenate(
            [back * up * slope, back * active, hidden, jnp.broadcast_to(gp, (gp.shape[0], extra))], axis=1
        )

    def gather_first():
        waits(rs_recv.at[pl.ds(0, tp - 1), pl.ds(0, own_rows)], SCATTER, 1)
        waits(rs_recv.at[pl.ds(0, tp - 1), pl.ds(own_rows, own_tall - own_rows)], SCATTER_BACK, 1)
        total = part[q]
        for i in range(1, tp):
            total = total + rs_recv[tp_peer(i)].astype(F32)
        dall[q] = gradients(total, own_rows).astype(BF16)
        mine = dall.at[q]
        for i in tp_order:
            send(mine, mine, GATHER, {"tp": tp_peer(i)})

    def finish_first():
        waits(dall.at[pl.ds(0, tp - 1)], GATHER, 1)
        for b in range(tp):
            lo, hi = b * own_rows, min((b + 1) * own_rows, first_rows)
            dfull[lo:hi, :] = dall[b].astype(F32)[0 : hi - lo]

    def finish_rest(group):
        n = group - 1
        waits(rest_recv[n].at[pl.ds(0, tp - 1)], SCATTER + 2 * group, 1)
        total = rest[n][...]
        for i in range(1, tp):
            total = total + rest_recv[n][tp_peer(i)].astype(F32)
        base, count = groups[group][0] * cap, groups[group][1] * cap
        dfull[base : base + count, :] = gradients(total, count)

    def send_back(group):
        start, places = groups[group]
        base, count = start * cap, places * cap
        d = dfull[base : base + count, :]
        dxr = dot_nn(d[:, 0 : 2 * ff].astype(BF16), wq[0 : 2 * ff, :])
        for lo, n in steps_of(0, count):
            stacked = jnp.concatenate(
                [dxr[lo : lo + n, b * 128 : (b + 1) * 128] for b in range(nb)], axis=0
            ).astype(BF16)
            moved = dot_nn(swap_back[n], stacked)
            back_send[base + lo : base + lo + n] = moved.reshape(n, nb, 128).astype(BF16)
        for lo, hi, dz, place in positions(group):
            if dz == 0 and lo == 0:
                back_recv[pl.ds(me * cap, cap)] = back_send[place * cap : (place + 1) * cap]

            @pl.loop(max(lo, 1) if dz == 0 else lo, hi, unroll=4)
            def _(w):
                to = {"ep": from_of(dz, w)}
                send(
                    back_send.at[pl.ds((place + w) * cap, cap)],
                    back_recv.at[pl.ds(me * cap, cap)],
                    BACK,
                    to,
                )

    def send_route_sums(group):
        start, places = groups[group]
        base, count = start * cap, places * cap
        d = dfull[base : base + count, :]
        src_row = lax.broadcasted_iota(I32, (places, count), 0)
        src_col = lax.broadcasted_iota(I32, (places, count), 1)
        collect = (src_col // cap == src_row).astype(F32)
        lane = lax.broadcasted_iota(I32, (count, 128), 1)
        slot_row = lax.broadcasted_iota(I32, (count, 128), 0)
        spread = jnp.where(lane == slot_row % cap, d[:, 3 * ff : 3 * ff + 1], 0.0)
        gp_send[start : start + places] = dot_nn(collect, spread).reshape(places, 1, 128)
        for lo, hi, dz, place in positions(group):
            if dz == 0:
                gp_mid[zz, lo:hi] = gp_send[place + lo : place + hi]
            else:
                send(
                    gp_send.at[pl.ds(place + lo, hi - lo)],
                    gp_mid.at[zz, pl.ds(lo, hi - lo)],
                    GP,
                    {"ep": from_of(dz, 0)},
                )

    def spread_route_sums():
        if nz > 1:
            waits(gp_mid.at[pl.ds(0, nz - 1)], GP, 1)
        for w in range(1, nyc):
            send(gp_mid.at[:, w], gp_recv.at[:, yc], GP + 2, {"ep": from_of(0, w)})
        gp_recv[:, yc] = gp_mid[:, 0]

    for t in range(3):
        wq[pl.ds(pl.multiple_of(t * ff + q * fo, 16), fo), :] = staged[t, :, own_cols]
    waits(wq.at[pl.ds(0, 2 * (tp - 1) * fo), :], WEIGHTS, 1)
    arrived(0)
    scatter_up()
    waits(wq.at[pl.ds(0, (tp - 1) * fo), :], DOWN, 1)
    scatter_back()
    gather_first()
    arrived(1)
    spread_rest(1)
    arrived(2)
    spread_rest(2)
    for i in tp_order:
        send(sdx_send.at[tp_peer(i)], sdx_recv.at[q], SHARED_DX, {"tp": tp_peer(i)})
    if ny > 1:
        waits(sh2_recv.at[pl.ds(0, ny - 1)], SHARED_2, 1)
    for z in range(nz):
        total = sh2[yy, z].astype(F32)
        for i in range(1, ny):
            total = total + sh2_recv[lax.rem(yy + i, ny), z].astype(F32)
        sh3[z] = total.astype(BF16)
    for i in range(1, nz):
        z = lax.rem(zz + i, nz)
        send(sh3.at[z], sh3_recv.at[zz], SHARED_3, {"ep": (z * ny + yy) * 2 + core})
    finish_rest(1)
    send_route_sums(1)
    send_back(1)
    finish_first()
    finish_rest(2)
    d = dfull[:, 0 : 3 * ff].astype(BF16)
    own_grads = []

    def send_grads(t, out):
        for i in tp_order:
            src_rows = pl.ds(pl.multiple_of(t * ff + tp_peer(i) * fo, 16), fo)
            send(dw_send.at[src_rows, :], out.at[:, own_cols], GRADS, {"tp": tp_peer(i)})
        mine = pl.ds(pl.multiple_of(t * ff + q * fo, 16), fo)
        own_grads.append(pltpu.make_async_copy(dw_send.at[mine, :], out.at[:, own_cols], in_sem.at[t]))
        own_grads[-1].start()

    dw_send[2 * ff : 3 * ff, :] = dot_tn(d[:, 2 * ff : 3 * ff], rows[:, dq : 2 * dq]).astype(BF16)
    send_grads(2, gd_out)
    dw_send[0 : 2 * ff, :] = dot_tn(d[:, 0 : 2 * ff], rows[:, 0:dq]).astype(BF16)
    send_grads(0, gg_out)
    send_grads(1, gu_out)
    send_route_sums(2)
    send_route_sums(0)
    send_back(2)
    send_back(0)
    spread_route_sums()

    if nz > 1:
        waits(sh3_recv.at[pl.ds(0, nz - 1)], SHARED_3, 1)
    total = sh3[zz].astype(F32)
    for i in range(1, nz):
        total = total + sh3_recv[lax.rem(zz + i, nz)].astype(F32)
    sh4[...] = total
    send(sh4, sh4_recv, SHARED_4, {"ep": sib})
    waits(sdx_recv.at[pl.ds(0, tp - 1)], SHARED_DX, 1)
    waits(sh4_recv, SHARED_4, 1)
    first = core == 0
    full = jnp.concatenate(
        [
            jnp.where(first, sh4[...], sh4_recv[...]),
            jnp.where(first, sh4_recv[...], sh4[...]),
        ],
        axis=0,
    )
    gs_held[...] = jnp.where(first, full[:, 0 : cb // 2], full[:, cb // 2 : cb])
    own_grads.append(pltpu.make_async_copy(gs_held, gs_out, in_sem.at[3]))
    own_grads[-1].start()

    waits(back_recv.at[pl.ds(0, (ep - 1) * cap)], BACK, 1)
    waits(gp_recv.at[:, pl.ds(0, nyc - 1)], GP + 2, 1)
    row_lane = lax.broadcasted_iota(I32, (1, 128), 1)
    comb[...] = jnp.zeros_like(comb)
    for t in range(tok):
        total = back_recv[slot_of[t, 0]].astype(F32)
        for k in range(1, top):
            total = total + back_recv[slot_of[t, k]].astype(F32)
        comb[t] = total
        s = slot_of[t, q]
        value = jnp.where(row_lane == s % cap, gp_recv[s // (cap * nyc), (s // cap) % nyc], 0.0)
        grow[t : t + 1, :] = value
    gr_held[...] = jnp.sum(grow[...].T, axis=0, keepdims=True)[:, 0:tok] / weights[pl.ds(q, 1), :]
    swap_tok = swap_matrix(nb, 16)
    for part_no in range(2):
        lo = part_no * 16
        hi = min(tok, lo + 16)
        v = comb[lo : lo + 16].reshape(16 * nb, 128)
        top_half = v.astype(BF16)
        rest = (v - top_half.astype(F32)).astype(BF16)
        moved = dot_nn(swap_tok, top_half) + dot_nn(swap_tok, rest)
        for b in range(nb):
            cols = slice(b * 128, (b + 1) * 128)
            value = moved[b * 16 : b * 16 + hi - lo]
            value = value + sdx_send[q, lo:hi, cols].astype(F32)
            for i in range(1, tp):
                value = value + sdx_recv[tp_peer(i), lo:hi, cols].astype(F32)
            dx_held[lo:hi, cols] = value.astype(BF16)

    for n, (src, dst) in enumerate(((dx_held, dx_out), (gr_held, gr_out))):
        own_grads.append(pltpu.make_async_copy(src, dst, in_sem.at[4 + n]))
        own_grads[-1].start()
    waits(wq.at[pl.ds(0, 2 * (tp - 1) * fo), :], WEIGHTS, 0)
    waits(wq.at[pl.ds(0, (tp - 1) * fo), :], DOWN, 0)
    for group, (start, count) in enumerate(groups):
        own = 1 if start <= own_place < start + count else 0
        waits(send_x.at[pl.ds(0, (count - own) * chunk), :], DISPATCH + 2 * group, 0)
    waits(sdx_send.at[pl.ds(0, tp - 1)], SHARED_DX, 0)
    waits(sh1_recv, SHARED_1, 0)
    if ny > 1:
        waits(sh2.at[pl.ds(0, ny - 1)], SHARED_2, 0)
    if nz > 1:
        waits(sh3.at[pl.ds(0, nz - 1)], SHARED_3, 0)
    waits(rs_send.at[pl.ds(0, tp - 1), pl.ds(0, own_rows)], SCATTER, 0)
    waits(rs_send.at[pl.ds(0, tp - 1), pl.ds(own_rows, own_tall - own_rows)], SCATTER_BACK, 0)
    waits(dall.at[pl.ds(0, tp - 1)], GATHER, 0)
    for n in range(2):
        waits(rest_recv[n].at[pl.ds(0, tp - 1)], SCATTER + 2 + 2 * n, 0)
    waits(back_send.at[pl.ds(0, (ep - 1) * cap)], BACK, 0)
    if nz > 1:
        waits(gp_mid.at[pl.ds(0, nz - 1)], GP, 0)
    waits(gp_recv.at[:, pl.ds(0, nyc - 1)], GP + 2, 0)
    waits(sh4, SHARED_4, 0)
    waits(dw_send.at[pl.ds(0, 3 * (tp - 1) * fo), :], GRADS, 0)
    for copy in own_grads:
        copy.wait()
    waits(dw_send.at[pl.ds(0, 3 * (tp - 1) * fo), :], GRADS, 1)


def finish(fo, dx, gr, gg, gu, gd, gs, dx_o, gr_o, gg_o, gu_o, gd_o, gsg_o, gsu_o, gsd_o, wide, small, sem):
    width = gg.shape[1]
    parts = 2
    step = width // parts
    last = 6 * parts
    others = [(gs, small[0]), (dx, small[1]), (gr, small[2])]
    ins = [pltpu.make_async_copy(src, dst, sem.at[last + n]) for n, (src, dst) in enumerate(others)]
    for copy in ins:
        copy.start()
    stores = []
    for t, (src, dst) in enumerate(((gg, gg_o), (gu, gu_o), (gd, gd_o))):
        for c in range(parts):
            cols = slice(c * step, (c + 1) * step)
            wide[t, :, cols] = src[:, cols].astype(F32)
            stores.append(pltpu.make_async_copy(wide.at[t, :, cols], dst.at[:, cols], sem.at[(3 + t) * parts + c]))
            stores[-1].start()
    for copy in ins:
        copy.wait()
    outs = [(small[0].at[t * fo : (t + 1) * fo], dst) for t, dst in enumerate((gsg_o, gsu_o, gsd_o))]
    outs += [(small[1], dx_o), (small[2], gr_o)]
    for n, (src, dst) in enumerate(outs):
        stores.append(pltpu.make_async_copy(src, dst, sem.at[last + 3 + n]))
        stores[-1].start()
    for copy in stores:
        copy.wait()


def local(axes, cap, tokens, cotangent, routes, route_weights, expert_gate, expert_up, expert_down, shared_gate, shared_up, shared_down):
    tok, width = tokens.shape
    top = routes.shape[1]
    nz, ny, _ = axes
    ep = lax.axis_size("ep")
    tp = lax.axis_size("tp")
    fo = expert_gate.shape[2]
    ff = fo * tp
    dq = width // tp
    nb = dq // 128
    cb = width // (nz * ny)
    slots = ep * cap
    groups = groups_of(ep)
    own_rows = own_rows_of(groups[0][1] * cap, tp)
    taller = lambda n: n + -(-n // 16) * 8
    rest_rows = [count * cap for _, count in groups[1:]]
    wide = -(-(3 * ff + 1) // 128) * 128
    half = 3 * fo // 2

    sizes = (ep, tp, nz, ny, cap, tok, top, dq, ff, cb)
    vmem = pl.BlockSpec(memory_space=pltpu.VMEM)
    hbm = pl.BlockSpec(memory_space=pltpu.HBM)
    outs = pl.pallas_call(
        functools.partial(kernel, sizes),
        out_shape=(
            jax.ShapeDtypeStruct((tok, dq), BF16),
            jax.ShapeDtypeStruct((1, tok), F32),
            jax.ShapeDtypeStruct((fo, width), BF16),
            jax.ShapeDtypeStruct((fo, width), BF16),
            jax.ShapeDtypeStruct((fo, width), BF16),
            jax.ShapeDtypeStruct((3 * fo, cb // 2), F32),
        ),
        in_specs=[hbm] * 10,
        out_specs=(hbm, hbm, vmem, vmem, vmem, hbm),
        scratch_shapes=[
            pltpu.VMEM((top, tok), I32),
            pltpu.VMEM((top, tok), F32),
            pltpu.VMEM((8, 128), F32),
            pltpu.VMEM((-(-cap // 8) * 8, 128), I32),
            pltpu.SMEM((-(-cap // 8) * 8, 128), I32),
            pltpu.VMEM((-(-cap // 8) * 8, 128), F32),
            pltpu.SMEM((-(-cap // 8) * 8, 128), F32),
            pltpu.VMEM((32, 128), I32),
            pltpu.SMEM((32, 128), I32),
            pltpu.VMEM((8, 128), I32),
            pltpu.VMEM((tok, width), BF16),
            pltpu.VMEM((tok, width), BF16),
            pltpu.VMEM((fo, width), BF16),
            pltpu.VMEM((fo, width), BF16),
            pltpu.VMEM((fo, width), BF16),
            pltpu.VMEM((3, fo, width), BF16),
            pltpu.VMEM((32, 2 * nb, 128), F32),
            pltpu.VMEM((slots * 2 * nb, 128), BF16),
            pltpu.VMEM((slots * 2 * nb, 128), BF16),
            pltpu.VMEM((3 * ff, dq), BF16),
            pltpu.VMEM((slots, 2 * dq), BF16),
            pltpu.VMEM((tp, taller(own_rows), 2 * ff), F32),
            pltpu.VMEM((tp, taller(own_rows), 2 * ff), BF16),
            pltpu.VMEM((tp, taller(own_rows), 2 * ff), BF16),
            [pltpu.VMEM((taller(n), 2 * ff), F32) for n in rest_rows],
            [pltpu.VMEM((taller(n), 2 * ff), BF16) for n in rest_rows],
            [pltpu.VMEM((tp, taller(n), 2 * ff), BF16) for n in rest_rows],
            pltpu.VMEM((tp, own_rows, wide), BF16),
            pltpu.VMEM((slots, wide), F32),
            pltpu.VMEM((slots, nb, 128), BF16),
            pltpu.VMEM((slots, nb, 128), BF16),
            pltpu.VMEM((ep, 1, 128), F32),
            pltpu.VMEM((nz, 2 * ny, 1, 128), F32),
            pltpu.VMEM((nz, 2 * ny, 1, 128), F32),
            pltpu.VMEM((3 * ff, dq), BF16),
            pltpu.VMEM((tp, tok, dq), BF16),
            pltpu.VMEM((tp, tok, dq), BF16),
            pltpu.VMEM((2, ny, nz, half, cb), BF16),
            pltpu.VMEM((ny, nz, half, cb), BF16),
            pltpu.VMEM((ny, nz, half, cb), BF16),
            pltpu.VMEM((ny, nz, half, cb), BF16),
            pltpu.VMEM((nz, half, cb), BF16),
            pltpu.VMEM((nz, half, cb), BF16),
            pltpu.VMEM((half, cb), F32),
            pltpu.VMEM((half, cb), F32),
            pltpu.VMEM((32, nb, 128), F32),
            pltpu.VMEM((32, 128), F32),
            pltpu.VMEM((3 * fo, cb // 2), F32),
            pltpu.VMEM((tok, dq), BF16),
            pltpu.VMEM((1, tok), F32),
            pltpu.SemaphoreType.DMA((2 * PAIRS,)),
            pltpu.SemaphoreType.DMA((13,)),
        ],
        compiler_params=pltpu.CompilerParams(
            collective_id=0, has_side_effects=True, vmem_limit_bytes=50*1024*1024
        ),
    )(
        *[pltpu.with_memory_space_constraint(a, pltpu.HBM) for a in (
        routes.T,
        route_weights.T,
        tokens,
        cotangent,
        expert_gate[0].T,
        expert_up[0].T,
        expert_down[0],
        shared_gate.T,
        shared_up.T,
        shared_down,
        )]
    )
    dx, gr, gg, gu, gd, gsg, gsu, gsd = pl.pallas_call(
        functools.partial(finish, fo),
        out_shape=(
            jax.ShapeDtypeStruct((tok, dq), BF16),
            jax.ShapeDtypeStruct((1, tok), F32),
            jax.ShapeDtypeStruct((fo, width), F32),
            jax.ShapeDtypeStruct((fo, width), F32),
            jax.ShapeDtypeStruct((fo, width), F32),
            jax.ShapeDtypeStruct((fo, cb // 2), F32),
            jax.ShapeDtypeStruct((fo, cb // 2), F32),
            jax.ShapeDtypeStruct((fo, cb // 2), F32),
        ),
        in_specs=[hbm, hbm, vmem, vmem, vmem, hbm],
        out_specs=(hbm,) * 8,
        scratch_shapes=[
            pltpu.VMEM((3, fo, width), F32),
            [pltpu.VMEM((3 * fo, cb // 2), F32), pltpu.VMEM((tok, dq), BF16), pltpu.VMEM((1, tok), F32)],
            pltpu.SemaphoreType.DMA((20,)),
        ],
        compiler_params=pltpu.CompilerParams(vmem_limit_bytes=16*1024*1024),
    )(*outs)
    return (dx, gr.T, gg.T[None], gu.T[None], gd[None], gsg.T, gsu.T, gsd)


def solution(mesh):
    placed = (
        P("ep", None),
        P("ep", None),
        P("ep", None),
        P("ep", None),
        P("ep", None, "tp"),
        P("ep", None, "tp"),
        P("ep", "tp", None),
        P(None, "tp"),
        P(None, "tp"),
        P("tp", None),
    )
    return jax.shard_map(
        functools.partial(local, EP_AXES, CAP),
        mesh=mesh,
        in_specs=placed,
        out_specs=(
            P("ep", "tp"),
            P("ep", "tp"),
            P("ep", None, "tp"),
            P("ep", None, "tp"),
            P("ep", "tp", None),
            P("ep", "tp"),
            P("ep", "tp"),
            P("tp", "ep"),
        ),
        check_vma=False,
    )
```

```python
import functools

import jax
import jax.numpy as jnp
from jax import lax
from jax.experimental import pallas as pl
from jax.experimental.pallas import tpu as pltpu
from jax.sharding import PartitionSpec as P

MESH = pl.DeviceIdType.MESH
F32 = jnp.float32
BF16 = jnp.bfloat16
I32 = jnp.int32
EP_AXES = (8, 4, 2)
CAP = 3
(WEIGHTS, SHARED_DX, SHARED_1, SHARED_2, SHARED_3, SHARED_4, GATHER, BACK, GRADS, GP, DISPATCH, SCATTER) = (
    *range(0, 20, 2),
    22,
    28,
)
DOWN, SCATTER_BACK = 34, 36
PAIRS = 19


def dot_nn(a, b):
    return lax.dot_general(a, b, (((1,), (0,)), ((), ())), preferred_element_type=F32)


def dot_nt(a, b):
    return lax.dot_general(a, b, (((1,), (1,)), ((), ())), preferred_element_type=F32)


def dot_tn(a, b):
    return lax.dot_general(a, b, (((0,), (0,)), ((), ())), preferred_element_type=F32)


def wait_bytes(ref, sem):
    pltpu.make_async_copy(ref, ref, sem).wait()


def swish_parts(v):
    sigma = jax.nn.sigmoid(v)
    return v * sigma, sigma * (1.0 + v * (1.0 - sigma))


def swap_matrix(outer, inner):
    size = outer * inner
    row = lax.broadcasted_iota(I32, (size, size), 0)
    col = lax.broadcasted_iota(I32, (size, size), 1)
    return ((row % inner) * outer + row // inner == col).astype(BF16)


def z_order(nz):
    if nz == 8:
        return (1, 7, 0, 2, 6, 3, 5, 4)
    return tuple(range(nz))


def groups_of(ep):
    part = ep // 8
    return ((0, 5 * part), (5 * part, 2 * part), (7 * part, part))


def own_rows_of(first_rows, tp):
    return -(-first_rows // (8 * tp)) * 8


def kernel(
    sizes,
    routes_in,
    weights_in,
    x_in,
    g_in,
    wg_in,
    wu_in,
    wd_in,
    sg_in,
    su_in,
    sd_in,
    dx_out,
    gr_out,
    gg_out,
    gu_out,
    gd_out,
    gs_out,
    routes,
    weights,
    weight_turn,
    assign_table,
    assign_of,
    scale_table,
    scale_of,
    slot_table,
    slot_of,
    turn,
    x_ref,
    g_ref,
    sg_ref,
    su_ref,
    sd_ref,
    staged,
    tiles,
    send_x,
    recv_x,
    wq,
    rows,
    part,
    rs_send,
    rs_recv,
    rest,
    rest_send,
    rest_recv,
    dall,
    dfull,
    back_send,
    back_recv,
    gp_send,
    gp_mid,
    gp_recv,
    dw_send,
    sdx_send,
    sdx_recv,
    sh1,
    sh1_recv,
    sh2,
    sh2_recv,
    sh3,
    sh3_recv,
    sh4,
    sh4_recv,
    comb,
    grow,
    gs_held,
    dx_held,
    gr_held,
    sem,
    in_sem,
):
    ep, tp, nz, ny, cap, tok, top, dq, ff, cb = sizes
    slots = ep * cap
    nb = dq // 128
    nyc = 2 * ny
    groups = groups_of(ep)
    first_rows = groups[0][1] * cap
    own_rows = own_rows_of(first_rows, tp)
    fo = ff // tp
    chunk = cap * 2 * nb
    me = lax.axis_index("ep")
    q = lax.axis_index("tp")
    core = lax.rem(me, 2)
    yc = lax.rem(me, nyc)
    yy = yc // 2
    zz = me // nyc
    sib = me + 1 - 2 * core

    tp_order = sorted(range(1, tp), key=lambda i: -min(i, tp - i))

    def tp_peer(i):
        return lax.rem(q + i, tp)

    def to_of(dz, w):
        return lax.rem(zz + dz, nz) * nyc + lax.rem(yc + w, nyc)

    def from_of(dz, w):
        return lax.rem(zz + nz - dz, nz) * nyc + lax.rem(yc + nyc - w, nyc)

    def send(src, dst, kind, device):
        pltpu.make_async_remote_copy(
            src_ref=src,
            dst_ref=dst,
            send_sem=sem.at[kind],
            recv_sem=sem.at[kind + 1],
            device_id=device,
            device_id_type=MESH,
        ).start()

    def waits(ref, kind, side):
        wait_bytes(ref, sem.at[kind + side])

    def positions(group):
        start, count = groups[group]
        for k, dz in enumerate(z_order(nz)):
            lo = max(k * nyc, start)
            hi = min((k + 1) * nyc, start + count)
            if lo < hi:
                yield lo - k * nyc, hi - k * nyc, dz, k * nyc

    own_place = z_order(nz).index(0) * nyc

    def block_of(i, size):
        return pl.ds(pl.multiple_of(i * size, size), size)

    barrier = pltpu.get_barrier_semaphore()
    for dz in sorted(range(nz), key=lambda dz: -min(dz, nz - dz)):
        for w in range(1 if dz == 0 else 0, nyc):
            pl.semaphore_signal(barrier, inc=1, device_id={"ep": to_of(dz, w)}, device_id_type=MESH)

    for i in range(1, tp):
        pl.semaphore_signal(barrier, inc=1, device_id={"tp": tp_peer(i)}, device_id_type=MESH)

    own_cols = pl.ds(pl.multiple_of(q * dq, 128), dq)
    fetches = [
        pltpu.make_async_copy(src, dst, in_sem.at[n])
        for n, (src, dst) in enumerate(
            [
                (routes_in, routes),
                (weights_in, weights),
                (x_in, x_ref),
                (g_in, g_ref),
                (sg_in, sg_ref),
                (su_in, su_ref),
                (sd_in, sd_ref),
            ]
            + [(ref, staged.at[t]) for t, ref in enumerate((wg_in, wu_in, wd_in))]
        )
    ]
    for fetch in fetches:
        fetch.start()

    fetches[0].wait()
    turn[...] = jnp.zeros_like(turn)
    turn[0:top, 0:tok] = routes[...]
    by_row = turn[...].T
    fetches[1].wait()
    weight_turn[...] = jnp.zeros_like(weight_turn)
    weight_turn[0:top, 0:tok] = weights[...]
    weight_by_row = weight_turn[...].T
    expert = lax.broadcasted_iota(I32, (32, 128), 1)
    token = lax.broadcasted_iota(I32, (32, 128), 0)
    named = [(by_row[0:32, k : k + 1] == expert) & (token < tok) for k in range(top)]
    count = jnp.zeros((32, 128), I32)
    for k in range(top):
        count = count + named[k].astype(I32)
    before = count
    for shift in (1, 2, 4, 8, 16):
        before = before + jnp.where(token < shift, 0, pltpu.roll(before, shift, 0))
    before = before - count
    weight = jnp.zeros((32, 128), F32)
    for k in range(top):
        weight = weight + jnp.where(named[k], weight_by_row[0:32, k : k + 1], 0.0)
    slot = jnp.zeros((32, 128), I32)
    for k in range(top):
        mine = jnp.sum(jnp.where(named[k], expert * cap + before, 0), axis=1, keepdims=True)
        slot = jnp.where(expert == k, mine, slot)
    slot_table[...] = slot
    for j in range(cap):
        here = (count > 0) & (before == j)
        which = jnp.sum(jnp.where(here, token + 1, 0), axis=0, keepdims=True)
        assign_table[j : j + 1, :] = jnp.where(which > 0, which - 1, tok)
        scale_table[j : j + 1, :] = jnp.sum(jnp.where(here, weight, 0.0), axis=0, keepdims=True)
    tables = [
        pltpu.make_async_copy(assign_table, assign_of, in_sem.at[10]),
        pltpu.make_async_copy(scale_table, scale_of, in_sem.at[11]),
        pltpu.make_async_copy(slot_table, slot_of, in_sem.at[12]),
    ]
    for table in tables:
        table.start()

    fetches[2].wait()
    fetches[3].wait()
    col0 = q * dq
    swap_out = swap_matrix(16, 2 * nb)
    for part_no in range(2):
        lo = part_no * 16
        hi = min(tok, lo + 16)
        pieces = []
        for ref in (x_ref, g_ref):
            for b in range(nb):
                cols = pl.ds(pl.multiple_of(col0 + b * 128, 128), 128)
                piece = ref[lo:hi, cols].astype(F32)
                if hi - lo < 16:
                    piece = jnp.concatenate([piece, jnp.zeros((16 - hi + lo, 128), F32)], axis=0)
                pieces.append(piece)
        stacked = jnp.concatenate(pieces, axis=0).astype(BF16)
        moved = dot_nn(swap_out, stacked)
        tiles[lo : lo + 16] = moved.reshape(16, 2 * nb, 128)

    for table in tables:
        table.wait()
    lower = lax.broadcasted_iota(I32, (2 * nb, 128), 0) < nb

    def pick(group):
        for lo, hi, dz, place in positions(group):

            @pl.loop(lo, hi, unroll=4)
            def _(w):
                p = to_of(dz, w)
                for j in range(cap):
                    tile = tiles[assign_of[j, p]]
                    scale = jnp.where(lower, jnp.float32(1.0), scale_of[j, p])
                    at = pl.ds(pl.multiple_of(((place + w) * cap + j) * 2 * nb, 2 * nb), 2 * nb)
                    send_x[at, :] = (tile * scale).astype(BF16)

    def dispatch(group):
        for lo, hi, dz, place in positions(group):

            @pl.loop(max(lo, 1) if dz == 0 else lo, hi, unroll=4)
            def _(w):
                here = block_of(place + w, chunk)
                send(send_x.at[here, :], recv_x.at[here, :], DISPATCH + 2 * group, {"ep": to_of(dz, w)})

    pick(0)
    pl.semaphore_wait(barrier, ep - 1 + tp - 1)

    dispatch(0)
    for n in (7, 8, 9):
        fetches[n].wait()
    for types, kind in (((0, 1), WEIGHTS), ((2,), DOWN)):
        for i in tp_order:
            for t in types:
                dst_rows = pl.ds(pl.multiple_of(t * ff + q * fo, 16), fo)
                src_cols = pl.ds(pl.multiple_of(tp_peer(i) * dq, 128), dq)
                send(staged.at[t, :, src_cols], wq.at[dst_rows, :], kind, {"tp": tp_peer(i)})
    pick(1)
    dispatch(1)
    pick(2)
    dispatch(2)
    recv_x[own_place * chunk : (own_place + 1) * chunk, :] = send_x[own_place * chunk : (own_place + 1) * chunk, :]

    for n in (4, 5, 6):
        fetches[n].wait()
    x = x_ref[...]
    s_gate = dot_nt(x, sg_ref[...])
    s_up = dot_nt(x, su_ref[...])
    s_back = dot_nt(g_ref[...], sd_ref[...])
    s_active, s_slope = swish_parts(s_gate)
    s_hidden = (s_active * s_up).astype(BF16)
    ds_gate = (s_back * s_up * s_slope).astype(BF16)
    ds_up = (s_back * s_active).astype(BF16)
    for j in range(tp):
        cols = slice(j * dq, (j + 1) * dq)
        piece = dot_nn(ds_gate, sg_ref[:, cols]) + dot_nn(ds_up, su_ref[:, cols])
        sdx_send[j] = piece.astype(BF16)
    half = 3 * fo // 2
    for z in range(nz):
        cols = slice(z * ny * cb, (z + 1) * ny * cb)
        xz = x_ref[:, cols]
        whole = jnp.concatenate(
            [dot_tn(ds_gate, xz), dot_tn(ds_up, xz), dot_tn(s_hidden, g_ref[:, cols])], axis=0
        )
        for y in range(ny):
            for h in range(2):
                sh1[h, y, z] = whole[h * half : (h + 1) * half, y * cb : (y + 1) * cb].astype(BF16)
    send(sh1.at[1 - core], sh1_recv, SHARED_1, {"ep": sib})

    waits(sh1_recv, SHARED_1, 1)
    for y in range(ny):
        for z in range(nz):
            both = sh1[core, y, z].astype(F32) + sh1_recv[y, z].astype(F32)
            sh2[y, z] = both.astype(BF16)
    for i in range(1, ny):
        y = lax.rem(yy + i, ny)
        send(sh2.at[y], sh2_recv.at[yy], SHARED_2, {"ep": (zz * ny + y) * 2 + core})

    swap_in = {n: swap_matrix(2 * nb, n) for n in (8, 16)}
    swap_back = {n: swap_matrix(n, nb) for n in (8, 16)}

    def steps_of(base, count):
        lo = base
        while lo < base + count:
            n = 16 if lo % 16 == 0 and lo + 16 <= base + count else 8
            yield lo, n
            lo += n

    def arrived(group):
        start, count = groups[group]
        own = 1 if start <= own_place < start + count else 0
        waits(recv_x.at[pl.ds(0, (count - own) * chunk), :], DISPATCH + 2 * group, 1)

    def relayout(group):
        base, count = groups[group][0] * cap, groups[group][1] * cap
        for lo, n in steps_of(base, count):
            moved = dot_nn(swap_in[n], recv_x[lo * 2 * nb : (lo + n) * 2 * nb, :])
            for b in range(2 * nb):
                rows[lo : lo + n, b * 128 : (b + 1) * 128] = moved[b * n : (b + 1) * n].astype(BF16)

    def contract(group):
        base, count = groups[group][0] * cap, groups[group][1] * cap
        relayout(group)
        up_part = dot_nt(rows[base : base + count, 0:dq], wq[0 : 2 * ff, :])
        back_part = dot_nt(rows[base : base + count, dq : 2 * dq], wq[2 * ff : 3 * ff, :])
        return up_part, back_part

    def packed_rows(n):
        return n + -(-n // 16) * 8

    def pack(ref, up, back):
        n = up.shape[0]
        half_n = packed_rows(n) - n
        ref[0:n, :] = up.astype(ref.dtype)
        ref[n : n + half_n, 0:ff] = back[0:half_n].astype(ref.dtype)
        ref[n : n + n - half_n, ff : 2 * ff] = back[half_n:n].astype(ref.dtype)

    def unpacked(total, n):
        half_n = packed_rows(n) - n
        back = jnp.concatenate([total[n : n + half_n, 0:ff], total[n : n + n - half_n, ff : 2 * ff]], axis=0)
        return total[0:n, 0:ff], total[0:n, ff : 2 * ff], back

    own_tall = packed_rows(own_rows)

    def blocks_of(whole):
        for b in range(tp):
            lo, hi = b * own_rows, min((b + 1) * own_rows, first_rows)
            block = whole[lo:hi]
            if hi - lo < own_rows:
                block = jnp.concatenate([block, jnp.zeros((own_rows - hi + lo, whole.shape[1]), F32)], axis=0)
            yield b, block

    def scatter_up():
        relayout(0)
        for b, block in blocks_of(dot_nt(rows[0:first_rows, 0:dq], wq[0 : 2 * ff, :])):
            part[b, 0:own_rows, :] = block
            rs_send[b, 0:own_rows, :] = block.astype(BF16)
        here = pl.ds(0, own_rows)
        for i in tp_order:
            send(rs_send.at[tp_peer(i), here], rs_recv.at[q, here], SCATTER, {"tp": tp_peer(i)})

    def scatter_back():
        half_n = own_tall - own_rows
        for b, block in blocks_of(dot_nt(rows[0:first_rows, dq : 2 * dq], wq[2 * ff : 3 * ff, :])):
            for ref in (part, rs_send):
                ref[b, own_rows:own_tall, 0:ff] = block[0:half_n].astype(ref.dtype)
                ref[b, own_rows : 2 * own_rows - half_n, ff : 2 * ff] = block[half_n:own_rows].astype(ref.dtype)
        here = pl.ds(own_rows, half_n)
        for i in tp_order:
            send(rs_send.at[tp_peer(i), here], rs_recv.at[q, here], SCATTER_BACK, {"tp": tp_peer(i)})

    def spread_rest(group):
        up_part, back_part = contract(group)
        n = group - 1
        pack(rest[n], up_part, back_part)
        pack(rest_send[n], up_part, back_part)
        for i in tp_order:
            send(rest_send[n], rest_recv[n].at[q], SCATTER + 2 * group, {"tp": tp_peer(i)})

    def gradients(total, n):
        gate, up, back = unpacked(total, n)
        active, slope = swish_parts(gate)
        hidden = (active * up).astype(BF16).astype(F32)
        gp = jnp.sum(hidden * back, axis=1, keepdims=True)
        extra = dfull.shape[1] - 3 * ff
        return jnp.concatenate(
            [back * up * slope, back * active, hidden, jnp.broadcast_to(gp, (gp.shape[0], extra))], axis=1
        )

    def gather_first():
        waits(rs_recv.at[pl.ds(0, tp - 1), pl.ds(0, own_rows)], SCATTER, 1)
        waits(rs_recv.at[pl.ds(0, tp - 1), pl.ds(own_rows, own_tall - own_rows)], SCATTER_BACK, 1)
        total = part[q]
        for i in range(1, tp):
            total = total + rs_recv[tp_peer(i)].astype(F32)
        dall[q] = gradients(total, own_rows).astype(BF16)
        mine = dall.at[q]
        for i in tp_order:
            send(mine, mine, GATHER, {"tp": tp_peer(i)})

    def finish_first():
        waits(dall.at[pl.ds(0, tp - 1)], GATHER, 1)
        for b in range(tp):
            lo, hi = b * own_rows, min((b + 1) * own_rows, first_rows)
            dfull[lo:hi, :] = dall[b].astype(F32)[0 : hi - lo]

    def finish_rest(group):
        n = group - 1
        waits(rest_recv[n].at[pl.ds(0, tp - 1)], SCATTER + 2 * group, 1)
        total = rest[n][...]
        for i in range(1, tp):
            total = total + rest_recv[n][tp_peer(i)].astype(F32)
        base, count = groups[group][0] * cap, groups[group][1] * cap
        dfull[base : base + count, :] = gradients(total, count)

    def send_back(group):
        start, places = groups[group]
        base, count = start * cap, places * cap
        d = dfull[base : base + count, :]
        dxr = dot_nn(d[:, 0 : 2 * ff].astype(BF16), wq[0 : 2 * ff, :])
        for lo, n in steps_of(0, count):
            stacked = jnp.concatenate(
                [dxr[lo : lo + n, b * 128 : (b + 1) * 128] for b in range(nb)], axis=0
            ).astype(BF16)
            moved = dot_nn(swap_back[n], stacked)
            back_send[base + lo : base + lo + n] = moved.reshape(n, nb, 128).astype(BF16)
        for lo, hi, dz, place in positions(group):
            if dz == 0 and lo == 0:
                back_recv[pl.ds(me * cap, cap)] = back_send[place * cap : (place + 1) * cap]

            @pl.loop(max(lo, 1) if dz == 0 else lo, hi, unroll=4)
            def _(w):
                to = {"ep": from_of(dz, w)}
                send(
                    back_send.at[pl.ds((place + w) * cap, cap)],
                    back_recv.at[pl.ds(me * cap, cap)],
                    BACK,
                    to,
                )

    def send_route_sums(group):
        start, places = groups[group]
        base, count = start * cap, places * cap
        d = dfull[base : base + count, :]
        src_row = lax.broadcasted_iota(I32, (places, count), 0)
        src_col = lax.broadcasted_iota(I32, (places, count), 1)
        collect = (src_col // cap == src_row).astype(F32)
        lane = lax.broadcasted_iota(I32, (count, 128), 1)
        slot_row = lax.broadcasted_iota(I32, (count, 128), 0)
        spread = jnp.where(lane == slot_row % cap, d[:, 3 * ff : 3 * ff + 1], 0.0)
        gp_send[start : start + places] = dot_nn(collect, spread).reshape(places, 1, 128)
        for lo, hi, dz, place in positions(group):
            if dz == 0:
                gp_mid[zz, lo:hi] = gp_send[place + lo : place + hi]
            else:
                send(
                    gp_send.at[pl.ds(place + lo, hi - lo)],
                    gp_mid.at[zz, pl.ds(lo, hi - lo)],
                    GP,
                    {"ep": from_of(dz, 0)},
                )

    def spread_route_sums():
        if nz > 1:
            waits(gp_mid.at[pl.ds(0, nz - 1)], GP, 1)
        for w in range(1, nyc):
            send(gp_mid.at[:, w], gp_recv.at[:, yc], GP + 2, {"ep": from_of(0, w)})
        gp_recv[:, yc] = gp_mid[:, 0]

    for t in range(3):
        wq[pl.ds(pl.multiple_of(t * ff + q * fo, 16), fo), :] = staged[t, :, own_cols]
    waits(wq.at[pl.ds(0, 2 * (tp - 1) * fo), :], WEIGHTS, 1)
    arrived(0)
    scatter_up()
    waits(wq.at[pl.ds(0, (tp - 1) * fo), :], DOWN, 1)
    scatter_back()
    gather_first()
    arrived(1)
    spread_rest(1)
    arrived(2)
    spread_rest(2)
    for i in tp_order:
        send(sdx_send.at[tp_peer(i)], sdx_recv.at[q], SHARED_DX, {"tp": tp_peer(i)})
    if ny > 1:
        waits(sh2_recv.at[pl.ds(0, ny - 1)], SHARED_2, 1)
    for z in range(nz):
        total = sh2[yy, z].astype(F32)
        for i in range(1, ny):
            total = total + sh2_recv[lax.rem(yy + i, ny), z].astype(F32)
        sh3[z] = total.astype(BF16)
    for i in range(1, nz):
        z = lax.rem(zz + i, nz)
        send(sh3.at[z], sh3_recv.at[zz], SHARED_3, {"ep": (z * ny + yy) * 2 + core})
    finish_rest(1)
    send_route_sums(1)
    send_back(1)
    finish_first()
    finish_rest(2)
    d = dfull[:, 0 : 3 * ff].astype(BF16)
    own_grads = []

    def send_grads(t, out):
        for i in tp_order:
            src_rows = pl.ds(pl.multiple_of(t * ff + tp_peer(i) * fo, 16), fo)
            send(dw_send.at[src_rows, :], out.at[:, own_cols], GRADS, {"tp": tp_peer(i)})
        mine = pl.ds(pl.multiple_of(t * ff + q * fo, 16), fo)
        own_grads.append(pltpu.make_async_copy(dw_send.at[mine, :], out.at[:, own_cols], in_sem.at[t]))
        own_grads[-1].start()

    dw_send[2 * ff : 3 * ff, :] = dot_tn(d[:, 2 * ff : 3 * ff], rows[:, dq : 2 * dq]).astype(BF16)
    send_grads(2, gd_out)
    dw_send[0 : 2 * ff, :] = dot_tn(d[:, 0 : 2 * ff], rows[:, 0:dq]).astype(BF16)
    send_grads(0, gg_out)
    send_grads(1, gu_out)
    send_route_sums(2)
    send_route_sums(0)
    send_back(2)
    send_back(0)
    spread_route_sums()

    if nz > 1:
        waits(sh3_recv.at[pl.ds(0, nz - 1)], SHARED_3, 1)
    total = sh3[zz].astype(F32)
    for i in range(1, nz):
        total = total + sh3_recv[lax.rem(zz + i, nz)].astype(F32)
    sh4[...] = total
    send(sh4, sh4_recv, SHARED_4, {"ep": sib})
    waits(sdx_recv.at[pl.ds(0, tp - 1)], SHARED_DX, 1)
    waits(sh4_recv, SHARED_4, 1)
    first = core == 0
    full = jnp.concatenate(
        [
            jnp.where(first, sh4[...], sh4_recv[...]),
            jnp.where(first, sh4_recv[...], sh4[...]),
        ],
        axis=0,
    )
    gs_held[...] = jnp.where(first, full[:, 0 : cb // 2], full[:, cb // 2 : cb])
    own_grads.append(pltpu.make_async_copy(gs_held, gs_out, in_sem.at[3]))
    own_grads[-1].start()

    waits(back_recv.at[pl.ds(0, (ep - 1) * cap)], BACK, 1)
    waits(gp_recv.at[:, pl.ds(0, nyc - 1)], GP + 2, 1)
    row_lane = lax.broadcasted_iota(I32, (1, 128), 1)
    comb[...] = jnp.zeros_like(comb)
    for t in range(tok):
        total = back_recv[slot_of[t, 0]].astype(F32)
        for k in range(1, top):
            total = total + back_recv[slot_of[t, k]].astype(F32)
        comb[t] = total
        s = slot_of[t, q]
        value = jnp.where(row_lane == s % cap, gp_recv[s // (cap * nyc), (s // cap) % nyc], 0.0)
        grow[t : t + 1, :] = value
    gr_held[...] = jnp.sum(grow[...].T, axis=0, keepdims=True)[:, 0:tok] / weights[pl.ds(q, 1), :]
    swap_tok = swap_matrix(nb, 16)
    for part_no in range(2):
        lo = part_no * 16
        hi = min(tok, lo + 16)
        v = comb[lo : lo + 16].reshape(16 * nb, 128)
        top_half = v.astype(BF16)
        rest = (v - top_half.astype(F32)).astype(BF16)
        moved = dot_nn(swap_tok, top_half) + dot_nn(swap_tok, rest)
        for b in range(nb):
            cols = slice(b * 128, (b + 1) * 128)
            value = moved[b * 16 : b * 16 + hi - lo]
            value = value + sdx_send[q, lo:hi, cols].astype(F32)
            for i in range(1, tp):
                value = value + sdx_recv[tp_peer(i), lo:hi, cols].astype(F32)
            dx_held[lo:hi, cols] = value.astype(BF16)

    for n, (src, dst) in enumerate(((dx_held, dx_out), (gr_held, gr_out))):
        own_grads.append(pltpu.make_async_copy(src, dst, in_sem.at[4 + n]))
        own_grads[-1].start()
    waits(wq.at[pl.ds(0, 2 * (tp - 1) * fo), :], WEIGHTS, 0)
    waits(wq.at[pl.ds(0, (tp - 1) * fo), :], DOWN, 0)
    for group, (start, count) in enumerate(groups):
        own = 1 if start <= own_place < start + count else 0
        waits(send_x.at[pl.ds(0, (count - own) * chunk), :], DISPATCH + 2 * group, 0)
    waits(sdx_send.at[pl.ds(0, tp - 1)], SHARED_DX, 0)
    waits(sh1_recv, SHARED_1, 0)
    if ny > 1:
        waits(sh2.at[pl.ds(0, ny - 1)], SHARED_2, 0)
    if nz > 1:
        waits(sh3.at[pl.ds(0, nz - 1)], SHARED_3, 0)
    waits(rs_send.at[pl.ds(0, tp - 1), pl.ds(0, own_rows)], SCATTER, 0)
    waits(rs_send.at[pl.ds(0, tp - 1), pl.ds(own_rows, own_tall - own_rows)], SCATTER_BACK, 0)
    waits(dall.at[pl.ds(0, tp - 1)], GATHER, 0)
    for n in range(2):
        waits(rest_recv[n].at[pl.ds(0, tp - 1)], SCATTER + 2 + 2 * n, 0)
    waits(back_send.at[pl.ds(0, (ep - 1) * cap)], BACK, 0)
    if nz > 1:
        waits(gp_mid.at[pl.ds(0, nz - 1)], GP, 0)
    waits(gp_recv.at[:, pl.ds(0, nyc - 1)], GP + 2, 0)
    waits(sh4, SHARED_4, 0)
    waits(dw_send.at[pl.ds(0, 3 * (tp - 1) * fo), :], GRADS, 0)
    for copy in own_grads:
        copy.wait()
    waits(dw_send.at[pl.ds(0, 3 * (tp - 1) * fo), :], GRADS, 1)


def finish(fo, dx, gr, gg, gu, gd, gs, dx_o, gr_o, gg_o, gu_o, gd_o, gsg_o, gsu_o, gsd_o, wide, small, sem):
    width = gg.shape[1]
    parts = 2
    step = width // parts
    others = [(gs, small[0]), (dx, small[1]), (gr, small[2])]
    ins = [pltpu.make_async_copy(src, dst, sem.at[1 + n]) for n, (src, dst) in enumerate(others)]
    for copy in ins:
        copy.start()
    stores = []
    for t, (src, dst) in enumerate(((gg, gg_o), (gu, gu_o), (gd, gd_o))):
        for c in range(parts):
            cols = slice(c * step, (c + 1) * step)
            wide[t, :, cols] = src[:, cols].astype(F32)
            pltpu.make_async_copy(wide.at[t, :, cols], dst.at[:, cols], sem.at[0]).start()
    for copy in ins:
        copy.wait()
    outs = [(small[0].at[t * fo : (t + 1) * fo], dst) for t, dst in enumerate((gsg_o, gsu_o, gsd_o))]
    outs += [(small[1], dx_o), (small[2], gr_o)]
    for n, (src, dst) in enumerate(outs):
        stores.append(pltpu.make_async_copy(src, dst, sem.at[4 + n]))
        stores[-1].start()
    for copy in stores:
        copy.wait()
    wait_bytes(wide, sem.at[0])


def local(axes, cap, tokens, cotangent, routes, route_weights, expert_gate, expert_up, expert_down, shared_gate, shared_up, shared_down):
    tok, width = tokens.shape
    top = routes.shape[1]
    nz, ny, _ = axes
    ep = lax.axis_size("ep")
    tp = lax.axis_size("tp")
    fo = expert_gate.shape[2]
    ff = fo * tp
    dq = width // tp
    nb = dq // 128
    cb = width // (nz * ny)
    slots = ep * cap
    groups = groups_of(ep)
    own_rows = own_rows_of(groups[0][1] * cap, tp)
    taller = lambda n: n + -(-n // 16) * 8
    rest_rows = [count * cap for _, count in groups[1:]]
    wide = -(-(3 * ff + 1) // 128) * 128
    half = 3 * fo // 2

    sizes = (ep, tp, nz, ny, cap, tok, top, dq, ff, cb)
    vmem = pl.BlockSpec(memory_space=pltpu.VMEM)
    hbm = pl.BlockSpec(memory_space=pltpu.HBM)
    outs = pl.pallas_call(
        functools.partial(kernel, sizes),
        out_shape=(
            jax.ShapeDtypeStruct((tok, dq), BF16),
            jax.ShapeDtypeStruct((1, tok), F32),
            jax.ShapeDtypeStruct((fo, width), BF16),
            jax.ShapeDtypeStruct((fo, width), BF16),
            jax.ShapeDtypeStruct((fo, width), BF16),
            jax.ShapeDtypeStruct((3 * fo, cb // 2), F32),
        ),
        in_specs=[hbm] * 10,
        out_specs=(hbm, hbm, vmem, vmem, vmem, hbm),
        scratch_shapes=[
            pltpu.VMEM((top, tok), I32),
            pltpu.VMEM((top, tok), F32),
            pltpu.VMEM((8, 128), F32),
            pltpu.VMEM((-(-cap // 8) * 8, 128), I32),
            pltpu.SMEM((-(-cap // 8) * 8, 128), I32),
            pltpu.VMEM((-(-cap // 8) * 8, 128), F32),
            pltpu.SMEM((-(-cap // 8) * 8, 128), F32),
            pltpu.VMEM((32, 128), I32),
            pltpu.SMEM((32, 128), I32),
            pltpu.VMEM((8, 128), I32),
            pltpu.VMEM((tok, width), BF16),
            pltpu.VMEM((tok, width), BF16),
            pltpu.VMEM((fo, width), BF16),
            pltpu.VMEM((fo, width), BF16),
            pltpu.VMEM((fo, width), BF16),
            pltpu.VMEM((3, fo, width), BF16),
            pltpu.VMEM((32, 2 * nb, 128), F32),
            pltpu.VMEM((slots * 2 * nb, 128), BF16),
            pltpu.VMEM((slots * 2 * nb, 128), BF16),
            pltpu.VMEM((3 * ff, dq), BF16),
            pltpu.VMEM((slots, 2 * dq), BF16),
            pltpu.VMEM((tp, taller(own_rows), 2 * ff), F32),
            pltpu.VMEM((tp, taller(own_rows), 2 * ff), BF16),
            pltpu.VMEM((tp, taller(own_rows), 2 * ff), BF16),
            [pltpu.VMEM((taller(n), 2 * ff), F32) for n in rest_rows],
            [pltpu.VMEM((taller(n), 2 * ff), BF16) for n in rest_rows],
            [pltpu.VMEM((tp, taller(n), 2 * ff), BF16) for n in rest_rows],
            pltpu.VMEM((tp, own_rows, wide), BF16),
            pltpu.VMEM((slots, wide), F32),
            pltpu.VMEM((slots, nb, 128), BF16),
            pltpu.VMEM((slots, nb, 128), BF16),
            pltpu.VMEM((ep, 1, 128), F32),
            pltpu.VMEM((nz, 2 * ny, 1, 128), F32),
            pltpu.VMEM((nz, 2 * ny, 1, 128), F32),
            pltpu.VMEM((3 * ff, dq), BF16),
            pltpu.VMEM((tp, tok, dq), BF16),
            pltpu.VMEM((tp, tok, dq), BF16),
            pltpu.VMEM((2, ny, nz, half, cb), BF16),
            pltpu.VMEM((ny, nz, half, cb), BF16),
            pltpu.VMEM((ny, nz, half, cb), BF16),
            pltpu.VMEM((ny, nz, half, cb), BF16),
            pltpu.VMEM((nz, half, cb), BF16),
            pltpu.VMEM((nz, half, cb), BF16),
            pltpu.VMEM((half, cb), F32),
            pltpu.VMEM((half, cb), F32),
            pltpu.VMEM((32, nb, 128), F32),
            pltpu.VMEM((32, 128), F32),
            pltpu.VMEM((3 * fo, cb // 2), F32),
            pltpu.VMEM((tok, dq), BF16),
            pltpu.VMEM((1, tok), F32),
            pltpu.SemaphoreType.DMA((2 * PAIRS,)),
            pltpu.SemaphoreType.DMA((13,)),
        ],
        compiler_params=pltpu.CompilerParams(
            collective_id=0, has_side_effects=True, vmem_limit_bytes=50*1024*1024
        ),
    )(
        *[pltpu.with_memory_space_constraint(a, pltpu.HBM) for a in (
        routes.T,
        route_weights.T,
        tokens,
        cotangent,
        expert_gate[0].T,
        expert_up[0].T,
        expert_down[0],
        shared_gate.T,
        shared_up.T,
        shared_down,
        )]
    )
    dx, gr, gg, gu, gd, gsg, gsu, gsd = pl.pallas_call(
        functools.partial(finish, fo),
        out_shape=(
            jax.ShapeDtypeStruct((tok, dq), BF16),
            jax.ShapeDtypeStruct((1, tok), F32),
            jax.ShapeDtypeStruct((fo, width), F32),
            jax.ShapeDtypeStruct((fo, width), F32),
            jax.ShapeDtypeStruct((fo, width), F32),
            jax.ShapeDtypeStruct((fo, cb // 2), F32),
            jax.ShapeDtypeStruct((fo, cb // 2), F32),
            jax.ShapeDtypeStruct((fo, cb // 2), F32),
        ),
        in_specs=[hbm, hbm, vmem, vmem, vmem, hbm],
        out_specs=(hbm,) * 8,
        scratch_shapes=[
            pltpu.VMEM((3, fo, width), F32),
            [pltpu.VMEM((3 * fo, cb // 2), F32), pltpu.VMEM((tok, dq), BF16), pltpu.VMEM((1, tok), F32)],
            pltpu.SemaphoreType.DMA((9,)),
        ],
        compiler_params=pltpu.CompilerParams(vmem_limit_bytes=16*1024*1024),
    )(*outs)
    return (dx, gr.T, gg.T[None], gu.T[None], gd[None], gsg.T, gsu.T, gsd)


def solution(mesh):
    placed = (
        P("ep", None),
        P("ep", None),
        P("ep", None),
        P("ep", None),
        P("ep", None, "tp"),
        P("ep", None, "tp"),
        P("ep", "tp", None),
        P(None, "tp"),
        P(None, "tp"),
        P("tp", None),
    )
    return jax.shard_map(
        functools.partial(local, EP_AXES, CAP),
        mesh=mesh,
        in_specs=placed,
        out_specs=(
            P("ep", "tp"),
            P("ep", "tp"),
            P("ep", None, "tp"),
            P("ep", None, "tp"),
            P("ep", "tp", None),
            P("ep", "tp"),
            P("ep", "tp"),
            P("tp", "ep"),
        ),
        check_vma=False,
    )
```

```python
import functools

import jax
import jax.numpy as jnp
from jax import lax
from jax.experimental import pallas as pl
from jax.experimental.pallas import tpu as pltpu
from jax.sharding import PartitionSpec as P

MESH = pl.DeviceIdType.MESH
F32 = jnp.float32
BF16 = jnp.bfloat16
I32 = jnp.int32
EP_AXES = (8, 4, 2)
CAP = 3
(WEIGHTS, SHARED_DX, SHARED_1, SHARED_2, SHARED_3, SHARED_4, GATHER, BACK, GRADS, GP, DISPATCH, SCATTER) = (
    *range(0, 20, 2),
    22,
    28,
)
DOWN, SCATTER_BACK = 34, 36
PAIRS = 19


def dot_nn(a, b):
    return lax.dot_general(a, b, (((1,), (0,)), ((), ())), preferred_element_type=F32)


def dot_nt(a, b):
    return lax.dot_general(a, b, (((1,), (1,)), ((), ())), preferred_element_type=F32)


def dot_tn(a, b):
    return lax.dot_general(a, b, (((0,), (0,)), ((), ())), preferred_element_type=F32)


def wait_bytes(ref, sem):
    pltpu.make_async_copy(ref, ref, sem).wait()


def swish_parts(v):
    sigma = jax.nn.sigmoid(v)
    return v * sigma, sigma * (1.0 + v * (1.0 - sigma))


def swap_matrix(outer, inner):
    size = outer * inner
    row = lax.broadcasted_iota(I32, (size, size), 0)
    col = lax.broadcasted_iota(I32, (size, size), 1)
    return ((row % inner) * outer + row // inner == col).astype(BF16)


def z_order(nz):
    if nz == 8:
        return (1, 7, 0, 2, 6, 3, 5, 4)
    return tuple(range(nz))


def groups_of(ep):
    part = ep // 8
    return ((0, 5 * part), (5 * part, 2 * part), (7 * part, part))


def own_rows_of(first_rows, tp):
    return -(-first_rows // (8 * tp)) * 8


def kernel(
    sizes,
    routes_in,
    weights_in,
    x_in,
    g_in,
    wg_in,
    wu_in,
    wd_in,
    sg_in,
    su_in,
    sd_in,
    dx_out,
    gr_out,
    gg_out,
    gu_out,
    gd_out,
    gs_out,
    routes,
    weights,
    weight_turn,
    assign_table,
    assign_of,
    scale_table,
    scale_of,
    slot_table,
    slot_of,
    turn,
    x_ref,
    g_ref,
    sg_ref,
    su_ref,
    sd_ref,
    staged,
    tiles,
    send_x,
    recv_x,
    wq,
    rows,
    part,
    rs_send,
    rs_recv,
    rest,
    rest_send,
    rest_recv,
    dall,
    dfull,
    back_send,
    back_recv,
    gp_send,
    gp_mid,
    gp_recv,
    dw_send,
    sdx_send,
    sdx_recv,
    sh1,
    sh1_recv,
    sh2,
    sh2_recv,
    sh3,
    sh3_recv,
    sh4,
    sh4_recv,
    comb,
    grow,
    gs_held,
    dx_held,
    gr_held,
    sem,
    in_sem,
):
    ep, tp, nz, ny, cap, tok, top, dq, ff, cb = sizes
    slots = ep * cap
    nb = dq // 128
    nyc = 2 * ny
    groups = groups_of(ep)
    first_rows = groups[0][1] * cap
    own_rows = own_rows_of(first_rows, tp)
    fo = ff // tp
    chunk = cap * 2 * nb
    me = lax.axis_index("ep")
    q = lax.axis_index("tp")
    core = lax.rem(me, 2)
    yc = lax.rem(me, nyc)
    yy = yc // 2
    zz = me // nyc
    sib = me + 1 - 2 * core

    tp_order = sorted(range(1, tp), key=lambda i: -min(i, tp - i))

    def tp_peer(i):
        return lax.rem(q + i, tp)

    def to_of(dz, w):
        return lax.rem(zz + dz, nz) * nyc + lax.rem(yc + w, nyc)

    def from_of(dz, w):
        return lax.rem(zz + nz - dz, nz) * nyc + lax.rem(yc + nyc - w, nyc)

    def send(src, dst, kind, device):
        pltpu.make_async_remote_copy(
            src_ref=src,
            dst_ref=dst,
            send_sem=sem.at[kind],
            recv_sem=sem.at[kind + 1],
            device_id=device,
            device_id_type=MESH,
        ).start()

    def waits(ref, kind, side):
        wait_bytes(ref, sem.at[kind + side])

    def positions(group):
        start, count = groups[group]
        for k, dz in enumerate(z_order(nz)):
            lo = max(k * nyc, start)
            hi = min((k + 1) * nyc, start + count)
            if lo < hi:
                yield lo - k * nyc, hi - k * nyc, dz, k * nyc

    own_place = z_order(nz).index(0) * nyc

    def block_of(i, size):
        return pl.ds(pl.multiple_of(i * size, size), size)

    barrier = pltpu.get_barrier_semaphore()
    for dz in sorted(range(nz), key=lambda dz: -min(dz, nz - dz)):
        for w in range(1 if dz == 0 else 0, nyc):
            pl.semaphore_signal(barrier, inc=1, device_id={"ep": to_of(dz, w)}, device_id_type=MESH)

    for i in range(1, tp):
        pl.semaphore_signal(barrier, inc=1, device_id={"tp": tp_peer(i)}, device_id_type=MESH)

    own_cols = pl.ds(pl.multiple_of(q * dq, 128), dq)
    fetches = [
        pltpu.make_async_copy(src, dst, in_sem.at[n])
        for n, (src, dst) in enumerate(
            [
                (routes_in, routes),
                (weights_in, weights),
                (x_in, x_ref),
                (g_in, g_ref),
                (sg_in, sg_ref),
                (su_in, su_ref),
                (sd_in, sd_ref),
            ]
            + [(ref, staged.at[t]) for t, ref in enumerate((wg_in, wu_in, wd_in))]
        )
    ]
    for fetch in fetches:
        fetch.start()

    fetches[0].wait()
    turn[...] = jnp.zeros_like(turn)
    turn[0:top, 0:tok] = routes[...]
    by_row = turn[...].T
    fetches[1].wait()
    weight_turn[...] = jnp.zeros_like(weight_turn)
    weight_turn[0:top, 0:tok] = weights[...]
    weight_by_row = weight_turn[...].T
    expert = lax.broadcasted_iota(I32, (32, 128), 1)
    token = lax.broadcasted_iota(I32, (32, 128), 0)
    named = [(by_row[0:32, k : k + 1] == expert) & (token < tok) for k in range(top)]
    count = jnp.zeros((32, 128), I32)
    for k in range(top):
        count = count + named[k].astype(I32)
    before = count
    for shift in (1, 2, 4, 8, 16):
        before = before + jnp.where(token < shift, 0, pltpu.roll(before, shift, 0))
    before = before - count
    weight = jnp.zeros((32, 128), F32)
    for k in range(top):
        weight = weight + jnp.where(named[k], weight_by_row[0:32, k : k + 1], 0.0)
    slot = jnp.zeros((32, 128), I32)
    for k in range(top):
        mine = jnp.sum(jnp.where(named[k], expert * cap + before, 0), axis=1, keepdims=True)
        slot = jnp.where(expert == k, mine, slot)
    slot_table[...] = slot
    for j in range(cap):
        here = (count > 0) & (before == j)
        which = jnp.sum(jnp.where(here, token + 1, 0), axis=0, keepdims=True)
        assign_table[j : j + 1, :] = jnp.where(which > 0, which - 1, tok)
        scale_table[j : j + 1, :] = jnp.sum(jnp.where(here, weight, 0.0), axis=0, keepdims=True)
    tables = [
        pltpu.make_async_copy(assign_table, assign_of, in_sem.at[10]),
        pltpu.make_async_copy(scale_table, scale_of, in_sem.at[11]),
        pltpu.make_async_copy(slot_table, slot_of, in_sem.at[12]),
    ]
    for table in tables:
        table.start()

    fetches[2].wait()
    fetches[3].wait()
    col0 = q * dq
    swap_out = swap_matrix(16, 2 * nb)
    for part_no in range(2):
        lo = part_no * 16
        hi = min(tok, lo + 16)
        pieces = []
        for ref in (x_ref, g_ref):
            for b in range(nb):
                cols = pl.ds(pl.multiple_of(col0 + b * 128, 128), 128)
                piece = ref[lo:hi, cols].astype(F32)
                if hi - lo < 16:
                    piece = jnp.concatenate([piece, jnp.zeros((16 - hi + lo, 128), F32)], axis=0)
                pieces.append(piece)
        stacked = jnp.concatenate(pieces, axis=0).astype(BF16)
        moved = dot_nn(swap_out, stacked)
        tiles[lo : lo + 16] = moved.reshape(16, 2 * nb, 128)

    for table in tables:
        table.wait()
    lower = lax.broadcasted_iota(I32, (2 * nb, 128), 0) < nb

    def pick(group):
        for lo, hi, dz, place in positions(group):

            @pl.loop(lo, hi, unroll=4)
            def _(w):
                p = to_of(dz, w)
                for j in range(cap):
                    tile = tiles[assign_of[j, p]]
                    scale = jnp.where(lower, jnp.float32(1.0), scale_of[j, p])
                    at = pl.ds(pl.multiple_of(((place + w) * cap + j) * 2 * nb, 2 * nb), 2 * nb)
                    send_x[at, :] = (tile * scale).astype(BF16)

    def dispatch(group):
        for lo, hi, dz, place in positions(group):

            @pl.loop(max(lo, 1) if dz == 0 else lo, hi, unroll=4)
            def _(w):
                here = block_of(place + w, chunk)
                send(send_x.at[here, :], recv_x.at[here, :], DISPATCH + 2 * group, {"ep": to_of(dz, w)})

    pick(0)
    pl.semaphore_wait(barrier, ep - 1 + tp - 1)

    dispatch(0)
    for n in (7, 8, 9):
        fetches[n].wait()
    for types, kind in (((0, 1), WEIGHTS), ((2,), DOWN)):
        for i in tp_order:
            for t in types:
                dst_rows = pl.ds(pl.multiple_of(t * ff + q * fo, 16), fo)
                src_cols = pl.ds(pl.multiple_of(tp_peer(i) * dq, 128), dq)
                send(staged.at[t, :, src_cols], wq.at[dst_rows, :], kind, {"tp": tp_peer(i)})
    pick(1)
    dispatch(1)
    pick(2)
    dispatch(2)
    recv_x[own_place * chunk : (own_place + 1) * chunk, :] = send_x[own_place * chunk : (own_place + 1) * chunk, :]

    for n in (4, 5, 6):
        fetches[n].wait()
    x = x_ref[...]
    s_gate = dot_nt(x, sg_ref[...])
    s_up = dot_nt(x, su_ref[...])
    s_back = dot_nt(g_ref[...], sd_ref[...])
    s_active, s_slope = swish_parts(s_gate)
    s_hidden = (s_active * s_up).astype(BF16)
    ds_gate = (s_back * s_up * s_slope).astype(BF16)
    ds_up = (s_back * s_active).astype(BF16)
    for j in range(tp):
        cols = slice(j * dq, (j + 1) * dq)
        piece = dot_nn(ds_gate, sg_ref[:, cols]) + dot_nn(ds_up, su_ref[:, cols])
        sdx_send[j] = piece.astype(BF16)
    half = 3 * fo // 2
    for z in range(nz):
        cols = slice(z * ny * cb, (z + 1) * ny * cb)
        xz = x_ref[:, cols]
        whole = jnp.concatenate(
            [dot_tn(ds_gate, xz), dot_tn(ds_up, xz), dot_tn(s_hidden, g_ref[:, cols])], axis=0
        )
        for y in range(ny):
            for h in range(2):
                sh1[h, y, z] = whole[h * half : (h + 1) * half, y * cb : (y + 1) * cb].astype(BF16)
    send(sh1.at[1 - core], sh1_recv, SHARED_1, {"ep": sib})

    waits(sh1_recv, SHARED_1, 1)
    for y in range(ny):
        for z in range(nz):
            both = sh1[core, y, z].astype(F32) + sh1_recv[y, z].astype(F32)
            sh2[y, z] = both.astype(BF16)
    for i in range(1, ny):
        y = lax.rem(yy + i, ny)
        send(sh2.at[y], sh2_recv.at[yy], SHARED_2, {"ep": (zz * ny + y) * 2 + core})

    swap_in = {n: swap_matrix(2 * nb, n) for n in (8, 16)}
    swap_back = {n: swap_matrix(n, nb) for n in (8, 16)}

    def steps_of(base, count):
        lo = base
        while lo < base + count:
            n = 16 if lo % 16 == 0 and lo + 16 <= base + count else 8
            yield lo, n
            lo += n

    def arrived(group):
        start, count = groups[group]
        own = 1 if start <= own_place < start + count else 0
        waits(recv_x.at[pl.ds(0, (count - own) * chunk), :], DISPATCH + 2 * group, 1)

    def relayout(group):
        base, count = groups[group][0] * cap, groups[group][1] * cap
        for lo, n in steps_of(base, count):
            moved = dot_nn(swap_in[n], recv_x[lo * 2 * nb : (lo + n) * 2 * nb, :])
            for b in range(2 * nb):
                rows[lo : lo + n, b * 128 : (b + 1) * 128] = moved[b * n : (b + 1) * n].astype(BF16)

    def contract(group):
        base, count = groups[group][0] * cap, groups[group][1] * cap
        relayout(group)
        up_part = dot_nt(rows[base : base + count, 0:dq], wq[0 : 2 * ff, :])
        back_part = dot_nt(rows[base : base + count, dq : 2 * dq], wq[2 * ff : 3 * ff, :])
        return up_part, back_part

    def packed_rows(n):
        return n + -(-n // 16) * 8

    def pack(ref, up, back):
        n = up.shape[0]
        half_n = packed_rows(n) - n
        ref[0:n, :] = up.astype(ref.dtype)
        ref[n : n + half_n, 0:ff] = back[0:half_n].astype(ref.dtype)
        ref[n : n + n - half_n, ff : 2 * ff] = back[half_n:n].astype(ref.dtype)

    def unpacked(total, n):
        half_n = packed_rows(n) - n
        back = jnp.concatenate([total[n : n + half_n, 0:ff], total[n : n + n - half_n, ff : 2 * ff]], axis=0)
        return total[0:n, 0:ff], total[0:n, ff : 2 * ff], back

    own_tall = packed_rows(own_rows)

    def blocks_of(whole):
        for b in range(tp):
            lo, hi = b * own_rows, min((b + 1) * own_rows, first_rows)
            block = whole[lo:hi]
            if hi - lo < own_rows:
                block = jnp.concatenate([block, jnp.zeros((own_rows - hi + lo, whole.shape[1]), F32)], axis=0)
            yield b, block

    def scatter_up():
        relayout(0)
        for b, block in blocks_of(dot_nt(rows[0:first_rows, 0:dq], wq[0 : 2 * ff, :])):
            part[b, 0:own_rows, :] = block
            rs_send[b, 0:own_rows, :] = block.astype(BF16)
        here = pl.ds(0, own_rows)
        for i in tp_order:
            send(rs_send.at[tp_peer(i), here], rs_recv.at[q, here], SCATTER, {"tp": tp_peer(i)})

    def scatter_back():
        half_n = own_tall - own_rows
        for b, block in blocks_of(dot_nt(rows[0:first_rows, dq : 2 * dq], wq[2 * ff : 3 * ff, :])):
            for ref in (part, rs_send):
                ref[b, own_rows:own_tall, 0:ff] = block[0:half_n].astype(ref.dtype)
                ref[b, own_rows : 2 * own_rows - half_n, ff : 2 * ff] = block[half_n:own_rows].astype(ref.dtype)
        here = pl.ds(own_rows, half_n)
        for i in tp_order:
            send(rs_send.at[tp_peer(i), here], rs_recv.at[q, here], SCATTER_BACK, {"tp": tp_peer(i)})

    def spread_rest(group):
        up_part, back_part = contract(group)
        n = group - 1
        pack(rest[n], up_part, back_part)
        pack(rest_send[n], up_part, back_part)
        for i in tp_order:
            send(rest_send[n], rest_recv[n].at[q], SCATTER + 2 * group, {"tp": tp_peer(i)})

    def gradients(total, n):
        gate, up, back = unpacked(total, n)
        active, slope = swish_parts(gate)
        hidden = (active * up).astype(BF16).astype(F32)
        gp = jnp.sum(hidden * back, axis=1, keepdims=True)
        extra = dfull.shape[1] - 3 * ff
        return jnp.concatenate(
            [back * up * slope, back * active, hidden, jnp.broadcast_to(gp, (gp.shape[0], extra))], axis=1
        )

    def gather_first():
        waits(rs_recv.at[pl.ds(0, tp - 1), pl.ds(0, own_rows)], SCATTER, 1)
        waits(rs_recv.at[pl.ds(0, tp - 1), pl.ds(own_rows, own_tall - own_rows)], SCATTER_BACK, 1)
        total = part[q]
        for i in range(1, tp):
            total = total + rs_recv[tp_peer(i)].astype(F32)
        dall[q] = gradients(total, own_rows).astype(BF16)
        mine = dall.at[q]
        for i in tp_order:
            send(mine, mine, GATHER, {"tp": tp_peer(i)})

    def finish_first():
        waits(dall.at[pl.ds(0, tp - 1)], GATHER, 1)
        for b in range(tp):
            lo, hi = b * own_rows, min((b + 1) * own_rows, first_rows)
            dfull[lo:hi, :] = dall[b].astype(F32)[0 : hi - lo]

    def finish_rest(group):
        n = group - 1
        waits(rest_recv[n].at[pl.ds(0, tp - 1)], SCATTER + 2 * group, 1)
        total = rest[n][...]
        for i in range(1, tp):
            total = total + rest_recv[n][tp_peer(i)].astype(F32)
        base, count = groups[group][0] * cap, groups[group][1] * cap
        dfull[base : base + count, :] = gradients(total, count)

    def send_back(group):
        start, places = groups[group]
        base, count = start * cap, places * cap
        d = dfull[base : base + count, :]
        dxr = dot_nn(d[:, 0 : 2 * ff].astype(BF16), wq[0 : 2 * ff, :])
        for lo, n in steps_of(0, count):
            stacked = jnp.concatenate(
                [dxr[lo : lo + n, b * 128 : (b + 1) * 128] for b in range(nb)], axis=0
            ).astype(BF16)
            moved = dot_nn(swap_back[n], stacked)
            back_send[base + lo : base + lo + n] = moved.reshape(n, nb, 128).astype(BF16)
        for lo, hi, dz, place in positions(group):
            if dz == 0 and lo == 0:
                back_recv[pl.ds(me * cap, cap)] = back_send[place * cap : (place + 1) * cap]

            @pl.loop(max(lo, 1) if dz == 0 else lo, hi, unroll=4)
            def _(w):
                to = {"ep": from_of(dz, w)}
                send(
                    back_send.at[pl.ds((place + w) * cap, cap)],
                    back_recv.at[pl.ds(me * cap, cap)],
                    BACK,
                    to,
                )

    def send_route_sums(group):
        start, places = groups[group]
        base, count = start * cap, places * cap
        d = dfull[base : base + count, :]
        src_row = lax.broadcasted_iota(I32, (places, count), 0)
        src_col = lax.broadcasted_iota(I32, (places, count), 1)
        collect = (src_col // cap == src_row).astype(F32)
        lane = lax.broadcasted_iota(I32, (count, 128), 1)
        slot_row = lax.broadcasted_iota(I32, (count, 128), 0)
        spread = jnp.where(lane == slot_row % cap, d[:, 3 * ff : 3 * ff + 1], 0.0)
        gp_send[start : start + places] = dot_nn(collect, spread).reshape(places, 1, 128)
        for lo, hi, dz, place in positions(group):
            if dz == 0:
                gp_mid[zz, lo:hi] = gp_send[place + lo : place + hi]
            else:
                send(
                    gp_send.at[pl.ds(place + lo, hi - lo)],
                    gp_mid.at[zz, pl.ds(lo, hi - lo)],
                    GP,
                    {"ep": from_of(dz, 0)},
                )

    def spread_route_sums():
        if nz > 1:
            waits(gp_mid.at[pl.ds(0, nz - 1)], GP, 1)
        for w in range(1, nyc):
            send(gp_mid.at[:, w], gp_recv.at[:, yc], GP + 2, {"ep": from_of(0, w)})
        gp_recv[:, yc] = gp_mid[:, 0]

    for t in range(3):
        wq[pl.ds(pl.multiple_of(t * ff + q * fo, 16), fo), :] = staged[t, :, own_cols]
    waits(wq.at[pl.ds(0, 2 * (tp - 1) * fo), :], WEIGHTS, 1)
    arrived(0)
    scatter_up()
    waits(wq.at[pl.ds(0, (tp - 1) * fo), :], DOWN, 1)
    scatter_back()
    for i in tp_order:
        send(sdx_send.at[tp_peer(i)], sdx_recv.at[q], SHARED_DX, {"tp": tp_peer(i)})
    gather_first()
    arrived(1)
    spread_rest(1)
    arrived(2)
    spread_rest(2)
    if ny > 1:
        waits(sh2_recv.at[pl.ds(0, ny - 1)], SHARED_2, 1)
    for z in range(nz):
        total = sh2[yy, z].astype(F32)
        for i in range(1, ny):
            total = total + sh2_recv[lax.rem(yy + i, ny), z].astype(F32)
        sh3[z] = total.astype(BF16)
    for i in range(1, nz):
        z = lax.rem(zz + i, nz)
        send(sh3.at[z], sh3_recv.at[zz], SHARED_3, {"ep": (z * ny + yy) * 2 + core})
    finish_rest(1)
    send_route_sums(1)
    send_back(1)
    finish_first()
    finish_rest(2)
    d = dfull[:, 0 : 3 * ff].astype(BF16)
    own_grads = []

    def send_grads(t, out):
        for i in tp_order:
            src_rows = pl.ds(pl.multiple_of(t * ff + tp_peer(i) * fo, 16), fo)
            send(dw_send.at[src_rows, :], out.at[:, own_cols], GRADS, {"tp": tp_peer(i)})
        mine = pl.ds(pl.multiple_of(t * ff + q * fo, 16), fo)
        own_grads.append(pltpu.make_async_copy(dw_send.at[mine, :], out.at[:, own_cols], in_sem.at[t]))
        own_grads[-1].start()

    dw_send[2 * ff : 3 * ff, :] = dot_tn(d[:, 2 * ff : 3 * ff], rows[:, dq : 2 * dq]).astype(BF16)
    send_grads(2, gd_out)
    dw_send[0 : 2 * ff, :] = dot_tn(d[:, 0 : 2 * ff], rows[:, 0:dq]).astype(BF16)
    send_grads(0, gg_out)
    send_grads(1, gu_out)
    send_route_sums(2)
    send_route_sums(0)
    send_back(2)
    send_back(0)
    spread_route_sums()

    if nz > 1:
        waits(sh3_recv.at[pl.ds(0, nz - 1)], SHARED_3, 1)
    total = sh3[zz].astype(F32)
    for i in range(1, nz):
        total = total + sh3_recv[lax.rem(zz + i, nz)].astype(F32)
    sh4[...] = total
    send(sh4, sh4_recv, SHARED_4, {"ep": sib})
    waits(sdx_recv.at[pl.ds(0, tp - 1)], SHARED_DX, 1)
    waits(sh4_recv, SHARED_4, 1)
    first = core == 0
    full = jnp.concatenate(
        [
            jnp.where(first, sh4[...], sh4_recv[...]),
            jnp.where(first, sh4_recv[...], sh4[...]),
        ],
        axis=0,
    )
    gs_held[...] = jnp.where(first, full[:, 0 : cb // 2], full[:, cb // 2 : cb])
    own_grads.append(pltpu.make_async_copy(gs_held, gs_out, in_sem.at[3]))
    own_grads[-1].start()

    waits(back_recv.at[pl.ds(0, (ep - 1) * cap)], BACK, 1)
    waits(gp_recv.at[:, pl.ds(0, nyc - 1)], GP + 2, 1)
    row_lane = lax.broadcasted_iota(I32, (1, 128), 1)
    comb[...] = jnp.zeros_like(comb)
    for t in range(tok):
        total = back_recv[slot_of[t, 0]].astype(F32)
        for k in range(1, top):
            total = total + back_recv[slot_of[t, k]].astype(F32)
        comb[t] = total
        s = slot_of[t, q]
        value = jnp.where(row_lane == s % cap, gp_recv[s // (cap * nyc), (s // cap) % nyc], 0.0)
        grow[t : t + 1, :] = value
    gr_held[...] = jnp.sum(grow[...].T, axis=0, keepdims=True)[:, 0:tok] / weights[pl.ds(q, 1), :]
    swap_tok = swap_matrix(nb, 16)
    for part_no in range(2):
        lo = part_no * 16
        hi = min(tok, lo + 16)
        v = comb[lo : lo + 16].reshape(16 * nb, 128)
        top_half = v.astype(BF16)
        rest = (v - top_half.astype(F32)).astype(BF16)
        moved = dot_nn(swap_tok, top_half) + dot_nn(swap_tok, rest)
        for b in range(nb):
            cols = slice(b * 128, (b + 1) * 128)
            value = moved[b * 16 : b * 16 + hi - lo]
            value = value + sdx_send[q, lo:hi, cols].astype(F32)
            for i in range(1, tp):
                value = value + sdx_recv[tp_peer(i), lo:hi, cols].astype(F32)
            dx_held[lo:hi, cols] = value.astype(BF16)

    for n, (src, dst) in enumerate(((dx_held, dx_out), (gr_held, gr_out))):
        own_grads.append(pltpu.make_async_copy(src, dst, in_sem.at[4 + n]))
        own_grads[-1].start()
    waits(wq.at[pl.ds(0, 2 * (tp - 1) * fo), :], WEIGHTS, 0)
    waits(wq.at[pl.ds(0, (tp - 1) * fo), :], DOWN, 0)
    for group, (start, count) in enumerate(groups):
        own = 1 if start <= own_place < start + count else 0
        waits(send_x.at[pl.ds(0, (count - own) * chunk), :], DISPATCH + 2 * group, 0)
    waits(sdx_send.at[pl.ds(0, tp - 1)], SHARED_DX, 0)
    waits(sh1_recv, SHARED_1, 0)
    if ny > 1:
        waits(sh2.at[pl.ds(0, ny - 1)], SHARED_2, 0)
    if nz > 1:
        waits(sh3.at[pl.ds(0, nz - 1)], SHARED_3, 0)
    waits(rs_send.at[pl.ds(0, tp - 1), pl.ds(0, own_rows)], SCATTER, 0)
    waits(rs_send.at[pl.ds(0, tp - 1), pl.ds(own_rows, own_tall - own_rows)], SCATTER_BACK, 0)
    waits(dall.at[pl.ds(0, tp - 1)], GATHER, 0)
    for n in range(2):
        waits(rest_recv[n].at[pl.ds(0, tp - 1)], SCATTER + 2 + 2 * n, 0)
    waits(back_send.at[pl.ds(0, (ep - 1) * cap)], BACK, 0)
    if nz > 1:
        waits(gp_mid.at[pl.ds(0, nz - 1)], GP, 0)
    waits(gp_recv.at[:, pl.ds(0, nyc - 1)], GP + 2, 0)
    waits(sh4, SHARED_4, 0)
    waits(dw_send.at[pl.ds(0, 3 * (tp - 1) * fo), :], GRADS, 0)
    for copy in own_grads:
        copy.wait()
    waits(dw_send.at[pl.ds(0, 3 * (tp - 1) * fo), :], GRADS, 1)


def finish(fo, dx, gr, gg, gu, gd, gs, dx_o, gr_o, gg_o, gu_o, gd_o, gsg_o, gsu_o, gsd_o, wide, small, sem):
    width = gg.shape[1]
    parts = 2
    step = width // parts
    others = [(gs, small[0]), (dx, small[1]), (gr, small[2])]
    ins = [pltpu.make_async_copy(src, dst, sem.at[1 + n]) for n, (src, dst) in enumerate(others)]
    for copy in ins:
        copy.start()
    stores = []
    for t, (src, dst) in enumerate(((gg, gg_o), (gu, gu_o), (gd, gd_o))):
        for c in range(parts):
            cols = slice(c * step, (c + 1) * step)
            wide[t, :, cols] = src[:, cols].astype(F32)
            pltpu.make_async_copy(wide.at[t, :, cols], dst.at[:, cols], sem.at[0]).start()
    for copy in ins:
        copy.wait()
    outs = [(small[0].at[t * fo : (t + 1) * fo], dst) for t, dst in enumerate((gsg_o, gsu_o, gsd_o))]
    outs += [(small[1], dx_o), (small[2], gr_o)]
    for n, (src, dst) in enumerate(outs):
        stores.append(pltpu.make_async_copy(src, dst, sem.at[4 + n]))
        stores[-1].start()
    for copy in stores:
        copy.wait()
    wait_bytes(wide, sem.at[0])


def local(axes, cap, tokens, cotangent, routes, route_weights, expert_gate, expert_up, expert_down, shared_gate, shared_up, shared_down):
    tok, width = tokens.shape
    top = routes.shape[1]
    nz, ny, _ = axes
    ep = lax.axis_size("ep")
    tp = lax.axis_size("tp")
    fo = expert_gate.shape[2]
    ff = fo * tp
    dq = width // tp
    nb = dq // 128
    cb = width // (nz * ny)
    slots = ep * cap
    groups = groups_of(ep)
    own_rows = own_rows_of(groups[0][1] * cap, tp)
    taller = lambda n: n + -(-n // 16) * 8
    rest_rows = [count * cap for _, count in groups[1:]]
    wide = -(-(3 * ff + 1) // 128) * 128
    half = 3 * fo // 2

    sizes = (ep, tp, nz, ny, cap, tok, top, dq, ff, cb)
    vmem = pl.BlockSpec(memory_space=pltpu.VMEM)
    hbm = pl.BlockSpec(memory_space=pltpu.HBM)
    outs = pl.pallas_call(
        functools.partial(kernel, sizes),
        out_shape=(
            jax.ShapeDtypeStruct((tok, dq), BF16),
            jax.ShapeDtypeStruct((1, tok), F32),
            jax.ShapeDtypeStruct((fo, width), BF16),
            jax.ShapeDtypeStruct((fo, width), BF16),
            jax.ShapeDtypeStruct((fo, width), BF16),
            jax.ShapeDtypeStruct((3 * fo, cb // 2), F32),
        ),
        in_specs=[hbm] * 10,
        out_specs=(hbm, hbm, vmem, vmem, vmem, hbm),
        scratch_shapes=[
            pltpu.VMEM((top, tok), I32),
            pltpu.VMEM((top, tok), F32),
            pltpu.VMEM((8, 128), F32),
            pltpu.VMEM((-(-cap // 8) * 8, 128), I32),
            pltpu.SMEM((-(-cap // 8) * 8, 128), I32),
            pltpu.VMEM((-(-cap // 8) * 8, 128), F32),
            pltpu.SMEM((-(-cap // 8) * 8, 128), F32),
            pltpu.VMEM((32, 128), I32),
            pltpu.SMEM((32, 128), I32),
            pltpu.VMEM((8, 128), I32),
            pltpu.VMEM((tok, width), BF16),
            pltpu.VMEM((tok, width), BF16),
            pltpu.VMEM((fo, width), BF16),
            pltpu.VMEM((fo, width), BF16),
            pltpu.VMEM((fo, width), BF16),
            pltpu.VMEM((3, fo, width), BF16),
            pltpu.VMEM((32, 2 * nb, 128), F32),
            pltpu.VMEM((slots * 2 * nb, 128), BF16),
            pltpu.VMEM((slots * 2 * nb, 128), BF16),
            pltpu.VMEM((3 * ff, dq), BF16),
            pltpu.VMEM((slots, 2 * dq), BF16),
            pltpu.VMEM((tp, taller(own_rows), 2 * ff), F32),
            pltpu.VMEM((tp, taller(own_rows), 2 * ff), BF16),
            pltpu.VMEM((tp, taller(own_rows), 2 * ff), BF16),
            [pltpu.VMEM((taller(n), 2 * ff), F32) for n in rest_rows],
            [pltpu.VMEM((taller(n), 2 * ff), BF16) for n in rest_rows],
            [pltpu.VMEM((tp, taller(n), 2 * ff), BF16) for n in rest_rows],
            pltpu.VMEM((tp, own_rows, wide), BF16),
            pltpu.VMEM((slots, wide), F32),
            pltpu.VMEM((slots, nb, 128), BF16),
            pltpu.VMEM((slots, nb, 128), BF16),
            pltpu.VMEM((ep, 1, 128), F32),
            pltpu.VMEM((nz, 2 * ny, 1, 128), F32),
            pltpu.VMEM((nz, 2 * ny, 1, 128), F32),
            pltpu.VMEM((3 * ff, dq), BF16),
            pltpu.VMEM((tp, tok, dq), BF16),
            pltpu.VMEM((tp, tok, dq), BF16),
            pltpu.VMEM((2, ny, nz, half, cb), BF16),
            pltpu.VMEM((ny, nz, half, cb), BF16),
            pltpu.VMEM((ny, nz, half, cb), BF16),
            pltpu.VMEM((ny, nz, half, cb), BF16),
            pltpu.VMEM((nz, half, cb), BF16),
            pltpu.VMEM((nz, half, cb), BF16),
            pltpu.VMEM((half, cb), F32),
            pltpu.VMEM((half, cb), F32),
            pltpu.VMEM((32, nb, 128), F32),
            pltpu.VMEM((32, 128), F32),
            pltpu.VMEM((3 * fo, cb // 2), F32),
            pltpu.VMEM((tok, dq), BF16),
            pltpu.VMEM((1, tok), F32),
            pltpu.SemaphoreType.DMA((2 * PAIRS,)),
            pltpu.SemaphoreType.DMA((13,)),
        ],
        compiler_params=pltpu.CompilerParams(
            collective_id=0, has_side_effects=True, vmem_limit_bytes=50*1024*1024
        ),
    )(
        *[pltpu.with_memory_space_constraint(a, pltpu.HBM) for a in (
        routes.T,
        route_weights.T,
        tokens,
        cotangent,
        expert_gate[0].T,
        expert_up[0].T,
        expert_down[0],
        shared_gate.T,
        shared_up.T,
        shared_down,
        )]
    )
    dx, gr, gg, gu, gd, gsg, gsu, gsd = pl.pallas_call(
        functools.partial(finish, fo),
        out_shape=(
            jax.ShapeDtypeStruct((tok, dq), BF16),
            jax.ShapeDtypeStruct((1, tok), F32),
            jax.ShapeDtypeStruct((fo, width), F32),
            jax.ShapeDtypeStruct((fo, width), F32),
            jax.ShapeDtypeStruct((fo, width), F32),
            jax.ShapeDtypeStruct((fo, cb // 2), F32),
            jax.ShapeDtypeStruct((fo, cb // 2), F32),
            jax.ShapeDtypeStruct((fo, cb // 2), F32),
        ),
        in_specs=[hbm, hbm, vmem, vmem, vmem, hbm],
        out_specs=(hbm,) * 8,
        scratch_shapes=[
            pltpu.VMEM((3, fo, width), F32),
            [pltpu.VMEM((3 * fo, cb // 2), F32), pltpu.VMEM((tok, dq), BF16), pltpu.VMEM((1, tok), F32)],
            pltpu.SemaphoreType.DMA((9,)),
        ],
        compiler_params=pltpu.CompilerParams(vmem_limit_bytes=16*1024*1024),
    )(*outs)
    return (dx, gr.T, gg.T[None], gu.T[None], gd[None], gsg.T, gsu.T, gsd)


def solution(mesh):
    placed = (
        P("ep", None),
        P("ep", None),
        P("ep", None),
        P("ep", None),
        P("ep", None, "tp"),
        P("ep", None, "tp"),
        P("ep", "tp", None),
        P(None, "tp"),
        P(None, "tp"),
        P("tp", None),
    )
    return jax.shard_map(
        functools.partial(local, EP_AXES, CAP),
        mesh=mesh,
        in_specs=placed,
        out_specs=(
            P("ep", "tp"),
            P("ep", "tp"),
            P("ep", None, "tp"),
            P("ep", None, "tp"),
            P("ep", "tp", None),
            P("ep", "tp"),
            P("ep", "tp"),
            P("tp", "ep"),
        ),
        check_vma=False,
    )
```

```python
import functools

import jax
import jax.numpy as jnp
from jax import lax
from jax.experimental import pallas as pl
from jax.experimental.pallas import tpu as pltpu
from jax.sharding import PartitionSpec as P

MESH = pl.DeviceIdType.MESH
F32 = jnp.float32
BF16 = jnp.bfloat16
I32 = jnp.int32
EP_AXES = (8, 4, 2)
CAP = 3
(WEIGHTS, SHARED_DX, SHARED_1, SHARED_2, SHARED_3, SHARED_4, GATHER, BACK, GRADS, GP, DISPATCH, SCATTER) = (
    *range(0, 20, 2),
    22,
    28,
)
DOWN, SCATTER_BACK = 34, 36
PAIRS = 19


def dot_nn(a, b):
    return lax.dot_general(a, b, (((1,), (0,)), ((), ())), preferred_element_type=F32)


def dot_nt(a, b):
    return lax.dot_general(a, b, (((1,), (1,)), ((), ())), preferred_element_type=F32)


def dot_tn(a, b):
    return lax.dot_general(a, b, (((0,), (0,)), ((), ())), preferred_element_type=F32)


def wait_bytes(ref, sem):
    pltpu.make_async_copy(ref, ref, sem).wait()


def swish_parts(v):
    sigma = jax.nn.sigmoid(v)
    return v * sigma, sigma * (1.0 + v * (1.0 - sigma))


def swap_matrix(outer, inner):
    size = outer * inner
    row = lax.broadcasted_iota(I32, (size, size), 0)
    col = lax.broadcasted_iota(I32, (size, size), 1)
    return ((row % inner) * outer + row // inner == col).astype(BF16)


def z_order(nz):
    if nz == 8:
        return (1, 7, 0, 2, 6, 3, 5, 4)
    return tuple(range(nz))


def groups_of(ep):
    part = ep // 8
    return ((0, 5 * part), (5 * part, 2 * part), (7 * part, part))


def own_rows_of(first_rows, tp):
    return -(-first_rows // (8 * tp)) * 8


def kernel(
    sizes,
    routes_in,
    weights_in,
    x_in,
    g_in,
    wg_in,
    wu_in,
    wd_in,
    sg_in,
    su_in,
    sd_in,
    dx_out,
    gr_out,
    gg_out,
    gu_out,
    gd_out,
    gs_out,
    routes,
    weights,
    weight_turn,
    assign_table,
    assign_of,
    scale_table,
    scale_of,
    slot_table,
    slot_of,
    turn,
    x_ref,
    g_ref,
    sg_ref,
    su_ref,
    sd_ref,
    staged,
    tiles,
    send_x,
    recv_x,
    wq,
    rows,
    part,
    rs_send,
    rs_recv,
    rest,
    rest_send,
    rest_recv,
    dall,
    dfull,
    back_send,
    back_recv,
    gp_send,
    gp_mid,
    gp_recv,
    dw_send,
    sdx_send,
    sdx_recv,
    sh1,
    sh1_recv,
    sh2,
    sh2_recv,
    sh3,
    sh3_recv,
    sh4,
    sh4_recv,
    comb,
    grow,
    gs_held,
    dx_held,
    gr_held,
    sem,
    in_sem,
):
    ep, tp, nz, ny, cap, tok, top, dq, ff, cb = sizes
    slots = ep * cap
    nb = dq // 128
    nyc = 2 * ny
    groups = groups_of(ep)
    first_rows = groups[0][1] * cap
    own_rows = own_rows_of(first_rows, tp)
    fo = ff // tp
    chunk = cap * 2 * nb
    me = lax.axis_index("ep")
    q = lax.axis_index("tp")
    core = lax.rem(me, 2)
    yc = lax.rem(me, nyc)
    yy = yc // 2
    zz = me // nyc
    sib = me + 1 - 2 * core

    tp_order = sorted(range(1, tp), key=lambda i: -min(i, tp - i))

    def tp_peer(i):
        return lax.rem(q + i, tp)

    def to_of(dz, w):
        return lax.rem(zz + dz, nz) * nyc + lax.rem(yc + w, nyc)

    def from_of(dz, w):
        return lax.rem(zz + nz - dz, nz) * nyc + lax.rem(yc + nyc - w, nyc)

    def send(src, dst, kind, device):
        pltpu.make_async_remote_copy(
            src_ref=src,
            dst_ref=dst,
            send_sem=sem.at[kind],
            recv_sem=sem.at[kind + 1],
            device_id=device,
            device_id_type=MESH,
        ).start()

    def waits(ref, kind, side):
        wait_bytes(ref, sem.at[kind + side])

    def positions(group):
        start, count = groups[group]
        for k, dz in enumerate(z_order(nz)):
            lo = max(k * nyc, start)
            hi = min((k + 1) * nyc, start + count)
            if lo < hi:
                yield lo - k * nyc, hi - k * nyc, dz, k * nyc

    own_place = z_order(nz).index(0) * nyc

    def block_of(i, size):
        return pl.ds(pl.multiple_of(i * size, size), size)

    barrier = pltpu.get_barrier_semaphore()
    for dz in sorted(range(nz), key=lambda dz: -min(dz, nz - dz)):
        for w in range(1 if dz == 0 else 0, nyc):
            pl.semaphore_signal(barrier, inc=1, device_id={"ep": to_of(dz, w)}, device_id_type=MESH)

    for i in range(1, tp):
        pl.semaphore_signal(barrier, inc=1, device_id={"tp": tp_peer(i)}, device_id_type=MESH)

    own_cols = pl.ds(pl.multiple_of(q * dq, 128), dq)
    fetches = [
        pltpu.make_async_copy(src, dst, in_sem.at[n])
        for n, (src, dst) in enumerate(
            [
                (routes_in, routes),
                (weights_in, weights),
                (x_in, x_ref),
                (g_in, g_ref),
                (sg_in, sg_ref),
                (su_in, su_ref),
                (sd_in, sd_ref),
            ]
            + [(ref, staged.at[t]) for t, ref in enumerate((wg_in, wu_in, wd_in))]
        )
    ]
    for fetch in fetches:
        fetch.start()

    fetches[0].wait()
    turn[...] = jnp.zeros_like(turn)
    turn[0:top, 0:tok] = routes[...]
    by_row = turn[...].T
    fetches[1].wait()
    weight_turn[...] = jnp.zeros_like(weight_turn)
    weight_turn[0:top, 0:tok] = weights[...]
    weight_by_row = weight_turn[...].T
    expert = lax.broadcasted_iota(I32, (32, 128), 1)
    token = lax.broadcasted_iota(I32, (32, 128), 0)
    named = [(by_row[0:32, k : k + 1] == expert) & (token < tok) for k in range(top)]
    count = jnp.zeros((32, 128), I32)
    for k in range(top):
        count = count + named[k].astype(I32)
    before = count
    for shift in (1, 2, 4, 8, 16):
        before = before + jnp.where(token < shift, 0, pltpu.roll(before, shift, 0))
    before = before - count
    weight = jnp.zeros((32, 128), F32)
    for k in range(top):
        weight = weight + jnp.where(named[k], weight_by_row[0:32, k : k + 1], 0.0)
    slot = jnp.zeros((32, 128), I32)
    for k in range(top):
        mine = jnp.sum(jnp.where(named[k], expert * cap + before, 0), axis=1, keepdims=True)
        slot = jnp.where(expert == k, mine, slot)
    slot_table[...] = slot
    for j in range(cap):
        here = (count > 0) & (before == j)
        which = jnp.sum(jnp.where(here, token + 1, 0), axis=0, keepdims=True)
        assign_table[j : j + 1, :] = jnp.where(which > 0, which - 1, tok)
        scale_table[j : j + 1, :] = jnp.sum(jnp.where(here, weight, 0.0), axis=0, keepdims=True)
    tables = [
        pltpu.make_async_copy(assign_table, assign_of, in_sem.at[10]),
        pltpu.make_async_copy(scale_table, scale_of, in_sem.at[11]),
        pltpu.make_async_copy(slot_table, slot_of, in_sem.at[12]),
    ]
    for table in tables:
        table.start()

    fetches[2].wait()
    fetches[3].wait()
    col0 = q * dq
    swap_out = swap_matrix(16, 2 * nb)
    for part_no in range(2):
        lo = part_no * 16
        hi = min(tok, lo + 16)
        pieces = []
        for ref in (x_ref, g_ref):
            for b in range(nb):
                cols = pl.ds(pl.multiple_of(col0 + b * 128, 128), 128)
                piece = ref[lo:hi, cols].astype(F32)
                if hi - lo < 16:
                    piece = jnp.concatenate([piece, jnp.zeros((16 - hi + lo, 128), F32)], axis=0)
                pieces.append(piece)
        stacked = jnp.concatenate(pieces, axis=0).astype(BF16)
        moved = dot_nn(swap_out, stacked)
        tiles[lo : lo + 16] = moved.reshape(16, 2 * nb, 128)

    for table in tables:
        table.wait()
    lower = lax.broadcasted_iota(I32, (2 * nb, 128), 0) < nb

    def pick(group):
        for lo, hi, dz, place in positions(group):

            @pl.loop(lo, hi, unroll=4)
            def _(w):
                p = to_of(dz, w)
                for j in range(cap):
                    tile = tiles[assign_of[j, p]]
                    scale = jnp.where(lower, jnp.float32(1.0), scale_of[j, p])
                    at = pl.ds(pl.multiple_of(((place + w) * cap + j) * 2 * nb, 2 * nb), 2 * nb)
                    send_x[at, :] = (tile * scale).astype(BF16)

    def dispatch(group):
        for lo, hi, dz, place in positions(group):

            @pl.loop(max(lo, 1) if dz == 0 else lo, hi, unroll=4)
            def _(w):
                here = block_of(place + w, chunk)
                send(send_x.at[here, :], recv_x.at[here, :], DISPATCH + 2 * group, {"ep": to_of(dz, w)})

    pick(0)
    pl.semaphore_wait(barrier, ep - 1 + tp - 1)

    dispatch(0)
    for n in (7, 8, 9):
        fetches[n].wait()
    for types, kind in (((0, 1), WEIGHTS), ((2,), DOWN)):
        for i in tp_order:
            for t in types:
                dst_rows = pl.ds(pl.multiple_of(t * ff + q * fo, 16), fo)
                src_cols = pl.ds(pl.multiple_of(tp_peer(i) * dq, 128), dq)
                send(staged.at[t, :, src_cols], wq.at[dst_rows, :], kind, {"tp": tp_peer(i)})
    pick(1)
    dispatch(1)
    pick(2)
    dispatch(2)
    recv_x[own_place * chunk : (own_place + 1) * chunk, :] = send_x[own_place * chunk : (own_place + 1) * chunk, :]

    for n in (4, 5, 6):
        fetches[n].wait()
    x = x_ref[...]
    s_gate = dot_nt(x, sg_ref[...])
    s_up = dot_nt(x, su_ref[...])
    s_back = dot_nt(g_ref[...], sd_ref[...])
    s_active, s_slope = swish_parts(s_gate)
    s_hidden = (s_active * s_up).astype(BF16)
    ds_gate = (s_back * s_up * s_slope).astype(BF16)
    ds_up = (s_back * s_active).astype(BF16)
    for j in range(tp):
        cols = slice(j * dq, (j + 1) * dq)
        piece = dot_nn(ds_gate, sg_ref[:, cols]) + dot_nn(ds_up, su_ref[:, cols])
        sdx_send[j] = piece.astype(BF16)
    half = 3 * fo // 2
    for z in range(nz):
        cols = slice(z * ny * cb, (z + 1) * ny * cb)
        xz = x_ref[:, cols]
        whole = jnp.concatenate(
            [dot_tn(ds_gate, xz), dot_tn(ds_up, xz), dot_tn(s_hidden, g_ref[:, cols])], axis=0
        )
        for y in range(ny):
            for h in range(2):
                sh1[h, y, z] = whole[h * half : (h + 1) * half, y * cb : (y + 1) * cb].astype(BF16)
    send(sh1.at[1 - core], sh1_recv, SHARED_1, {"ep": sib})

    waits(sh1_recv, SHARED_1, 1)
    for y in range(ny):
        for z in range(nz):
            both = sh1[core, y, z].astype(F32) + sh1_recv[y, z].astype(F32)
            sh2[y, z] = both.astype(BF16)
    for i in range(1, ny):
        y = lax.rem(yy + i, ny)
        send(sh2.at[y], sh2_recv.at[yy], SHARED_2, {"ep": (zz * ny + y) * 2 + core})

    swap_in = {n: swap_matrix(2 * nb, n) for n in (8, 16)}
    swap_back = {n: swap_matrix(n, nb) for n in (8, 16)}

    def steps_of(base, count):
        lo = base
        while lo < base + count:
            n = 16 if lo % 16 == 0 and lo + 16 <= base + count else 8
            yield lo, n
            lo += n

    def arrived(group):
        start, count = groups[group]
        own = 1 if start <= own_place < start + count else 0
        waits(recv_x.at[pl.ds(0, (count - own) * chunk), :], DISPATCH + 2 * group, 1)

    def relayout(group):
        base, count = groups[group][0] * cap, groups[group][1] * cap
        for lo, n in steps_of(base, count):
            moved = dot_nn(swap_in[n], recv_x[lo * 2 * nb : (lo + n) * 2 * nb, :])
            for b in range(2 * nb):
                rows[lo : lo + n, b * 128 : (b + 1) * 128] = moved[b * n : (b + 1) * n].astype(BF16)

    def contract(group):
        base, count = groups[group][0] * cap, groups[group][1] * cap
        relayout(group)
        up_part = dot_nt(rows[base : base + count, 0:dq], wq[0 : 2 * ff, :])
        back_part = dot_nt(rows[base : base + count, dq : 2 * dq], wq[2 * ff : 3 * ff, :])
        return up_part, back_part

    def packed_rows(n):
        return n + -(-n // 16) * 8

    def pack(ref, up, back):
        n = up.shape[0]
        half_n = packed_rows(n) - n
        ref[0:n, :] = up.astype(ref.dtype)
        ref[n : n + half_n, 0:ff] = back[0:half_n].astype(ref.dtype)
        ref[n : n + n - half_n, ff : 2 * ff] = back[half_n:n].astype(ref.dtype)

    def unpacked(total, n):
        half_n = packed_rows(n) - n
        back = jnp.concatenate([total[n : n + half_n, 0:ff], total[n : n + n - half_n, ff : 2 * ff]], axis=0)
        return total[0:n, 0:ff], total[0:n, ff : 2 * ff], back

    own_tall = packed_rows(own_rows)

    def blocks_of(whole):
        for b in range(tp):
            lo, hi = b * own_rows, min((b + 1) * own_rows, first_rows)
            block = whole[lo:hi]
            if hi - lo < own_rows:
                block = jnp.concatenate([block, jnp.zeros((own_rows - hi + lo, whole.shape[1]), F32)], axis=0)
            yield b, block

    def scatter_up():
        relayout(0)
        for b, block in blocks_of(dot_nt(rows[0:first_rows, 0:dq], wq[0 : 2 * ff, :])):
            part[b, 0:own_rows, :] = block
            rs_send[b, 0:own_rows, :] = block.astype(BF16)
        here = pl.ds(0, own_rows)
        for i in tp_order:
            send(rs_send.at[tp_peer(i), here], rs_recv.at[q, here], SCATTER, {"tp": tp_peer(i)})

    def scatter_back():
        half_n = own_tall - own_rows
        for b, block in blocks_of(dot_nt(rows[0:first_rows, dq : 2 * dq], wq[2 * ff : 3 * ff, :])):
            for ref in (part, rs_send):
                ref[b, own_rows:own_tall, 0:ff] = block[0:half_n].astype(ref.dtype)
                ref[b, own_rows : 2 * own_rows - half_n, ff : 2 * ff] = block[half_n:own_rows].astype(ref.dtype)
        here = pl.ds(own_rows, half_n)
        for i in tp_order:
            send(rs_send.at[tp_peer(i), here], rs_recv.at[q, here], SCATTER_BACK, {"tp": tp_peer(i)})

    def spread_rest(group):
        up_part, back_part = contract(group)
        n = group - 1
        pack(rest[n], up_part, back_part)
        pack(rest_send[n], up_part, back_part)
        for i in tp_order:
            send(rest_send[n], rest_recv[n].at[q], SCATTER + 2 * group, {"tp": tp_peer(i)})

    def gradients(total, n):
        gate, up, back = unpacked(total, n)
        active, slope = swish_parts(gate)
        hidden = (active * up).astype(BF16).astype(F32)
        gp = jnp.sum(hidden * back, axis=1, keepdims=True)
        extra = dfull.shape[1] - 3 * ff
        return jnp.concatenate(
            [back * up * slope, back * active, hidden, jnp.broadcast_to(gp, (gp.shape[0], extra))], axis=1
        )

    def gather_first():
        waits(rs_recv.at[pl.ds(0, tp - 1), pl.ds(0, own_rows)], SCATTER, 1)
        waits(rs_recv.at[pl.ds(0, tp - 1), pl.ds(own_rows, own_tall - own_rows)], SCATTER_BACK, 1)
        total = part[q]
        for i in range(1, tp):
            total = total + rs_recv[tp_peer(i)].astype(F32)
        dall[q] = gradients(total, own_rows).astype(BF16)
        mine = dall.at[q]
        for i in tp_order:
            send(mine, mine, GATHER, {"tp": tp_peer(i)})

    def finish_first():
        waits(dall.at[pl.ds(0, tp - 1)], GATHER, 1)
        for b in range(tp):
            lo, hi = b * own_rows, min((b + 1) * own_rows, first_rows)
            dfull[lo:hi, :] = dall[b].astype(F32)[0 : hi - lo]

    def finish_rest(group):
        n = group - 1
        waits(rest_recv[n].at[pl.ds(0, tp - 1)], SCATTER + 2 * group, 1)
        total = rest[n][...]
        for i in range(1, tp):
            total = total + rest_recv[n][tp_peer(i)].astype(F32)
        base, count = groups[group][0] * cap, groups[group][1] * cap
        dfull[base : base + count, :] = gradients(total, count)

    def send_back(group):
        start, places = groups[group]
        base, count = start * cap, places * cap
        d = dfull[base : base + count, :]
        dxr = dot_nn(d[:, 0 : 2 * ff].astype(BF16), wq[0 : 2 * ff, :])
        for lo, n in steps_of(0, count):
            stacked = jnp.concatenate(
                [dxr[lo : lo + n, b * 128 : (b + 1) * 128] for b in range(nb)], axis=0
            ).astype(BF16)
            moved = dot_nn(swap_back[n], stacked)
            back_send[base + lo : base + lo + n] = moved.reshape(n, nb, 128).astype(BF16)
        for lo, hi, dz, place in positions(group):
            if dz == 0 and lo == 0:
                back_recv[pl.ds(me * cap, cap)] = back_send[place * cap : (place + 1) * cap]

            @pl.loop(max(lo, 1) if dz == 0 else lo, hi, unroll=4)
            def _(w):
                to = {"ep": from_of(dz, w)}
                send(
                    back_send.at[pl.ds((place + w) * cap, cap)],
                    back_recv.at[pl.ds(me * cap, cap)],
                    BACK,
                    to,
                )

    def send_route_sums(group):
        start, places = groups[group]
        base, count = start * cap, places * cap
        d = dfull[base : base + count, :]
        src_row = lax.broadcasted_iota(I32, (places, count), 0)
        src_col = lax.broadcasted_iota(I32, (places, count), 1)
        collect = (src_col // cap == src_row).astype(F32)
        lane = lax.broadcasted_iota(I32, (count, 128), 1)
        slot_row = lax.broadcasted_iota(I32, (count, 128), 0)
        spread = jnp.where(lane == slot_row % cap, d[:, 3 * ff : 3 * ff + 1], 0.0)
        gp_send[start : start + places] = dot_nn(collect, spread).reshape(places, 1, 128)
        for lo, hi, dz, place in positions(group):
            if dz == 0:
                gp_mid[zz, lo:hi] = gp_send[place + lo : place + hi]
            else:
                send(
                    gp_send.at[pl.ds(place + lo, hi - lo)],
                    gp_mid.at[zz, pl.ds(lo, hi - lo)],
                    GP,
                    {"ep": from_of(dz, 0)},
                )

    def spread_route_sums():
        if nz > 1:
            waits(gp_mid.at[pl.ds(0, nz - 1)], GP, 1)
        for w in range(1, nyc):
            send(gp_mid.at[:, w], gp_recv.at[:, yc], GP + 2, {"ep": from_of(0, w)})
        gp_recv[:, yc] = gp_mid[:, 0]

    for t in range(3):
        wq[pl.ds(pl.multiple_of(t * ff + q * fo, 16), fo), :] = staged[t, :, own_cols]
    waits(wq.at[pl.ds(0, 2 * (tp - 1) * fo), :], WEIGHTS, 1)
    arrived(0)
    scatter_up()
    waits(wq.at[pl.ds(0, (tp - 1) * fo), :], DOWN, 1)
    scatter_back()
    for i in tp_order:
        send(sdx_send.at[tp_peer(i)], sdx_recv.at[q], SHARED_DX, {"tp": tp_peer(i)})
    gather_first()
    arrived(1)
    spread_rest(1)
    arrived(2)
    spread_rest(2)
    if ny > 1:
        waits(sh2_recv.at[pl.ds(0, ny - 1)], SHARED_2, 1)
    for z in range(nz):
        total = sh2[yy, z].astype(F32)
        for i in range(1, ny):
            total = total + sh2_recv[lax.rem(yy + i, ny), z].astype(F32)
        sh3[z] = total.astype(BF16)
    for i in range(1, nz):
        z = lax.rem(zz + i, nz)
        send(sh3.at[z], sh3_recv.at[zz], SHARED_3, {"ep": (z * ny + yy) * 2 + core})
    finish_first()
    send_route_sums(0)
    send_back(0)
    finish_rest(1)
    finish_rest(2)
    d = dfull[:, 0 : 3 * ff].astype(BF16)
    own_grads = []

    def send_grads(t, out):
        for i in tp_order:
            src_rows = pl.ds(pl.multiple_of(t * ff + tp_peer(i) * fo, 16), fo)
            send(dw_send.at[src_rows, :], out.at[:, own_cols], GRADS, {"tp": tp_peer(i)})
        mine = pl.ds(pl.multiple_of(t * ff + q * fo, 16), fo)
        own_grads.append(pltpu.make_async_copy(dw_send.at[mine, :], out.at[:, own_cols], in_sem.at[t]))
        own_grads[-1].start()

    dw_send[2 * ff : 3 * ff, :] = dot_tn(d[:, 2 * ff : 3 * ff], rows[:, dq : 2 * dq]).astype(BF16)
    send_grads(2, gd_out)
    dw_send[0 : 2 * ff, :] = dot_tn(d[:, 0 : 2 * ff], rows[:, 0:dq]).astype(BF16)
    send_grads(0, gg_out)
    send_grads(1, gu_out)
    send_route_sums(2)
    send_route_sums(1)
    send_back(2)
    send_back(1)
    spread_route_sums()

    if nz > 1:
        waits(sh3_recv.at[pl.ds(0, nz - 1)], SHARED_3, 1)
    total = sh3[zz].astype(F32)
    for i in range(1, nz):
        total = total + sh3_recv[lax.rem(zz + i, nz)].astype(F32)
    sh4[...] = total
    send(sh4, sh4_recv, SHARED_4, {"ep": sib})
    waits(sdx_recv.at[pl.ds(0, tp - 1)], SHARED_DX, 1)
    waits(sh4_recv, SHARED_4, 1)
    first = core == 0
    full = jnp.concatenate(
        [
            jnp.where(first, sh4[...], sh4_recv[...]),
            jnp.where(first, sh4_recv[...], sh4[...]),
        ],
        axis=0,
    )
    gs_held[...] = jnp.where(first, full[:, 0 : cb // 2], full[:, cb // 2 : cb])
    own_grads.append(pltpu.make_async_copy(gs_held, gs_out, in_sem.at[3]))
    own_grads[-1].start()

    waits(back_recv.at[pl.ds(0, (ep - 1) * cap)], BACK, 1)
    waits(gp_recv.at[:, pl.ds(0, nyc - 1)], GP + 2, 1)
    row_lane = lax.broadcasted_iota(I32, (1, 128), 1)
    comb[...] = jnp.zeros_like(comb)
    for t in range(tok):
        total = back_recv[slot_of[t, 0]].astype(F32)
        for k in range(1, top):
            total = total + back_recv[slot_of[t, k]].astype(F32)
        comb[t] = total
        s = slot_of[t, q]
        value = jnp.where(row_lane == s % cap, gp_recv[s // (cap * nyc), (s // cap) % nyc], 0.0)
        grow[t : t + 1, :] = value
    gr_held[...] = jnp.sum(grow[...].T, axis=0, keepdims=True)[:, 0:tok] / weights[pl.ds(q, 1), :]
    swap_tok = swap_matrix(nb, 16)
    for part_no in range(2):
        lo = part_no * 16
        hi = min(tok, lo + 16)
        v = comb[lo : lo + 16].reshape(16 * nb, 128)
        top_half = v.astype(BF16)
        rest = (v - top_half.astype(F32)).astype(BF16)
        moved = dot_nn(swap_tok, top_half) + dot_nn(swap_tok, rest)
        for b in range(nb):
            cols = slice(b * 128, (b + 1) * 128)
            value = moved[b * 16 : b * 16 + hi - lo]
            value = value + sdx_send[q, lo:hi, cols].astype(F32)
            for i in range(1, tp):
                value = value + sdx_recv[tp_peer(i), lo:hi, cols].astype(F32)
            dx_held[lo:hi, cols] = value.astype(BF16)

    for n, (src, dst) in enumerate(((dx_held, dx_out), (gr_held, gr_out))):
        own_grads.append(pltpu.make_async_copy(src, dst, in_sem.at[4 + n]))
        own_grads[-1].start()
    waits(wq.at[pl.ds(0, 2 * (tp - 1) * fo), :], WEIGHTS, 0)
    waits(wq.at[pl.ds(0, (tp - 1) * fo), :], DOWN, 0)
    for group, (start, count) in enumerate(groups):
        own = 1 if start <= own_place < start + count else 0
        waits(send_x.at[pl.ds(0, (count - own) * chunk), :], DISPATCH + 2 * group, 0)
    waits(sdx_send.at[pl.ds(0, tp - 1)], SHARED_DX, 0)
    waits(sh1_recv, SHARED_1, 0)
    if ny > 1:
        waits(sh2.at[pl.ds(0, ny - 1)], SHARED_2, 0)
    if nz > 1:
        waits(sh3.at[pl.ds(0, nz - 1)], SHARED_3, 0)
    waits(rs_send.at[pl.ds(0, tp - 1), pl.ds(0, own_rows)], SCATTER, 0)
    waits(rs_send.at[pl.ds(0, tp - 1), pl.ds(own_rows, own_tall - own_rows)], SCATTER_BACK, 0)
    waits(dall.at[pl.ds(0, tp - 1)], GATHER, 0)
    for n in range(2):
        waits(rest_recv[n].at[pl.ds(0, tp - 1)], SCATTER + 2 + 2 * n, 0)
    waits(back_send.at[pl.ds(0, (ep - 1) * cap)], BACK, 0)
    if nz > 1:
        waits(gp_mid.at[pl.ds(0, nz - 1)], GP, 0)
    waits(gp_recv.at[:, pl.ds(0, nyc - 1)], GP + 2, 0)
    waits(sh4, SHARED_4, 0)
    waits(dw_send.at[pl.ds(0, 3 * (tp - 1) * fo), :], GRADS, 0)
    for copy in own_grads:
        copy.wait()
    waits(dw_send.at[pl.ds(0, 3 * (tp - 1) * fo), :], GRADS, 1)


def finish(fo, dx, gr, gg, gu, gd, gs, dx_o, gr_o, gg_o, gu_o, gd_o, gsg_o, gsu_o, gsd_o, wide, small, sem):
    width = gg.shape[1]
    parts = 2
    step = width // parts
    others = [(gs, small[0]), (dx, small[1]), (gr, small[2])]
    ins = [pltpu.make_async_copy(src, dst, sem.at[1 + n]) for n, (src, dst) in enumerate(others)]
    for copy in ins:
        copy.start()
    stores = []
    for t, (src, dst) in enumerate(((gg, gg_o), (gu, gu_o), (gd, gd_o))):
        for c in range(parts):
            cols = slice(c * step, (c + 1) * step)
            wide[t, :, cols] = src[:, cols].astype(F32)
            pltpu.make_async_copy(wide.at[t, :, cols], dst.at[:, cols], sem.at[0]).start()
    for copy in ins:
        copy.wait()
    outs = [(small[0].at[t * fo : (t + 1) * fo], dst) for t, dst in enumerate((gsg_o, gsu_o, gsd_o))]
    outs += [(small[1], dx_o), (small[2], gr_o)]
    for n, (src, dst) in enumerate(outs):
        stores.append(pltpu.make_async_copy(src, dst, sem.at[4 + n]))
        stores[-1].start()
    for copy in stores:
        copy.wait()
    wait_bytes(wide, sem.at[0])


def local(axes, cap, tokens, cotangent, routes, route_weights, expert_gate, expert_up, expert_down, shared_gate, shared_up, shared_down):
    tok, width = tokens.shape
    top = routes.shape[1]
    nz, ny, _ = axes
    ep = lax.axis_size("ep")
    tp = lax.axis_size("tp")
    fo = expert_gate.shape[2]
    ff = fo * tp
    dq = width // tp
    nb = dq // 128
    cb = width // (nz * ny)
    slots = ep * cap
    groups = groups_of(ep)
    own_rows = own_rows_of(groups[0][1] * cap, tp)
    taller = lambda n: n + -(-n // 16) * 8
    rest_rows = [count * cap for _, count in groups[1:]]
    wide = -(-(3 * ff + 1) // 128) * 128
    half = 3 * fo // 2

    sizes = (ep, tp, nz, ny, cap, tok, top, dq, ff, cb)
    vmem = pl.BlockSpec(memory_space=pltpu.VMEM)
    hbm = pl.BlockSpec(memory_space=pltpu.HBM)
    outs = pl.pallas_call(
        functools.partial(kernel, sizes),
        out_shape=(
            jax.ShapeDtypeStruct((tok, dq), BF16),
            jax.ShapeDtypeStruct((1, tok), F32),
            jax.ShapeDtypeStruct((fo, width), BF16),
            jax.ShapeDtypeStruct((fo, width), BF16),
            jax.ShapeDtypeStruct((fo, width), BF16),
            jax.ShapeDtypeStruct((3 * fo, cb // 2), F32),
        ),
        in_specs=[hbm] * 10,
        out_specs=(hbm, hbm, vmem, vmem, vmem, hbm),
        scratch_shapes=[
            pltpu.VMEM((top, tok), I32),
            pltpu.VMEM((top, tok), F32),
            pltpu.VMEM((8, 128), F32),
            pltpu.VMEM((-(-cap // 8) * 8, 128), I32),
            pltpu.SMEM((-(-cap // 8) * 8, 128), I32),
            pltpu.VMEM((-(-cap // 8) * 8, 128), F32),
            pltpu.SMEM((-(-cap // 8) * 8, 128), F32),
            pltpu.VMEM((32, 128), I32),
            pltpu.SMEM((32, 128), I32),
            pltpu.VMEM((8, 128), I32),
            pltpu.VMEM((tok, width), BF16),
            pltpu.VMEM((tok, width), BF16),
            pltpu.VMEM((fo, width), BF16),
            pltpu.VMEM((fo, width), BF16),
            pltpu.VMEM((fo, width), BF16),
            pltpu.VMEM((3, fo, width), BF16),
            pltpu.VMEM((32, 2 * nb, 128), F32),
            pltpu.VMEM((slots * 2 * nb, 128), BF16),
            pltpu.VMEM((slots * 2 * nb, 128), BF16),
            pltpu.VMEM((3 * ff, dq), BF16),
            pltpu.VMEM((slots, 2 * dq), BF16),
            pltpu.VMEM((tp, taller(own_rows), 2 * ff), F32),
            pltpu.VMEM((tp, taller(own_rows), 2 * ff), BF16),
            pltpu.VMEM((tp, taller(own_rows), 2 * ff), BF16),
            [pltpu.VMEM((taller(n), 2 * ff), F32) for n in rest_rows],
            [pltpu.VMEM((taller(n), 2 * ff), BF16) for n in rest_rows],
            [pltpu.VMEM((tp, taller(n), 2 * ff), BF16) for n in rest_rows],
            pltpu.VMEM((tp, own_rows, wide), BF16),
            pltpu.VMEM((slots, wide), F32),
            pltpu.VMEM((slots, nb, 128), BF16),
            pltpu.VMEM((slots, nb, 128), BF16),
            pltpu.VMEM((ep, 1, 128), F32),
            pltpu.VMEM((nz, 2 * ny, 1, 128), F32),
            pltpu.VMEM((nz, 2 * ny, 1, 128), F32),
            pltpu.VMEM((3 * ff, dq), BF16),
            pltpu.VMEM((tp, tok, dq), BF16),
            pltpu.VMEM((tp, tok, dq), BF16),
            pltpu.VMEM((2, ny, nz, half, cb), BF16),
            pltpu.VMEM((ny, nz, half, cb), BF16),
            pltpu.VMEM((ny, nz, half, cb), BF16),
            pltpu.VMEM((ny, nz, half, cb), BF16),
            pltpu.VMEM((nz, half, cb), BF16),
            pltpu.VMEM((nz, half, cb), BF16),
            pltpu.VMEM((half, cb), F32),
            pltpu.VMEM((half, cb), F32),
            pltpu.VMEM((32, nb, 128), F32),
            pltpu.VMEM((32, 128), F32),
            pltpu.VMEM((3 * fo, cb // 2), F32),
            pltpu.VMEM((tok, dq), BF16),
            pltpu.VMEM((1, tok), F32),
            pltpu.SemaphoreType.DMA((2 * PAIRS,)),
            pltpu.SemaphoreType.DMA((13,)),
        ],
        compiler_params=pltpu.CompilerParams(
            collective_id=0, has_side_effects=True, vmem_limit_bytes=50*1024*1024
        ),
    )(
        *[pltpu.with_memory_space_constraint(a, pltpu.HBM) for a in (
        routes.T,
        route_weights.T,
        tokens,
        cotangent,
        expert_gate[0].T,
        expert_up[0].T,
        expert_down[0],
        shared_gate.T,
        shared_up.T,
        shared_down,
        )]
    )
    dx, gr, gg, gu, gd, gsg, gsu, gsd = pl.pallas_call(
        functools.partial(finish, fo),
        out_shape=(
            jax.ShapeDtypeStruct((tok, dq), BF16),
            jax.ShapeDtypeStruct((1, tok), F32),
            jax.ShapeDtypeStruct((fo, width), F32),
            jax.ShapeDtypeStruct((fo, width), F32),
            jax.ShapeDtypeStruct((fo, width), F32),
            jax.ShapeDtypeStruct((fo, cb // 2), F32),
            jax.ShapeDtypeStruct((fo, cb // 2), F32),
            jax.ShapeDtypeStruct((fo, cb // 2), F32),
        ),
        in_specs=[hbm, hbm, vmem, vmem, vmem, hbm],
        out_specs=(hbm,) * 8,
        scratch_shapes=[
            pltpu.VMEM((3, fo, width), F32),
            [pltpu.VMEM((3 * fo, cb // 2), F32), pltpu.VMEM((tok, dq), BF16), pltpu.VMEM((1, tok), F32)],
            pltpu.SemaphoreType.DMA((9,)),
        ],
        compiler_params=pltpu.CompilerParams(vmem_limit_bytes=16*1024*1024),
    )(*outs)
    return (dx, gr.T, gg.T[None], gu.T[None], gd[None], gsg.T, gsu.T, gsd)


def solution(mesh):
    placed = (
        P("ep", None),
        P("ep", None),
        P("ep", None),
        P("ep", None),
        P("ep", None, "tp"),
        P("ep", None, "tp"),
        P("ep", "tp", None),
        P(None, "tp"),
        P(None, "tp"),
        P("tp", None),
    )
    return jax.shard_map(
        functools.partial(local, EP_AXES, CAP),
        mesh=mesh,
        in_specs=placed,
        out_specs=(
            P("ep", "tp"),
            P("ep", "tp"),
            P("ep", None, "tp"),
            P("ep", None, "tp"),
            P("ep", "tp", None),
            P("ep", "tp"),
            P("ep", "tp"),
            P("tp", "ep"),
        ),
        check_vma=False,
    )
```
